32 devices in a mesh: fs: 16 (over z, y, x), tp: 2 (over core).
Axes of the slice: x: 2, y: 2, z: 4, core: 2. Of those that a mesh axis runs over, the one named last changes fastest.
Arguments:
- tokens: bfloat16 [5120, 2048], P('fs'), may hold values from -6 to 6
- w_gate: bfloat16 [2048, 5632], P('fs', 'tp'), may hold values from -0.125 to 0.125
- w_up: bfloat16 [2048, 5632], P('fs', 'tp'), may hold values from -0.125 to 0.125
- w_down: bfloat16 [5632, 2048], P('tp', 'fs'), may hold values from -0.078125 to 0.078125
- w_mix_in: bfloat16 [2048, 1024], P('fs', 'tp'), may hold values from -0.125 to 0.125
- w_mix_out: bfloat16 [1024, 2048], P('tp', 'fs'), may hold values from -0.1875 to 0.1875
- pool_w: bfloat16 [8, 128, 128], P('tp'), may hold values from -0.5 to 0.5
- pool_scale: bfloat16 [1024], P('tp'), may hold values from 0.099609375 to 1.8984375
- norm_gains: float32 [6, 2048], replicated, may hold values from 0.1 to 1.9
Outputs:
- layer_out: bfloat16 [5120, 2048], P(('fs', 'tp'))
The draws below stay inside these ranges and needn't reach their ends.
All inputs are finite; a program needn't handle non-finite values.
Results may differ from the reference program's by a relative error of at most 0.018.
Values may be sent and summed in bfloat16 or wider, within the bound.
A program may use at most 128 MiB of HBM per device.

```python
import jax
import jax.numpy as jnp
from jax import lax

D = 2048
FF = 5632
GD = 128
NGROUP = 8
POOLW = 1024
LEN = 64
TOKENS = 5120
N_TP = 2


def levels(stream_key, shape, pieces, least, high):
    level, own = 1.0, jax.random.fold_in(stream_key, 6)
    for axis_at, parts in pieces:
        draws = jnp.exp(jax.random.uniform(jax.random.fold_in(own, axis_at), (parts,), jnp.float32, least / len(pieces), high / len(pieces)))
        level = level * jnp.repeat(draws, shape[axis_at] // parts).reshape([-1 if axis == axis_at else 1 for axis in range(len(shape))])
    return level


def bell_draw(own_key, shape, spread, most, pieces=(), kind=jnp.bfloat16):
    array = jax.random.normal(own_key, shape, jnp.float32) * spread
    if len(pieces) > 0:
        array = levels(own_key, shape, pieces, -0.22, 0.18) * array
    return jnp.clip(array, min=-most, max=most).astype(kind)


def setup_inputs(seed: int = 0) -> dict:
    key_list = jax.random.split(jax.random.key(seed), 10)
    return {
        "tokens": bell_draw(key_list[0], (TOKENS, D), 1.0, 6.0, ((0, 16),)),
        "w_gate": bell_draw(key_list[1], (D, FF), D ** -0.5, 0.125, ((0, 16), (1, 2))),
        "w_up": bell_draw(key_list[2], (D, FF), D ** -0.5, 0.125, ((0, 16), (1, 2))),
        "w_down": bell_draw(key_list[3], (FF, D), FF ** -0.5, 0.078125, ((0, 2), (1, 16))),
        "w_mix_in": bell_draw(key_list[4], (D, POOLW), D ** -0.5, 0.125, ((0, 16), (1, 2))),
        "w_mix_out": bell_draw(key_list[5], (POOLW, D), POOLW ** -0.5, 0.1875, ((0, 2), (1, 16))),
        "pool_w": bell_draw(key_list[6], (NGROUP, GD, GD), GD ** -0.5, 0.5, ((0, 2),)),
        "pool_scale": jnp.clip(1.0 + 0.18 * jax.random.normal(key_list[7], (POOLW,), jnp.float32), 0.099609375, 1.8984375).astype(jnp.bfloat16),
        "norm_gains": jnp.clip(1.0 + 0.18 * jax.random.normal(key_list[8], (6, D), jnp.float32), 0.1, 1.9),
    }


def rms_scale(values, gain):
    return values * lax.rsqrt(lax.optimization_barrier(jnp.mean(values * values, axis=-1, keepdims=True)) + 1e-06) * gain

def split_sum(left_rows, right_matrix):
    block_width = left_rows.shape[1] // N_TP

    def add_block(block_id, running_sum):
        offset = (block_id * block_width).astype(jnp.int32)
        left_part = lax.dynamic_slice_in_dim(left_rows, offset, block_width, 1)
        right_part = lax.dynamic_slice_in_dim(right_matrix, offset, block_width, 0)
        partial_value = jnp.dot(left_part, right_part, preferred_element_type=jnp.float32).astype(jnp.bfloat16)
        partial_value = lax.optimization_barrier(partial_value)
        return running_sum + partial_value.astype(jnp.float32)
    initial = jnp.zeros((left_rows.shape[0], right_matrix.shape[1]), jnp.float32)
    return lax.fori_loop(0, N_TP, add_block, initial)

def gated(normed, w_gate, w_up):
    gate_part = jnp.dot(normed, w_gate, preferred_element_type=jnp.float32)
    up_part = jnp.dot(normed, w_up, preferred_element_type=jnp.float32)
    return (jax.nn.silu(gate_part) * up_part).astype(jnp.bfloat16)

def pool_mix(pooled_in, pool_w, pool_scale):
    values = pooled_in.astype(jnp.float32).reshape(-1, LEN, NGROUP, GD)
    totals = jnp.cumsum(values, axis=1)
    position = jnp.arange(1, LEN + 1).astype(jnp.float32)[None, :, None]
    averages = []
    for group_id in range(NGROUP):
        window = 2 ** (1 + group_id % 4)
        running = totals[:, :, group_id]
        lagged = jnp.pad(running, ((0, 0), (window, 0), (0, 0)))[:, :LEN]
        averages.append((running - lagged) / jnp.minimum(position, float(window)))
    average = jnp.stack(averages, axis=2)
    deviation = (average - values).astype(jnp.bfloat16)
    regrouped = jnp.einsum('btgi,gio->btgo', deviation.astype(jnp.float32), pool_w.astype(jnp.float32))
    regrouped = regrouped.reshape(-1, NGROUP * GD) * pool_scale.astype(jnp.float32)
    return regrouped.astype(jnp.bfloat16)

def reference(tokens, w_gate, w_up, w_down, w_mix_in, w_mix_out, pool_w, pool_scale, norm_gains):
    scales = norm_gains.astype(jnp.float32)
    stream = tokens.astype(jnp.float32)
    normed = rms_scale(stream, scales[0]).astype(jnp.bfloat16)
    stream = stream + 0.5 * rms_scale(split_sum(gated(normed, w_gate, w_up), w_down), scales[1])
    normed = rms_scale(stream, scales[2]).astype(jnp.bfloat16)
    pooled_in = jnp.dot(normed, w_mix_in, preferred_element_type=jnp.float32).astype(jnp.bfloat16)
    stream = stream + rms_scale(split_sum(pool_mix(pooled_in, pool_w, pool_scale), w_mix_out), scales[3])
    normed = rms_scale(stream, scales[4]).astype(jnp.bfloat16)
    stream = stream + 0.5 * rms_scale(split_sum(gated(normed, w_gate, w_up), w_down), scales[5])
    return stream.astype(jnp.bfloat16)
```

```python
import functools
import itertools

import jax
import jax.numpy as jnp
from jax import lax
from jax.experimental import pallas as pl
from jax.experimental.pallas import tpu as pltpu
from jax.sharding import PartitionSpec as P

LEN = 64
MESH = pl.DeviceIdType.MESH


def line_dims(mesh):
    devices = mesh.devices.reshape(mesh.shape["fs"], -1)[:, 0]
    count = len(devices)
    coords = [tuple(getattr(d, "coords", ())) for d in devices]
    dims = []
    for axis in range(len(coords[0])):
        values = sorted({c[axis] for c in coords})
        if len(values) > 1:
            stride = next(i for i in range(count) if coords[i][axis] != coords[0][axis])
            dims.append((len(values), stride, axis, values))
    dims.sort(key=lambda d: -d[1])
    good = len(dims) > 0 and all(
        sum(vals.index(c[axis]) * stride for _, stride, axis, vals in dims) == i
        for i, c in enumerate(coords)
    )
    if not good:
        return ((count, 1),)
    return tuple((d[0], d[1]) for d in dims)


def near(position, size, rank):
    inner = jnp.minimum(position, size - 1 - position)
    alternating = rank <= 2 * inner
    distance = jnp.where(alternating, (rank + 1) // 2, rank - inner)
    toward_high = jnp.where(alternating, rank % 2 == 1, 2 * position < size - 1)
    step = jnp.where(toward_high, 1, -1)
    return position + step * distance, -step


def piece_plan(dims, order):
    sizes = [dims[d][0] for d in order]
    slots = []
    for ranks in itertools.product(*[range(n) for n in sizes]):
        slots.append(ranks)
    slots.sort(key=lambda r: (sum(r), r))
    return slots


class Piece:
    def __init__(self, index, dims, order, src_of, dst_of):
        self.index, self.dims, self.order = index, dims, order
        self.src_of, self.dst_of = src_of, dst_of
        self.slots = piece_plan(dims, order)

    def locate(self, me, ranks):
        source, last, away = me, -1, None
        for place, (d, rank) in enumerate(zip(self.order, ranks)):
            if rank > 0:
                size, stride = self.dims[d]
                position = (me // stride) % size
                found, step = near(position, size, rank)
                source = source + (found - position) * stride
                last, away = place, step
        return source, last, away

    def sends(self, me, ranks):
        _, last, away = self.locate(me, ranks)
        out = []
        for place, d in enumerate(self.order):
            size, stride = self.dims[d]
            position = (me // stride) % size
            if place == last:
                if size > 2:
                    ok = jnp.logical_and(position + away >= 0, position + away < size)
                    out.append((ok, me + away * stride))
            elif place > last:
                if size == 2:
                    out.append((None, me + (1 - 2 * position) * stride))
                else:
                    out.append((position + 1 < size, me + stride))
                    out.append((position > 0, me - stride))
        return out


def when(condition, act):
    if condition is None:
        act()
    else:
        pl.when(condition)(act)


def spread(pieces, me, chunk, send_sem, recv_sem, low, high, mode):
    todo = []
    for piece in pieces:
        for ranks in piece.slots:
            todo.append((sum(ranks), piece, ranks))
    todo.sort(key=lambda t: t[0])
    for depth, piece, ranks in todo:
        if not low <= depth < high:
            continue
        source, last, _ = piece.locate(me, ranks)
        landed = piece.dst_of(chunk, source)
        origin = piece.src_of(chunk) if depth == 0 else landed
        recv = recv_sem.at[chunk, piece.index, source]
        if depth > 0 and mode == "start":
            pltpu.make_async_copy(landed, landed, recv).wait()
        base = piece.first_send[ranks]
        for offset, (ok, target) in enumerate(piece.sends(me, ranks)):
            copy = pltpu.make_async_remote_copy(
                src_ref=origin,
                dst_ref=landed,
                send_sem=send_sem.at[chunk, base + offset],
                recv_sem=recv,
                device_id={"fs": target},
                device_id_type=MESH,
            )
            when(ok, copy.start if mode == "start" else copy.wait_send)


def number_sends(pieces):
    total = 0
    for piece in pieces:
        piece.first_send = {}
        for ranks in piece.slots:
            piece.first_send[ranks] = total
            last = max([i for i, r in enumerate(ranks) if r > 0], default=-1)
            for place, d in enumerate(piece.order):
                size = piece.dims[d][0]
                if place == last:
                    total += 1 if size > 2 else 0
                elif place > last:
                    total += 1 if size == 2 else 2
    return total


def cut(extent, unit, share):
    return max(unit, min(extent - unit, round(extent * share / unit) * unit))


def gather_plan(dims, refs, outs, blocks):
    gate, up, down, mix_in, mix_out = refs
    gate_o, up_o, down_o, mix_in_o, mix_out_o = outs
    n = len(dims)
    first = tuple(range(n))
    second = first[1:] + first[:1]
    third = first[-1:] + first[:-1]
    pooled = mix_out.shape[0]

    def rows(ref, out, start_of, size):
        return (
            lambda c: ref.at[pl.ds(start_of(c), size), :],
            lambda c, s: out.at[s, pl.ds(start_of(c), size), :],
        )

    def at(block, offset):
        return lambda c: pl.multiple_of(c * block + offset, 16)

    block, tall = gate.shape[0] // blocks, down.shape[0] // blocks
    down_cut = cut(tall, 16, 2 / 3)
    main = [
        Piece(0, dims, first, *rows(gate, gate_o, at(block, 0), block)),
        Piece(1, dims, third, *rows(up, up_o, at(block, 0), block)),
        Piece(2, dims, first, *rows(down, down_o, at(tall, 0), down_cut)),
        Piece(3, dims, second, *rows(down, down_o, at(tall, down_cut), tall - down_cut)),
    ]
    mix_cut = cut(pooled, 16, 2 / 3)

    def fixed(offset):
        return lambda c: offset

    mix = [
        Piece(0, dims, first, *rows(mix_in, mix_in_o, fixed(0), mix_in.shape[0])),
        Piece(1, dims, third, *rows(mix_out, mix_out_o, fixed(0), mix_cut)),
        Piece(2, dims, second, *rows(mix_out, mix_out_o, fixed(mix_cut), pooled - mix_cut)),
    ]
    return main, mix


def gather_kernel(dims, blocks, *args):
    refs, outs = args[:5], args[5:10]
    beside = None
    if len(args) > 13:
        beside = args[10:12]
        args = args[:10] + args[12:]
    send_sem, recv_sem, local_sem = args[10:13]
    me = lax.axis_index("fs")
    barrier = pltpu.get_barrier_semaphore()
    expected = 0
    for size, stride in dims:
        position = (me // stride) % size
        for step, ok in ((1, position + 1 < size), (-1, position > 0)):
            def signal(step=step, stride=stride):
                pl.semaphore_signal(
                    barrier, inc=1, device_id={"fs": me + step * stride}, device_id_type=MESH
                )

            pl.when(ok)(signal)
            expected = expected + jnp.where(ok, 1, 0)
    pl.semaphore_wait(barrier, expected)

    main, mix = gather_plan(dims, refs, outs, blocks)
    number_sends(main)
    number_sends(mix)
    deepest = sum(size - 1 for size, _ in dims) + 1
    early = min(3, deepest)

    locals_ = []
    for i, (ref, out) in enumerate(zip(refs, outs)):
        if beside is not None and i in (2, 4):
            continue
        locals_.append(pltpu.make_async_copy(ref, out.at[me], local_sem.at[i]))

    go = functools.partial(spread, send_sem=send_sem, recv_sem=recv_sem)
    def shard_in(source, stage, sem, shard, across):
        return pltpu.make_async_copy(
            source, stage.at[:, pl.ds(shard * across, across)], sem.at[shard]
        )

    def lay_in(own, part, stage, sem, rows, height):
        for shard in range(part.shape[0]):
            for mine, source in ((True, own), (False, part.at[shard])):

                @pl.when((me == shard) if mine else (me != shard))
                def _(source=source, shard=shard):
                    piece = source.at[pl.ds(rows, height), :]
                    shard_in(piece, stage, sem, shard, part.shape[2]).start()

    def lay_out(part, whole, stage, sem, rows, height, mode):
        if mode == "start":
            for shard in range(part.shape[0]):
                piece = part.at[shard, pl.ds(rows, height), :]
                shard_in(piece, stage, sem, shard, part.shape[2]).wait()
        copy = pltpu.make_async_copy(
            stage, whole.at[pl.ds(rows, height), :], sem.at[part.shape[0]]
        )
        copy.start() if mode == "start" else copy.wait()

    if beside is not None:
        down_stage, mix_stage, down_sem, mix_sem = args[13:]
        tall = down_stage.shape[1]

        pooled = mix_stage.shape[0]

    def rows_of(c):
        return c * tall if isinstance(c, int) else pl.multiple_of(c * tall, 16)

    def down_in(c):
        slot = c % 2
        lay_in(refs[2], outs[2], down_stage.at[slot], down_sem.at[slot], rows_of(c), tall)

    def down_out(c, mode="start"):
        slot = c % 2
        lay_out(outs[2], beside[0], down_stage.at[slot], down_sem.at[slot], rows_of(c), tall, mode)

    go(mix, me, blocks, low=0, high=1, mode="start")
    go(main, me, 0, low=0, high=1, mode="start")
    for copy in locals_:
        copy.start()
    go(mix, me, blocks, low=1, high=deepest, mode="start")
    if beside is not None:
        lay_in(refs[4], outs[4], mix_stage, mix_sem, 0, pooled)

    def step(i, carry):
        @pl.when(i + 1 < blocks)
        def _():
            go(main, me, i + 1, low=0, high=1, mode="start")

        go(main, me, i, low=1, high=early, mode="start")

        @pl.when(i > 0)
        def _():
            go(main, me, i - 1, low=early, high=deepest, mode="start")

        if beside is not None:

            @pl.when(i > 2)
            def _():
                down_out(i - 3, "end")

            @pl.when(i > 0)
            def _():
                down_in(i - 1)

            @pl.when(i > 1)
            def _():
                down_out(i - 2)

        return carry

    lax.fori_loop(0, blocks, step, 0)
    go(main, me, blocks - 1, low=early, high=deepest, mode="start")
    if beside is not None:
        if blocks > 2:
            down_out(blocks - 3, "end")
        down_in(blocks - 1)
        if blocks > 1:
            down_out(blocks - 2)
        lay_out(outs[4], beside[1], mix_stage, mix_sem, 0, pooled, "start")
        down_out(blocks - 1)

    def finish(i, carry):
        go(main, me, i, low=0, high=deepest, mode="end")
        return carry

    lax.fori_loop(0, blocks, finish, 0)
    go(mix, me, blocks, low=0, high=deepest, mode="end")
    if beside is not None:
        if blocks > 1:
            down_out(blocks - 2, "end")
        down_out(blocks - 1, "end")
        lay_out(outs[4], beside[1], mix_stage, mix_sem, 0, pooled, "end")
    for copy in locals_:
        copy.wait()


def gather_weights(dims, w_gate, w_up, w_down, w_mix_in, w_mix_out):
    count = 1
    for size, _ in dims:
        count *= size
    tiles = (w_gate.shape[0] // 16, w_down.shape[0] // 16)
    blocks = next(b for b in (8, 4, 2, 1) if tiles[0] % b == 0 and tiles[1] % b == 0)
    weights = (w_gate, w_up, w_down, w_mix_in, w_mix_out)
    shapes = [jax.ShapeDtypeStruct((count, *a.shape), a.dtype) for a in weights]

    class Shape:
        def __init__(self, shape):
            self.shape = shape

    stand_in = [Shape(a.shape) for a in weights]
    main, mix = gather_plan(dims, stand_in, [Shape(s.shape) for s in shapes], blocks)
    sends = max(number_sends(main), number_sends(mix))
    scratch = [
        pltpu.SemaphoreType.DMA((blocks + 1, sends)),
        pltpu.SemaphoreType.DMA((blocks + 1, len(main), count)),
        pltpu.SemaphoreType.DMA((5,)),
    ]
    laid = w_down.shape[1] % 128 == 0
    if laid:
        tall, full = w_down.shape[0] // blocks, w_down.shape[1] * count
        shapes += [jax.ShapeDtypeStruct((a.shape[0], full), a.dtype) for a in (w_down, w_mix_out)]
        scratch += [
            pltpu.VMEM((2, tall, full), w_down.dtype),
            pltpu.VMEM((w_mix_out.shape[0], full), w_mix_out.dtype),
            pltpu.SemaphoreType.DMA((2, count + 1)),
            pltpu.SemaphoreType.DMA((count + 1,)),
        ]
    outs = pl.pallas_call(
        functools.partial(gather_kernel, dims, blocks),
        out_shape=shapes,
        in_specs=[pl.BlockSpec(memory_space=pltpu.HBM)] * 5,
        out_specs=[pl.BlockSpec(memory_space=pltpu.HBM)] * len(shapes),
        scratch_shapes=scratch,
        compiler_params=pltpu.CompilerParams(collective_id=0, has_side_effects=True),
        name="gather_weights",
    )(*weights)

    def stacked(a):
        return a.reshape(-1, a.shape[2])

    def beside(a):
        return jnp.transpose(a, (1, 0, 2)).reshape(a.shape[1], -1)

    gate, up, down, mix_in, mix_out = outs[:5]
    if laid:
        return stacked(gate), stacked(up), outs[5], stacked(mix_in), outs[6]
    return stacked(gate), stacked(up), beside(down), stacked(mix_in), beside(mix_out)


def rms_scale(values, gain):
    return values * lax.rsqrt(jnp.mean(values * values, axis=-1, keepdims=True) + 1e-06) * gain


def total_over_tp(left_rows, right_matrix):
    part = jnp.dot(left_rows, right_matrix, preferred_element_type=jnp.float32)
    part = part.astype(jnp.bfloat16)
    if lax.axis_size("tp") == 2:
        other = lax.ppermute(part, "tp", ((0, 1), (1, 0)))
        return part.astype(jnp.float32) + other.astype(jnp.float32)
    return lax.psum(part.astype(jnp.float32), "tp")


def own_total_over_tp(left_rows, right_matrix):
    part = jnp.dot(left_rows, right_matrix, preferred_element_type=jnp.float32)
    part = part.astype(jnp.bfloat16)
    if lax.axis_size("tp") == 2:
        mine = own_rows_of(part)
        half = mine.shape[0]
        theirs = lax.dynamic_slice_in_dim(part, (1 - lax.axis_index("tp")) * half, half, 0)
        other = lax.ppermute(theirs, "tp", ((0, 1), (1, 0)))
        return mine.astype(jnp.float32) + other.astype(jnp.float32)
    return lax.psum_scatter(part.astype(jnp.float32), "tp", scatter_dimension=0, tiled=True)


def own_rows_of(array):
    count = array.shape[0] // lax.axis_size("tp")
    return lax.dynamic_slice_in_dim(array, lax.axis_index("tp") * count, count, 0)


def body(dims, tokens, w_gate, w_up, w_down, w_mix_in, w_mix_out, pool_w, pool_scale, norm_gains):
    rows_all = tokens.shape[0]
    stream = tokens.astype(jnp.float32)
    normed = rms_scale(stream, norm_gains[0]).astype(jnp.bfloat16)
    gate_full, up_full, down_full, mix_in_full, mix_out_full = gather_weights(
        dims, w_gate, w_up, w_down, w_mix_in, w_mix_out
    )
    gate_first = jnp.dot(normed, gate_full, preferred_element_type=jnp.float32)
    up_first = jnp.dot(normed, up_full, preferred_element_type=jnp.float32)
    hidden = (jax.nn.silu(gate_first) * up_first).astype(jnp.bfloat16)
    stream = stream + 0.5 * rms_scale(total_over_tp(hidden, down_full), norm_gains[1])
    normed = rms_scale(stream, norm_gains[2]).astype(jnp.bfloat16)
    pooled_in = jnp.dot(normed, mix_in_full, preferred_element_type=jnp.float32)
    pooled_in = pooled_in.astype(jnp.bfloat16)
    groups_here = pool_w.shape[0]
    group_dim = pool_w.shape[1]
    values = pooled_in.astype(jnp.float32).reshape(rows_all // LEN, LEN, groups_here, group_dim)
    totals = jnp.cumsum(values, axis=1)
    position = jnp.arange(1, LEN + 1).astype(jnp.float32)[None, :, None, None]
    window_ids = (lax.axis_index("tp") * groups_here + jnp.arange(groups_here)) % 4
    average = jnp.zeros_like(values)
    for window_slot in range(4):
        window = 2 ** (1 + window_slot)
        lagged = jnp.pad(totals, ((0, 0), (window, 0), (0, 0), (0, 0)))[:, :LEN]
        candidate = (totals - lagged) / jnp.minimum(position, float(window))
        average = jnp.where((window_ids == window_slot)[None, None, :, None], candidate, average)
    deviation = (average - values).astype(jnp.bfloat16)
    regrouped = jnp.einsum("btgi,gio->btgo", deviation, pool_w, preferred_element_type=jnp.float32)
    regrouped = (
        regrouped.reshape(rows_all, groups_here * group_dim) * pool_scale.astype(jnp.float32)
    ).astype(jnp.bfloat16)
    stream = stream + rms_scale(total_over_tp(regrouped, mix_out_full), norm_gains[3])
    normed = rms_scale(stream, norm_gains[4]).astype(jnp.bfloat16)
    gate_second = jnp.dot(normed, gate_full, preferred_element_type=jnp.float32)
    up_second = jnp.dot(normed, up_full, preferred_element_type=jnp.float32)
    hidden = (jax.nn.silu(gate_second) * up_second).astype(jnp.bfloat16)
    stream_own = own_rows_of(stream)
    stream_own = stream_own + 0.5 * rms_scale(own_total_over_tp(hidden, down_full), norm_gains[5])
    return stream_own.astype(jnp.bfloat16)


def silu(v):
    return v / (1.0 + jnp.exp(-v))


def rms_value(values, gain):
    return values * lax.rsqrt(jnp.mean(values * values, axis=-1, keepdims=True) + 1e-06) * gain


class Sends:
    def __init__(self, sem):
        self.sem, self.count, self.pending = sem, 0, []

    def put(self, src, dst, recv, to, ok=None):
        copy = pltpu.make_async_remote_copy(
            src_ref=src,
            dst_ref=dst,
            send_sem=self.sem.at[self.count],
            recv_sem=recv,
            device_id=to,
            device_id_type=MESH,
        )
        self.count += 1
        when(ok, copy.start)
        self.pending.append((ok, copy))

    def drain(self):
        for ok, copy in self.pending:
            when(ok, copy.wait_send)
        self.pending = []


SENDS = 192
F32, BF16 = jnp.float32, jnp.bfloat16


def layer_kernel(dims, *refs):
    (tokens, gate, up, down, mix_in, mix_out, pool_w, pool_scale, gains, out) = refs[:10]
    (gate_v, up_v, down_v, min_v, mout_v) = refs[10:15]
    (tok_v, norm_v, own_v, far_v, hid_v, part_v, part2_v, partm_v) = refs[15:23]
    (got1, got2o, got2f, gotm, sum1, sum2, far1, far2) = refs[23:31]
    (stream_v, mid_v, pin_v, rg_v, out_v) = refs[31:36]
    (send_sem, ff_sem, mix_sem, act_sem, local_sem, loc_ff) = refs[36:]
    (nz, sz), (_, sy), (_, sx) = dims
    me, core = lax.axis_index("fs"), lax.axis_index("tp")
    z = me // sz
    col = me - z * sz
    xn = me + (1 - 2 * ((me // sx) % 2)) * sx
    yn = me + (1 - 2 * ((me // sy) % 2)) * sy
    dg = xn + yn - me
    sign = 1 - 2 * (z % 2)
    peer = me + sign * sz
    depth = gate.shape[0]
    hid = gate_v.shape[1]
    rows = tokens.shape[0]
    half = rows // 2
    wide = down.shape[1]
    feat = tokens.shape[1]
    span = sz * wide

    barrier = pltpu.get_barrier_semaphore()
    friends = [({"fs": xn}), ({"fs": yn}), ({"tp": 1 - core})]
    for k in range(1, nz):
        friends.append({"fs": lax.rem(z + k, nz) * sz + col})
    for to in friends:
        pl.semaphore_signal(barrier, inc=1, device_id=to, device_id_type=MESH)
    pl.semaphore_wait(barrier, len(friends))

    sends = Sends(send_sem)

    def mo(v, n):
        return v if isinstance(v, int) else pl.multiple_of(v, n)

    def plane(p):
        return near(z, nz, p)[0] if p else z

    weights = ((gate, gate_v), (up, up_v), (down, down_v))

    def own_piece(m, h, u):
        ref = weights[m][0]
        if m < 2:
            return ref.at[pl.ds(u * (depth // 2), depth // 2), pl.ds(mo(h * hid, 128), hid)]
        return ref.at[pl.ds(mo(h * hid + u * (hid // 2), 16), hid // 2), :]

    def place(m, src, u):
        buf = weights[m][1]
        if m < 2:
            return buf.at[pl.ds(mo(src * depth + u * (depth // 2), 16), depth // 2), :]
        return buf.at[src, pl.ds(u * (hid // 2), hid // 2), :]

    def arrived(ref, sem):
        pltpu.make_async_copy(ref, ref, sem).wait()

    locals_ = {}

    def local(key, src, dst, sem):
        copy = pltpu.make_async_copy(src, dst, sem)
        copy.start()
        locals_[key] = copy

    steps = [(m, p) for m in range(4) for p in range(nz)]

    def pieces(m):
        return range(2) if m < 3 else range(1)

    def spot(m, src, u):
        return place(m, src, u) if m < 3 else mout_v.at[src]

    def sem_of(m, src, u):
        return ff_sem.at[m, src, u]

    def origin(m, h, u):
        return own_piece(m, h, u) if m < 3 else mix_out

    def stage0(n):
        m, p = steps[n]
        if p == 0:
            return
        t = plane(p)
        for u in pieces(m):
            sends.put(origin(m, t % 2, u), spot(m, me, u), sem_of(m, me, u), {"fs": t * sz + col})

    def stage1(n):
        m, p = steps[n]
        src = plane(p) * sz + col
        for u in pieces(m):
            if p:
                arrived(spot(m, src, u), sem_of(m, src, u))
            for nb in (xn, yn):
                first = spot(m, src, u) if p else origin(m, z % 2, u)
                sends.put(first, spot(m, src, u), sem_of(m, src, u), {"fs": nb})
            if not p:
                local((m, u), origin(m, z % 2, u), spot(m, me, u), loc_ff.at[m, u])

    def three(p):
        shift = plane(p) * sz - z * sz
        return xn + shift, yn + shift, dg + shift

    def relay(m, p, u, across):
        a, b, _ = three(p)
        src, to = (a, yn) if across else (b, xn)
        arrived(spot(m, src, u), sem_of(m, src, u))
        sends.put(spot(m, src, u), spot(m, src, u), sem_of(m, src, u), {"fs": to})

    def stage2(n):
        m, p = steps[n]
        if m < 3:
            relay(m, p, 0, True)
            relay(m, p, 1, False)
        else:
            relay(m, p, 0, p % 2 == 0)

    def stage3(n):
        m, p = steps[n]
        a, b, d = three(p)
        if m < 3:
            todo = [(a, 1), (b, 0), (d, 0), (d, 1)]
        else:
            todo = [(b if p % 2 == 0 else a, 0), (d, 0)]
        for src, u in todo:
            arrived(spot(m, src, u), sem_of(m, src, u))
        if p == 0:
            for u in pieces(m):
                locals_[(m, u)].wait()

    def min_at(src):
        return min_v.at[pl.ds(mo(src * depth, 16), depth), :]

    def mix_own():
        for nb in (xn, yn):
            sends.put(mix_in, min_at(me), mix_sem.at[me], {"fs": nb})
        local("mix", mix_in, min_at(me), local_sem.at[0])

    def mix_turn():
        arrived(min_at(xn), mix_sem.at[xn])
        sends.put(min_at(xn), min_at(xn), mix_sem.at[xn], {"fs": yn})

    def mix_up():
        arrived(min_at(yn), mix_sem.at[yn])
        arrived(min_at(dg), mix_sem.at[dg])
        locals_["mix"].wait()
        for src in (me, xn, yn, dg):
            for step in (1, -1):
                ok = jnp.logical_and(z + step >= 0, z + step < nz)
                sends.put(min_at(src), min_at(src), mix_sem.at[src], {"fs": me + step * sz}, ok)

    def mix_on(p, forward=True):
        found, away = near(z, nz, p)
        shift = (found - z) * sz
        inside = jnp.logical_and(z + away >= 0, z + away < nz)
        for src in (me + shift, xn + shift, yn + shift, dg + shift):
            here, sem = min_at(src), mix_sem.at[src]
            if forward:
                when(inside, functools.partial(arrived, here, sem))
                sends.put(here, here, sem, {"fs": me + away * sz}, inside)
            else:
                when(jnp.logical_not(inside), functools.partial(arrived, here, sem))

    mine = pl.ds(mo(core * half, 16), half)
    theirs = pl.ds(mo((1 - core) * half, 16), half)
    mine_far = pl.ds(mo(rows + core * half, 16), half)
    theirs_far = pl.ds(mo(rows + (1 - core) * half, 16), half)
    partner = {"tp": 1 - core}
    buddy = {"fs": peer}

    def tokens_out():
        sends.put(tokens.at[mine, :], tok_v.at[mine_far, :], act_sem.at[0], buddy)
        local("tok", tokens, tok_v.at[pl.ds(0, rows), :], local_sem.at[1])

    def tokens_on():
        here = tok_v.at[mine_far, :]
        arrived(here, act_sem.at[0])
        sends.put(here, here, act_sem.at[1], partner)

    def first_norm():
        arrived(tok_v.at[theirs_far, :], act_sem.at[1])
        locals_["tok"].wait()

        def block(i, carry):
            at = pl.ds(pl.multiple_of(i * 32, 32), 32)
            v = tok_v[at, :].astype(F32)
            norm_v[at, :] = rms_value(v, gains[0:1, :]).astype(BF16)
            return carry

        lax.fori_loop(0, 2 * rows // 32, block, 0)

    def gate_up(src, at, dst):
        def tile(cols, n):
            w = jnp.concatenate([gate_v[:, cols], up_v[:, cols]], axis=1)
            both = jnp.dot(src[at, :], w, preferred_element_type=F32)
            hid_v[dst, cols] = (silu(both[:, :n]) * both[:, n:]).astype(BF16)

        whole = hid // 256

        def body(j, carry):
            tile(pl.ds(pl.multiple_of(j * 256, 256), 256), 256)
            return carry

        lax.fori_loop(0, whole, body, 0)
        if hid % 256:
            tile(pl.ds(whole * 256, hid % 256), hid % 256)

    def down_block(t, at):
        w = jnp.concatenate([down_v[t * sz + i] for i in range(sz)], axis=1)
        return jnp.dot(hid_v[at, :], w, preferred_element_type=F32).astype(BF16)

    def cols_of(t):
        return pl.ds(mo(t * span, 128), span)

    def down1(p):
        t = plane(p)
        cols = cols_of(t)
        for i, (base, other) in enumerate(((rows, theirs_far), (0, theirs))):
            at = pl.ds(base, rows)
            part_v[at, cols] = down_block(t, at)
            sends.put(part_v.at[other, cols], got1.at[1 - i, :, cols], act_sem.at[8 + 2 * p + i], partner)

    def reduce1(p):
        cols = cols_of(plane(p))
        for i in range(2):
            arrived(got1.at[1 - i, :, cols], act_sem.at[8 + 2 * p + i])
        total = part_v[mine_far, cols].astype(F32) + got1[1, :, cols].astype(F32)
        sum1[:, cols] = total.astype(BF16)
        sends.put(sum1.at[:, cols], far1.at[:, cols], act_sem.at[16 + plane(p)], buddy)

    def first_stream():
        for t in range(nz):
            cols = cols_of(t)
            arrived(far1.at[:, cols], act_sem.at[16 + t])

        def block(i, carry):
            r = pl.ds(pl.multiple_of(i * 16, 16), 16)
            at = pl.ds(pl.multiple_of(core * half + i * 16, 16), 16)
            y = part_v[at, :].astype(F32) + got1[0, r, :].astype(F32) + far1[r, :].astype(F32)
            s = tok_v[at, :].astype(F32) + 0.5 * rms_value(y, gains[1:2, :])
            stream_v[r, :] = s
            mid_v[at, :] = rms_value(s, gains[2:3, :]).astype(BF16)
            return carry

        lax.fori_loop(0, half // 16, block, 0)
        sends.put(mid_v.at[mine, :], mid_v.at[mine, :], act_sem.at[2], partner)

    def into_pool(at):
        v = jnp.dot(mid_v[at, :], min_v[...], preferred_element_type=F32)
        pin_v[at, :] = v.astype(BF16).astype(F32)

    def pool():
        length = LEN
        groups, dim = pool_w.shape[0], pool_w.shape[1]
        t = lax.broadcasted_iota(jnp.int32, (rows, dim), 0) % length
        for g in range(groups):
            cols = slice(g * dim, (g + 1) * dim)
            v = pin_v[:, cols]
            window = 2 ** (1 + g % 4)
            total, k = v, 1
            while k < window:
                total = total + jnp.where(t >= k, pltpu.roll(total, k, 0), 0.0)
                k *= 2
            count = jnp.minimum(t + 1, window).astype(F32)
            dev = (total / count - v).astype(BF16)
            o = jnp.dot(dev, pool_w[g], preferred_element_type=F32) * pool_scale[:, cols]
            rg_v[:, cols] = o.astype(BF16)

    def out_pool(at):
        for t in range(nz):
            w = jnp.concatenate([mout_v[t * sz + i] for i in range(sz)], axis=1)
            v = jnp.dot(rg_v[at, :], w, preferred_element_type=F32)
            partm_v[at, pl.ds(t * span, span)] = v.astype(BF16)

    quarter = half // 2

    def second_stream():
        arrived(gotm, act_sem.at[3])

        def block(i, carry):
            r = pl.ds(pl.multiple_of(i * 16, 16), 16)
            at = pl.ds(pl.multiple_of(core * half + i * 16, 16), 16)
            y = partm_v[at, :].astype(F32) + gotm[r, :].astype(F32)
            s = stream_v[r, :] + rms_value(y, gains[3:4, :])
            stream_v[r, :] = s
            own_v[at, :] = rms_value(s, gains[4:5, :]).astype(BF16)
            return carry

        for k in range(2):
            lax.fori_loop(k * quarter // 16, (k + 1) * quarter // 16, block, 0)
            src = own_v.at[pl.ds(mo(core * half + k * quarter, 16), quarter), :]
            sends.put(src, far_at(k, core), act_sem.at[4 + k], buddy)
        sends.put(own_v.at[mine, :], own_v.at[mine, :], act_sem.at[6], partner)

    def far_at(k, c):
        return far_v.at[pl.ds(mo((2 * k + c) * quarter, 16), quarter), :]

    def far_on(k):
        arrived(far_at(k, core), act_sem.at[4 + k])
        sends.put(far_at(k, core), far_at(k, core), act_sem.at[20 + k], partner)

    def down2(dst, base, count):
        at = pl.ds(base, count)

        def body(t, carry):
            part2_v[at, pl.ds(pl.multiple_of(t * span, 128), span)] = down_block(t, at)
            return carry

        lax.fori_loop(0, nz, body, 0)

    def far_part(k, c):
        return pl.ds(mo(rows + (2 * k + c) * quarter, 16), quarter)

    last = len(steps)
    stage1(0)
    for n in (1, 2, 3):
        stage0(n)
    mix_own()
    tokens_out()
    stage0(5)
    stage1(1)
    stage2(0)
    mix_turn()
    all_mine = pl.ds(0, rows)
    all_far = pl.ds(rows, rows)

    def advance(i):
        if i + 6 < last:
            stage0(i + 6)
        if i + 2 < last:
            stage1(i + 2)
        if i + 1 < last:
            stage2(i + 1)
        stage3(i)

    for i in range(3 * nz):
        advance(i)
        if i == 2:
            tokens_on()
        if i == 4:
            first_norm()
        if i == nz + 1:
            mix_up()
        if i == 2 * nz - 1:
            gate_up(norm_v, all_mine, all_mine)
        if i == 2 * nz:
            gate_up(norm_v, all_far, all_far)
        if i == 2 * nz + 1:
            down1(0)
            down1(1)
            mix_on(1)
        if 2 * nz + 1 < i:
            down1(i - 2 * nz)
            if i == 2 * nz + 2:
                reduce1(0)
                mix_on(2)
            reduce1(i - 2 * nz - 1)
    for p in range(3, nz):
        mix_on(p)
    advance(3 * nz)
    reduce1(nz - 1)
    for i in range(3 * nz + 1, last - 1):
        advance(i)
    first_stream()
    for p in range(1, nz):
        mix_on(p, forward=False)
    into_pool(mine)
    arrived(mid_v.at[theirs, :], act_sem.at[2])
    into_pool(theirs)
    pool()
    advance(last - 1)
    out_pool(theirs)
    sends.put(partm_v.at[theirs, :], gotm, act_sem.at[3], partner)
    out_pool(mine)
    second_stream()

    arrived(own_v.at[theirs, :], act_sem.at[6])
    gate_up(own_v, all_mine, all_mine)
    down2(own_v, 0, rows)
    sends.put(part2_v.at[theirs, :], got2o, act_sem.at[7], partner)
    for k in range(2):
        far_on(k)
        arrived(far_at(k, 1 - core), act_sem.at[20 + k])
        base = 2 * k * quarter
        gate_up(far_v, pl.ds(base, 2 * quarter), pl.ds(rows + base, 2 * quarter))
        down2(far_v, rows + base, 2 * quarter)
        sends.put(part2_v.at[far_part(k, 1 - core), :], got2f.at[k], act_sem.at[22 + k], partner)
        arrived(got2f.at[k], act_sem.at[22 + k])
        total = part2_v[far_part(k, core), :].astype(F32) + got2f[k].astype(F32)
        sum2[k] = total.astype(BF16)
        there = far2.at[pl.ds(k * quarter, quarter), :]
        sends.put(sum2.at[k], there, act_sem.at[24 + k], buddy)
    arrived(got2o, act_sem.at[7])

    def last_block(i, carry):
        r = pl.ds(pl.multiple_of(i * 16, 16), 16)
        at = pl.ds(pl.multiple_of(core * half + i * 16, 16), 16)
        y = part2_v[at, :].astype(F32) + got2o[r, :].astype(F32) + far2[r, :].astype(F32)
        s = stream_v[r, :] + 0.5 * rms_value(y, gains[5:6, :])
        out_v[r, :] = s.astype(BF16)
        return carry

    for k in range(2):
        arrived(far2.at[pl.ds(k * quarter, quarter), :], act_sem.at[24 + k])
        lax.fori_loop(k * quarter // 16, (k + 1) * quarter // 16, last_block, 0)
    final = pltpu.make_async_copy(out_v, out, local_sem.at[2])
    final.start()
    sends.drain()
    final.wait()


def whole_layer(dims, tokens, w_gate, w_up, w_down, w_mix_in, w_mix_out, pool_w, pool_scale, gains):
    count = 1
    for size, _ in dims:
        count *= size
    nz = dims[0][0]
    depth, units = w_gate.shape
    hid = units // 2
    rows, feat = tokens.shape
    half = rows // 2
    wide = w_down.shape[1]
    pooled = w_mix_in.shape[1]
    scale = pool_scale.astype(F32).reshape(1, -1)

    def buf(*shape, dtype=BF16):
        return pltpu.VMEM(shape, dtype)

    scratch = [
        buf(count * depth, hid),
        buf(count * depth, hid),
        buf(count, hid, wide),
        buf(count * depth, pooled),
        buf(count, w_mix_out.shape[0], wide),
        buf(2 * rows, feat),
        buf(2 * rows, feat),
        buf(rows, feat),
        buf(rows, feat),
        buf(2 * rows, hid),
        buf(2 * rows, feat),
        buf(2 * rows, feat),
        buf(rows, feat),
        buf(2, half, feat),
        buf(half, feat),
        buf(2, half // 2, feat),
        buf(half, feat),
        buf(half, feat),
        buf(2, half // 2, feat),
        buf(half, feat),
        buf(half, feat),
        buf(half, feat, dtype=F32),
        buf(rows, feat),
        buf(rows, pooled, dtype=F32),
        buf(rows, pooled),
        buf(half, feat),
        pltpu.SemaphoreType.DMA((SENDS,)),
        pltpu.SemaphoreType.DMA((4, count, 2)),
        pltpu.SemaphoreType.DMA((count,)),
        pltpu.SemaphoreType.DMA((32,)),
        pltpu.SemaphoreType.DMA((4,)),
        pltpu.SemaphoreType.DMA((4, 2)),
    ]
    hbm = pl.BlockSpec(memory_space=pltpu.HBM)
    vmem = pl.BlockSpec(memory_space=pltpu.VMEM)
    return pl.pallas_call(
        functools.partial(layer_kernel, dims),
        out_shape=jax.ShapeDtypeStruct((half, feat), tokens.dtype),
        in_specs=[hbm] * 6 + [vmem] * 3,
        out_specs=hbm,
        scratch_shapes=scratch,
        compiler_params=pltpu.CompilerParams(
            collective_id=1, has_side_effects=True, vmem_limit_bytes=67043328
        ),
        name="whole_layer",
    )(tokens, w_gate, w_up, w_down, w_mix_in, w_mix_out, pool_w, scale, gains)


def paired(dims, mesh):
    return (
        len(dims) == 3
        and dims[0][0] == 4
        and dims[1][0] == 2
        and dims[2][0] == 2
        and mesh.shape["tp"] == 2
    )


def solution(mesh):
    in_specs = (
        P("fs", None),
        P("fs", "tp"),
        P("fs", "tp"),
        P("tp", "fs"),
        P("fs", "tp"),
        P("tp", "fs"),
        P("tp", None, None),
        P("tp"),
        P(),
    )
    out_specs = P(("fs", "tp"), None)
    dims = line_dims(mesh)
    act = whole_layer if paired(dims, mesh) else body
    return jax.shard_map(
        functools.partial(act, dims), mesh=mesh, in_specs=in_specs, out_specs=out_specs, check_vma=False
    )
```

```python
import functools
import itertools

import jax
import jax.numpy as jnp
from jax import lax
from jax.experimental import pallas as pl
from jax.experimental.pallas import tpu as pltpu
from jax.sharding import PartitionSpec as P

LEN = 64
MESH = pl.DeviceIdType.MESH


def line_dims(mesh):
    devices = mesh.devices.reshape(mesh.shape["fs"], -1)[:, 0]
    count = len(devices)
    coords = [tuple(getattr(d, "coords", ())) for d in devices]
    dims = []
    for axis in range(len(coords[0])):
        values = sorted({c[axis] for c in coords})
        if len(values) > 1:
            stride = next(i for i in range(count) if coords[i][axis] != coords[0][axis])
            dims.append((len(values), stride, axis, values))
    dims.sort(key=lambda d: -d[1])
    good = len(dims) > 0 and all(
        sum(vals.index(c[axis]) * stride for _, stride, axis, vals in dims) == i
        for i, c in enumerate(coords)
    )
    if not good:
        return ((count, 1),)
    return tuple((d[0], d[1]) for d in dims)


def near(position, size, rank):
    inner = jnp.minimum(position, size - 1 - position)
    alternating = rank <= 2 * inner
    distance = jnp.where(alternating, (rank + 1) // 2, rank - inner)
    toward_high = jnp.where(alternating, rank % 2 == 1, 2 * position < size - 1)
    step = jnp.where(toward_high, 1, -1)
    return position + step * distance, -step


def piece_plan(dims, order):
    sizes = [dims[d][0] for d in order]
    slots = []
    for ranks in itertools.product(*[range(n) for n in sizes]):
        slots.append(ranks)
    slots.sort(key=lambda r: (sum(r), r))
    return slots


class Piece:
    def __init__(self, index, dims, order, src_of, dst_of):
        self.index, self.dims, self.order = index, dims, order
        self.src_of, self.dst_of = src_of, dst_of
        self.slots = piece_plan(dims, order)

    def locate(self, me, ranks):
        source, last, away = me, -1, None
        for place, (d, rank) in enumerate(zip(self.order, ranks)):
            if rank > 0:
                size, stride = self.dims[d]
                position = (me // stride) % size
                found, step = near(position, size, rank)
                source = source + (found - position) * stride
                last, away = place, step
        return source, last, away

    def sends(self, me, ranks):
        _, last, away = self.locate(me, ranks)
        out = []
        for place, d in enumerate(self.order):
            size, stride = self.dims[d]
            position = (me // stride) % size
            if place == last:
                if size > 2:
                    ok = jnp.logical_and(position + away >= 0, position + away < size)
                    out.append((ok, me + away * stride))
            elif place > last:
                if size == 2:
                    out.append((None, me + (1 - 2 * position) * stride))
                else:
                    out.append((position + 1 < size, me + stride))
                    out.append((position > 0, me - stride))
        return out


def when(condition, act):
    if condition is None:
        act()
    else:
        pl.when(condition)(act)


def spread(pieces, me, chunk, send_sem, recv_sem, low, high, mode):
    todo = []
    for piece in pieces:
        for ranks in piece.slots:
            todo.append((sum(ranks), piece, ranks))
    todo.sort(key=lambda t: t[0])
    for depth, piece, ranks in todo:
        if not low <= depth < high:
            continue
        source, last, _ = piece.locate(me, ranks)
        landed = piece.dst_of(chunk, source)
        origin = piece.src_of(chunk) if depth == 0 else landed
        recv = recv_sem.at[chunk, piece.index, source]
        if depth > 0 and mode == "start":
            pltpu.make_async_copy(landed, landed, recv).wait()
        base = piece.first_send[ranks]
        for offset, (ok, target) in enumerate(piece.sends(me, ranks)):
            copy = pltpu.make_async_remote_copy(
                src_ref=origin,
                dst_ref=landed,
                send_sem=send_sem.at[chunk, base + offset],
                recv_sem=recv,
                device_id={"fs": target},
                device_id_type=MESH,
            )
            when(ok, copy.start if mode == "start" else copy.wait_send)


def number_sends(pieces):
    total = 0
    for piece in pieces:
        piece.first_send = {}
        for ranks in piece.slots:
            piece.first_send[ranks] = total
            last = max([i for i, r in enumerate(ranks) if r > 0], default=-1)
            for place, d in enumerate(piece.order):
                size = piece.dims[d][0]
                if place == last:
                    total += 1 if size > 2 else 0
                elif place > last:
                    total += 1 if size == 2 else 2
    return total


def cut(extent, unit, share):
    return max(unit, min(extent - unit, round(extent * share / unit) * unit))


def gather_plan(dims, refs, outs, blocks):
    gate, up, down, mix_in, mix_out = refs
    gate_o, up_o, down_o, mix_in_o, mix_out_o = outs
    n = len(dims)
    first = tuple(range(n))
    second = first[1:] + first[:1]
    third = first[-1:] + first[:-1]
    pooled = mix_out.shape[0]

    def rows(ref, out, start_of, size):
        return (
            lambda c: ref.at[pl.ds(start_of(c), size), :],
            lambda c, s: out.at[s, pl.ds(start_of(c), size), :],
        )

    def at(block, offset):
        return lambda c: pl.multiple_of(c * block + offset, 16)

    block, tall = gate.shape[0] // blocks, down.shape[0] // blocks
    down_cut = cut(tall, 16, 2 / 3)
    main = [
        Piece(0, dims, first, *rows(gate, gate_o, at(block, 0), block)),
        Piece(1, dims, third, *rows(up, up_o, at(block, 0), block)),
        Piece(2, dims, first, *rows(down, down_o, at(tall, 0), down_cut)),
        Piece(3, dims, second, *rows(down, down_o, at(tall, down_cut), tall - down_cut)),
    ]
    mix_cut = cut(pooled, 16, 2 / 3)

    def fixed(offset):
        return lambda c: offset

    mix = [
        Piece(0, dims, first, *rows(mix_in, mix_in_o, fixed(0), mix_in.shape[0])),
        Piece(1, dims, third, *rows(mix_out, mix_out_o, fixed(0), mix_cut)),
        Piece(2, dims, second, *rows(mix_out, mix_out_o, fixed(mix_cut), pooled - mix_cut)),
    ]
    return main, mix


def gather_kernel(dims, blocks, *args):
    refs, outs = args[:5], args[5:10]
    beside = None
    if len(args) > 13:
        beside = args[10:12]
        args = args[:10] + args[12:]
    send_sem, recv_sem, local_sem = args[10:13]
    me = lax.axis_index("fs")
    barrier = pltpu.get_barrier_semaphore()
    expected = 0
    for size, stride in dims:
        position = (me // stride) % size
        for step, ok in ((1, position + 1 < size), (-1, position > 0)):
            def signal(step=step, stride=stride):
                pl.semaphore_signal(
                    barrier, inc=1, device_id={"fs": me + step * stride}, device_id_type=MESH
                )

            pl.when(ok)(signal)
            expected = expected + jnp.where(ok, 1, 0)
    pl.semaphore_wait(barrier, expected)

    main, mix = gather_plan(dims, refs, outs, blocks)
    number_sends(main)
    number_sends(mix)
    deepest = sum(size - 1 for size, _ in dims) + 1
    early = min(3, deepest)

    locals_ = []
    for i, (ref, out) in enumerate(zip(refs, outs)):
        if beside is not None and i in (2, 4):
            continue
        locals_.append(pltpu.make_async_copy(ref, out.at[me], local_sem.at[i]))

    go = functools.partial(spread, send_sem=send_sem, recv_sem=recv_sem)
    def shard_in(source, stage, sem, shard, across):
        return pltpu.make_async_copy(
            source, stage.at[:, pl.ds(shard * across, across)], sem.at[shard]
        )

    def lay_in(own, part, stage, sem, rows, height):
        for shard in range(part.shape[0]):
            for mine, source in ((True, own), (False, part.at[shard])):

                @pl.when((me == shard) if mine else (me != shard))
                def _(source=source, shard=shard):
                    piece = source.at[pl.ds(rows, height), :]
                    shard_in(piece, stage, sem, shard, part.shape[2]).start()

    def lay_out(part, whole, stage, sem, rows, height, mode):
        if mode == "start":
            for shard in range(part.shape[0]):
                piece = part.at[shard, pl.ds(rows, height), :]
                shard_in(piece, stage, sem, shard, part.shape[2]).wait()
        copy = pltpu.make_async_copy(
            stage, whole.at[pl.ds(rows, height), :], sem.at[part.shape[0]]
        )
        copy.start() if mode == "start" else copy.wait()

    if beside is not None:
        down_stage, mix_stage, down_sem, mix_sem = args[13:]
        tall = down_stage.shape[1]

        pooled = mix_stage.shape[0]

    def rows_of(c):
        return c * tall if isinstance(c, int) else pl.multiple_of(c * tall, 16)

    def down_in(c):
        slot = c % 2
        lay_in(refs[2], outs[2], down_stage.at[slot], down_sem.at[slot], rows_of(c), tall)

    def down_out(c, mode="start"):
        slot = c % 2
        lay_out(outs[2], beside[0], down_stage.at[slot], down_sem.at[slot], rows_of(c), tall, mode)

    go(mix, me, blocks, low=0, high=1, mode="start")
    go(main, me, 0, low=0, high=1, mode="start")
    for copy in locals_:
        copy.start()
    go(mix, me, blocks, low=1, high=deepest, mode="start")
    if beside is not None:
        lay_in(refs[4], outs[4], mix_stage, mix_sem, 0, pooled)

    def step(i, carry):
        @pl.when(i + 1 < blocks)
        def _():
            go(main, me, i + 1, low=0, high=1, mode="start")

        go(main, me, i, low=1, high=early, mode="start")

        @pl.when(i > 0)
        def _():
            go(main, me, i - 1, low=early, high=deepest, mode="start")

        if beside is not None:

            @pl.when(i > 2)
            def _():
                down_out(i - 3, "end")

            @pl.when(i > 0)
            def _():
                down_in(i - 1)

            @pl.when(i > 1)
            def _():
                down_out(i - 2)

        return carry

    lax.fori_loop(0, blocks, step, 0)
    go(main, me, blocks - 1, low=early, high=deepest, mode="start")
    if beside is not None:
        if blocks > 2:
            down_out(blocks - 3, "end")
        down_in(blocks - 1)
        if blocks > 1:
            down_out(blocks - 2)
        lay_out(outs[4], beside[1], mix_stage, mix_sem, 0, pooled, "start")
        down_out(blocks - 1)

    def finish(i, carry):
        go(main, me, i, low=0, high=deepest, mode="end")
        return carry

    lax.fori_loop(0, blocks, finish, 0)
    go(mix, me, blocks, low=0, high=deepest, mode="end")
    if beside is not None:
        if blocks > 1:
            down_out(blocks - 2, "end")
        down_out(blocks - 1, "end")
        lay_out(outs[4], beside[1], mix_stage, mix_sem, 0, pooled, "end")
    for copy in locals_:
        copy.wait()


def gather_weights(dims, w_gate, w_up, w_down, w_mix_in, w_mix_out):
    count = 1
    for size, _ in dims:
        count *= size
    tiles = (w_gate.shape[0] // 16, w_down.shape[0] // 16)
    blocks = next(b for b in (8, 4, 2, 1) if tiles[0] % b == 0 and tiles[1] % b == 0)
    weights = (w_gate, w_up, w_down, w_mix_in, w_mix_out)
    shapes = [jax.ShapeDtypeStruct((count, *a.shape), a.dtype) for a in weights]

    class Shape:
        def __init__(self, shape):
            self.shape = shape

    stand_in = [Shape(a.shape) for a in weights]
    main, mix = gather_plan(dims, stand_in, [Shape(s.shape) for s in shapes], blocks)
    sends = max(number_sends(main), number_sends(mix))
    scratch = [
        pltpu.SemaphoreType.DMA((blocks + 1, sends)),
        pltpu.SemaphoreType.DMA((blocks + 1, len(main), count)),
        pltpu.SemaphoreType.DMA((5,)),
    ]
    laid = w_down.shape[1] % 128 == 0
    if laid:
        tall, full = w_down.shape[0] // blocks, w_down.shape[1] * count
        shapes += [jax.ShapeDtypeStruct((a.shape[0], full), a.dtype) for a in (w_down, w_mix_out)]
        scratch += [
            pltpu.VMEM((2, tall, full), w_down.dtype),
            pltpu.VMEM((w_mix_out.shape[0], full), w_mix_out.dtype),
            pltpu.SemaphoreType.DMA((2, count + 1)),
            pltpu.SemaphoreType.DMA((count + 1,)),
        ]
    outs = pl.pallas_call(
        functools.partial(gather_kernel, dims, blocks),
        out_shape=shapes,
        in_specs=[pl.BlockSpec(memory_space=pltpu.HBM)] * 5,
        out_specs=[pl.BlockSpec(memory_space=pltpu.HBM)] * len(shapes),
        scratch_shapes=scratch,
        compiler_params=pltpu.CompilerParams(collective_id=0, has_side_effects=True),
        name="gather_weights",
    )(*weights)

    def stacked(a):
        return a.reshape(-1, a.shape[2])

    def beside(a):
        return jnp.transpose(a, (1, 0, 2)).reshape(a.shape[1], -1)

    gate, up, down, mix_in, mix_out = outs[:5]
    if laid:
        return stacked(gate), stacked(up), outs[5], stacked(mix_in), outs[6]
    return stacked(gate), stacked(up), beside(down), stacked(mix_in), beside(mix_out)


def rms_scale(values, gain):
    return values * lax.rsqrt(jnp.mean(values * values, axis=-1, keepdims=True) + 1e-06) * gain


def total_over_tp(left_rows, right_matrix):
    part = jnp.dot(left_rows, right_matrix, preferred_element_type=jnp.float32)
    part = part.astype(jnp.bfloat16)
    if lax.axis_size("tp") == 2:
        other = lax.ppermute(part, "tp", ((0, 1), (1, 0)))
        return part.astype(jnp.float32) + other.astype(jnp.float32)
    return lax.psum(part.astype(jnp.float32), "tp")


def own_total_over_tp(left_rows, right_matrix):
    part = jnp.dot(left_rows, right_matrix, preferred_element_type=jnp.float32)
    part = part.astype(jnp.bfloat16)
    if lax.axis_size("tp") == 2:
        mine = own_rows_of(part)
        half = mine.shape[0]
        theirs = lax.dynamic_slice_in_dim(part, (1 - lax.axis_index("tp")) * half, half, 0)
        other = lax.ppermute(theirs, "tp", ((0, 1), (1, 0)))
        return mine.astype(jnp.float32) + other.astype(jnp.float32)
    return lax.psum_scatter(part.astype(jnp.float32), "tp", scatter_dimension=0, tiled=True)


def own_rows_of(array):
    count = array.shape[0] // lax.axis_size("tp")
    return lax.dynamic_slice_in_dim(array, lax.axis_index("tp") * count, count, 0)


def body(dims, tokens, w_gate, w_up, w_down, w_mix_in, w_mix_out, pool_w, pool_scale, norm_gains):
    rows_all = tokens.shape[0]
    stream = tokens.astype(jnp.float32)
    normed = rms_scale(stream, norm_gains[0]).astype(jnp.bfloat16)
    gate_full, up_full, down_full, mix_in_full, mix_out_full = gather_weights(
        dims, w_gate, w_up, w_down, w_mix_in, w_mix_out
    )
    gate_first = jnp.dot(normed, gate_full, preferred_element_type=jnp.float32)
    up_first = jnp.dot(normed, up_full, preferred_element_type=jnp.float32)
    hidden = (jax.nn.silu(gate_first) * up_first).astype(jnp.bfloat16)
    stream = stream + 0.5 * rms_scale(total_over_tp(hidden, down_full), norm_gains[1])
    normed = rms_scale(stream, norm_gains[2]).astype(jnp.bfloat16)
    pooled_in = jnp.dot(normed, mix_in_full, preferred_element_type=jnp.float32)
    pooled_in = pooled_in.astype(jnp.bfloat16)
    groups_here = pool_w.shape[0]
    group_dim = pool_w.shape[1]
    values = pooled_in.astype(jnp.float32).reshape(rows_all // LEN, LEN, groups_here, group_dim)
    totals = jnp.cumsum(values, axis=1)
    position = jnp.arange(1, LEN + 1).astype(jnp.float32)[None, :, None, None]
    window_ids = (lax.axis_index("tp") * groups_here + jnp.arange(groups_here)) % 4
    average = jnp.zeros_like(values)
    for window_slot in range(4):
        window = 2 ** (1 + window_slot)
        lagged = jnp.pad(totals, ((0, 0), (window, 0), (0, 0), (0, 0)))[:, :LEN]
        candidate = (totals - lagged) / jnp.minimum(position, float(window))
        average = jnp.where((window_ids == window_slot)[None, None, :, None], candidate, average)
    deviation = (average - values).astype(jnp.bfloat16)
    regrouped = jnp.einsum("btgi,gio->btgo", deviation, pool_w, preferred_element_type=jnp.float32)
    regrouped = (
        regrouped.reshape(rows_all, groups_here * group_dim) * pool_scale.astype(jnp.float32)
    ).astype(jnp.bfloat16)
    stream = stream + rms_scale(total_over_tp(regrouped, mix_out_full), norm_gains[3])
    normed = rms_scale(stream, norm_gains[4]).astype(jnp.bfloat16)
    gate_second = jnp.dot(normed, gate_full, preferred_element_type=jnp.float32)
    up_second = jnp.dot(normed, up_full, preferred_element_type=jnp.float32)
    hidden = (jax.nn.silu(gate_second) * up_second).astype(jnp.bfloat16)
    stream_own = own_rows_of(stream)
    stream_own = stream_own + 0.5 * rms_scale(own_total_over_tp(hidden, down_full), norm_gains[5])
    return stream_own.astype(jnp.bfloat16)


def silu(v):
    return v / (1.0 + jnp.exp(-v))


def rms_value(values, gain):
    return values * lax.rsqrt(jnp.mean(values * values, axis=-1, keepdims=True) + 1e-06) * gain


def runs(first, count, most=32):
    out, at = [], first
    while at < first + count:
        size = min(most, first + count - at)
        out.append((at, size))
        at += size
    return out


class Sends:
    def __init__(self, sem):
        self.sem, self.count, self.pending = sem, 0, []

    def put(self, src, dst, recv, to, ok=None):
        copy = pltpu.make_async_remote_copy(
            src_ref=src,
            dst_ref=dst,
            send_sem=self.sem.at[self.count],
            recv_sem=recv,
            device_id=to,
            device_id_type=MESH,
        )
        self.count += 1
        when(ok, copy.start)
        self.pending.append((ok, copy))

    def drain(self):
        for ok, copy in self.pending:
            when(ok, copy.wait_send)
        self.pending = []


SENDS = 192
F32, BF16 = jnp.float32, jnp.bfloat16


def layer_kernel(dims, *refs):
    (tokens, gate, up, down, mix_in, mix_out, pool_w, pool_scale, gains, out) = refs[:10]
    (gate_v, up_v, down_v, min_v, mout_v) = refs[10:15]
    (tok_v, norm_v, own_v, far_v, hid_v, part_v, part2_v, partm_v) = refs[15:23]
    (got1, got2o, got2f, gotm, sum1, sum2, far1, far2) = refs[23:31]
    (stream_v, mid_v, pin_v, rg_v, out_v) = refs[31:36]
    (send_sem, ff_sem, mix_sem, act_sem, local_sem, loc_ff) = refs[36:]
    (nz, sz), (_, sy), (_, sx) = dims
    me, core = lax.axis_index("fs"), lax.axis_index("tp")
    z = me // sz
    col = me - z * sz
    xn = me + (1 - 2 * ((me // sx) % 2)) * sx
    yn = me + (1 - 2 * ((me // sy) % 2)) * sy
    dg = xn + yn - me
    sign = 1 - 2 * (z % 2)
    peer = me + sign * sz
    depth = gate.shape[0]
    hid = gate_v.shape[1]
    rows = tokens.shape[0]
    half = rows // 2
    wide = down.shape[1]
    feat = tokens.shape[1]
    span = sz * wide

    barrier = pltpu.get_barrier_semaphore()
    friends = [({"fs": xn}), ({"fs": yn}), ({"tp": 1 - core})]
    for k in range(1, nz):
        friends.append({"fs": lax.rem(z + k, nz) * sz + col})
    for to in friends:
        pl.semaphore_signal(barrier, inc=1, device_id=to, device_id_type=MESH)
    pl.semaphore_wait(barrier, len(friends))

    sends = Sends(send_sem)

    def mo(v, n):
        return v if isinstance(v, int) else pl.multiple_of(v, n)

    def plane(p):
        return near(z, nz, p)[0] if p else z

    weights = ((gate, gate_v), (up, up_v), (down, down_v))

    def own_piece(m, h, u):
        ref = weights[m][0]
        if m < 2:
            return ref.at[pl.ds(u * (depth // 2), depth // 2), pl.ds(mo(h * hid, 128), hid)]
        return ref.at[pl.ds(mo(h * hid + u * (hid // 2), 16), hid // 2), :]

    def place(m, src, u):
        buf = weights[m][1]
        if m < 2:
            return buf.at[pl.ds(mo(src * depth + u * (depth // 2), 16), depth // 2), :]
        return buf.at[src, pl.ds(u * (hid // 2), hid // 2), :]

    def arrived(ref, sem):
        pltpu.make_async_copy(ref, ref, sem).wait()

    locals_ = {}

    def local(key, src, dst, sem):
        copy = pltpu.make_async_copy(src, dst, sem)
        copy.start()
        locals_[key] = copy

    steps = [(m, 0) for m in range(2)] + [(m, p) for m in range(2) for p in range(1, nz)]
    steps += [(m, p) for m in range(2, 4) for p in range(nz)]

    def pieces(m):
        return range(2) if m < 3 else range(1)

    def spot(m, src, u):
        return place(m, src, u) if m < 3 else mout_v.at[src]

    def sem_of(m, src, u):
        return ff_sem.at[m, src, u]

    def origin(m, h, u):
        return own_piece(m, h, u) if m < 3 else mix_out

    def stage0(n):
        m, p = steps[n]
        if p == 0:
            return
        t = plane(p)
        for u in pieces(m):
            sends.put(origin(m, t % 2, u), spot(m, me, u), sem_of(m, me, u), {"fs": t * sz + col})

    def stage1(n):
        m, p = steps[n]
        src = plane(p) * sz + col
        for u in pieces(m):
            if p:
                arrived(spot(m, src, u), sem_of(m, src, u))
            for nb in (xn, yn):
                first = spot(m, src, u) if p else origin(m, z % 2, u)
                sends.put(first, spot(m, src, u), sem_of(m, src, u), {"fs": nb})
            if not p:
                local((m, u), origin(m, z % 2, u), spot(m, me, u), loc_ff.at[m, u])

    def three(p):
        shift = plane(p) * sz - z * sz
        return xn + shift, yn + shift, dg + shift

    def relay(m, p, u, across):
        a, b, _ = three(p)
        src, to = (a, yn) if across else (b, xn)
        arrived(spot(m, src, u), sem_of(m, src, u))
        sends.put(spot(m, src, u), spot(m, src, u), sem_of(m, src, u), {"fs": to})

    def stage2(n):
        m, p = steps[n]
        if m < 3:
            relay(m, p, 0, True)
            relay(m, p, 1, False)
        else:
            relay(m, p, 0, p % 2 == 0)

    def stage3(n):
        m, p = steps[n]
        a, b, d = three(p)
        if m < 3:
            todo = [(a, 1), (b, 0), (d, 0), (d, 1)]
        else:
            todo = [(b if p % 2 == 0 else a, 0), (d, 0)]
        for src, u in todo:
            arrived(spot(m, src, u), sem_of(m, src, u))
        if p == 0:
            for u in pieces(m):
                locals_[(m, u)].wait()

    def min_at(src):
        return min_v.at[pl.ds(mo(src * depth, 16), depth), :]

    def mix_own():
        for nb in (xn, yn):
            sends.put(mix_in, min_at(me), mix_sem.at[me], {"fs": nb})
        local("mix", mix_in, min_at(me), local_sem.at[0])

    def mix_turn():
        arrived(min_at(xn), mix_sem.at[xn])
        sends.put(min_at(xn), min_at(xn), mix_sem.at[xn], {"fs": yn})

    def mix_up():
        arrived(min_at(yn), mix_sem.at[yn])
        arrived(min_at(dg), mix_sem.at[dg])
        locals_["mix"].wait()
        for src in (me, xn, yn, dg):
            for step in (1, -1):
                ok = jnp.logical_and(z + step >= 0, z + step < nz)
                sends.put(min_at(src), min_at(src), mix_sem.at[src], {"fs": me + step * sz}, ok)

    def mix_on(p, forward=True):
        found, away = near(z, nz, p)
        shift = (found - z) * sz
        inside = jnp.logical_and(z + away >= 0, z + away < nz)
        for src in (me + shift, xn + shift, yn + shift, dg + shift):
            here, sem = min_at(src), mix_sem.at[src]
            if forward:
                when(inside, functools.partial(arrived, here, sem))
                sends.put(here, here, sem, {"fs": me + away * sz}, inside)
            else:
                when(jnp.logical_not(inside), functools.partial(arrived, here, sem))

    mine = pl.ds(mo(core * half, 16), half)
    theirs = pl.ds(mo((1 - core) * half, 16), half)
    mine_far = pl.ds(mo(rows + core * half, 16), half)
    theirs_far = pl.ds(mo(rows + (1 - core) * half, 16), half)
    partner = {"tp": 1 - core}
    buddy = {"fs": peer}

    def tokens_out():
        sends.put(tokens.at[mine, :], tok_v.at[mine_far, :], act_sem.at[0], buddy)
        local("tok", tokens, tok_v.at[pl.ds(0, rows), :], local_sem.at[1])

    def tokens_on():
        here = tok_v.at[mine_far, :]
        arrived(here, act_sem.at[0])
        sends.put(here, here, act_sem.at[1], partner)

    def first_norm():
        arrived(tok_v.at[theirs_far, :], act_sem.at[1])
        locals_["tok"].wait()

        def block(i, carry):
            at = pl.ds(pl.multiple_of(i * 32, 32), 32)
            v = tok_v[at, :].astype(F32)
            norm_v[at, :] = rms_value(v, gains[0:1, :]).astype(BF16)
            return carry

        lax.fori_loop(0, 2 * rows // 32, block, 0)

    def gate_up(src, at, dst):
        def tile(cols, n):
            w = jnp.concatenate([gate_v[:, cols], up_v[:, cols]], axis=1)
            both = jnp.dot(src[at, :], w, preferred_element_type=F32)
            hid_v[dst, cols] = (silu(both[:, :n]) * both[:, n:]).astype(BF16)

        whole = hid // 256

        def body(j, carry):
            tile(pl.ds(pl.multiple_of(j * 256, 256), 256), 256)
            return carry

        lax.fori_loop(0, whole, body, 0)
        if hid % 256:
            tile(pl.ds(whole * 256, hid % 256), hid % 256)

    def down_block(t, at):
        w = jnp.concatenate([down_v[t * sz + i] for i in range(sz)], axis=1)
        return jnp.dot(hid_v[at, :], w, preferred_element_type=F32).astype(BF16)

    def cols_of(t):
        return pl.ds(mo(t * span, 128), span)

    def down1(p):
        t = plane(p)
        cols = cols_of(t)
        for i, (base, other) in enumerate(((rows, theirs_far), (0, theirs))):
            at = pl.ds(base, rows)
            part_v[at, cols] = down_block(t, at)
            sends.put(part_v.at[other, cols], got1.at[1 - i, :, cols], act_sem.at[8 + 2 * p + i], partner)

    def reduce1(p):
        cols = cols_of(plane(p))
        for i in range(2):
            arrived(got1.at[1 - i, :, cols], act_sem.at[8 + 2 * p + i])
        total = part_v[mine_far, cols].astype(F32) + got1[1, :, cols].astype(F32)
        sum1[:, cols] = total.astype(BF16)
        sends.put(sum1.at[:, cols], far1.at[:, cols], act_sem.at[16 + plane(p)], buddy)

    def first_stream():
        for t in range(nz):
            cols = cols_of(t)
            arrived(far1.at[:, cols], act_sem.at[16 + t])

        for start, size in runs(0, half):
            r = pl.ds(start, size)
            at = pl.ds(pl.multiple_of(core * half + start, 16), size)
            y = part_v[at, :].astype(F32) + got1[0, r, :].astype(F32) + far1[r, :].astype(F32)
            s = tok_v[at, :].astype(F32) + 0.5 * rms_value(y, gains[1:2, :])
            stream_v[r, :] = s
            mid_v[at, :] = rms_value(s, gains[2:3, :]).astype(BF16)
        sends.put(mid_v.at[mine, :], mid_v.at[mine, :], act_sem.at[2], partner)

    def into_pool(at):
        v = jnp.dot(mid_v[at, :], min_v[...], preferred_element_type=F32)
        pin_v[at, :] = v.astype(BF16).astype(F32)

    def pool():
        length = LEN
        groups, dim = pool_w.shape[0], pool_w.shape[1]
        t = lax.broadcasted_iota(jnp.int32, (rows, dim), 0) % length
        for g in range(groups):
            cols = slice(g * dim, (g + 1) * dim)
            v = pin_v[:, cols]
            window = 2 ** (1 + g % 4)
            total, k = v, 1
            while k < window:
                total = total + jnp.where(t >= k, pltpu.roll(total, k, 0), 0.0)
                k *= 2
            count = jnp.minimum(t + 1, window).astype(F32)
            dev = (total / count - v).astype(BF16)
            o = jnp.dot(dev, pool_w[g], preferred_element_type=F32) * pool_scale[:, cols]
            rg_v[:, cols] = o.astype(BF16)

    def out_pool(at):
        for t in range(nz):
            w = jnp.concatenate([mout_v[t * sz + i] for i in range(sz)], axis=1)
            v = jnp.dot(rg_v[at, :], w, preferred_element_type=F32)
            partm_v[at, pl.ds(t * span, span)] = v.astype(BF16)

    units = half // 16
    firsts = [-(-units * k // 3) * 16 for k in range(4)]
    chunks = [(a, b - a) for a, b in zip(firsts[:-1], firsts[1:]) if b > a]

    def second_stream():
        arrived(gotm, act_sem.at[3])
        for k, (first, count) in enumerate(chunks):
            for start, size in runs(first, count):
                r = pl.ds(start, size)
                at = pl.ds(pl.multiple_of(core * half + start, 16), size)
                y = partm_v[at, :].astype(F32) + gotm[r, :].astype(F32)
                s = stream_v[r, :] + rms_value(y, gains[3:4, :])
                stream_v[r, :] = s
                own_v[at, :] = rms_value(s, gains[4:5, :]).astype(BF16)
            src = own_v.at[pl.ds(mo(core * half + first, 16), count), :]
            sends.put(src, far_at(k, core), act_sem.at[32 + k], buddy)
        sends.put(own_v.at[mine, :], own_v.at[mine, :], act_sem.at[6], partner)

    def far_rows(k, c):
        first, count = chunks[k]
        return mo(2 * first + c * count, 16), count

    def far_at(k, c):
        return far_v.at[pl.ds(*far_rows(k, c)), :]

    def far_on(k):
        arrived(far_at(k, core), act_sem.at[32 + k])
        sends.put(far_at(k, core), far_at(k, core), act_sem.at[36 + k], partner)

    def down2(base, count, low, high):
        at = pl.ds(base, count)

        def body(t, carry):
            part2_v[at, pl.ds(pl.multiple_of(t * span, 128), span)] = down_block(t, at)
            return carry

        lax.fori_loop(low, high, body, 0)

    def far_part(k, c):
        first, count = far_rows(k, c)
        return pl.ds(mo(rows + first, 16), count)

    last = len(steps)
    stage1(0)
    for n in range(2, 6):
        stage0(n)
    stage1(1)
    mix_own()
    tokens_out()
    stage2(0)
    all_mine = pl.ds(0, rows)
    all_far = pl.ds(rows, rows)

    def advance(i):
        if i + 6 < last:
            stage0(i + 6)
        if i + 2 < last:
            stage1(i + 2)
        if i + 1 < last:
            stage2(i + 1)
        stage3(i)

    for i in range(3 * nz):
        advance(i)
        if i == 0:
            mix_turn()
        if i == 2:
            tokens_on()
            mix_up()
        if i == 4:
            first_norm()
        for p in range(1, nz):
            if i == 3 + 2 * p:
                mix_on(p)
        if i == 2 * nz - 1:
            gate_up(norm_v, all_mine, all_mine)
        if i == 2 * nz:
            gate_up(norm_v, all_far, all_far)
        if i == 2 * nz + 1:
            down1(0)
            down1(1)
        if 2 * nz + 1 < i:
            down1(i - 2 * nz)
            if i == 2 * nz + 2:
                reduce1(0)
            reduce1(i - 2 * nz - 1)
    advance(3 * nz)
    reduce1(nz - 1)
    for i in range(3 * nz + 1, last - 1):
        advance(i)
    first_stream()
    for p in range(1, nz):
        mix_on(p, forward=False)
    into_pool(mine)
    arrived(mid_v.at[theirs, :], act_sem.at[2])
    into_pool(theirs)
    pool()
    advance(last - 1)
    out_pool(theirs)
    sends.put(partm_v.at[theirs, :], gotm, act_sem.at[3], partner)
    out_pool(mine)
    second_stream()

    arrived(own_v.at[theirs, :], act_sem.at[6])
    gate_up(own_v, all_mine, all_mine)
    down2(0, rows, 0, nz // 2)
    far_on(0)
    down2(0, rows, nz // 2, nz)
    sends.put(part2_v.at[theirs, :], got2o, act_sem.at[7], partner)
    for k, (first, count) in enumerate(chunks):
        arrived(far_at(k, 1 - core), act_sem.at[36 + k])
        here = pl.ds(first, count)
        gate_up(far_v, pl.ds(2 * first, 2 * count), pl.ds(rows + 2 * first, 2 * count))
        if k + 1 < len(chunks):
            far_on(k + 1)
        down2(rows + 2 * first, 2 * count, 0, nz)
        sends.put(part2_v.at[far_part(k, 1 - core), :], got2f.at[here, :], act_sem.at[40 + k], partner)
        arrived(got2f.at[here, :], act_sem.at[40 + k])
        total = part2_v[far_part(k, core), :].astype(F32) + got2f[here, :].astype(F32)
        sum2[here, :] = total.astype(BF16)
        sends.put(sum2.at[here, :], far2.at[here, :], act_sem.at[44 + k], buddy)
    arrived(got2o, act_sem.at[7])
    for k, (first, count) in enumerate(chunks):
        arrived(far2.at[pl.ds(first, count), :], act_sem.at[44 + k])
        for start, size in runs(first, count):
            r = pl.ds(start, size)
            at = pl.ds(pl.multiple_of(core * half + start, 16), size)
            y = part2_v[at, :].astype(F32) + got2o[r, :].astype(F32) + far2[r, :].astype(F32)
            s = stream_v[r, :] + 0.5 * rms_value(y, gains[5:6, :])
            out_v[r, :] = s.astype(BF16)
    final = pltpu.make_async_copy(out_v, out, local_sem.at[2])
    final.start()
    sends.drain()
    final.wait()


def whole_layer(dims, tokens, w_gate, w_up, w_down, w_mix_in, w_mix_out, pool_w, pool_scale, gains):
    count = 1
    for size, _ in dims:
        count *= size
    nz = dims[0][0]
    depth, units = w_gate.shape
    hid = units // 2
    rows, feat = tokens.shape
    half = rows // 2
    wide = w_down.shape[1]
    pooled = w_mix_in.shape[1]
    scale = pool_scale.astype(F32).reshape(1, -1)

    def buf(*shape, dtype=BF16):
        return pltpu.VMEM(shape, dtype)

    scratch = [
        buf(count * depth, hid),
        buf(count * depth, hid),
        buf(count, hid, wide),
        buf(count * depth, pooled),
        buf(count, w_mix_out.shape[0], wide),
        buf(2 * rows, feat),
        buf(2 * rows, feat),
        buf(rows, feat),
        buf(rows, feat),
        buf(2 * rows, hid),
        buf(2 * rows, feat),
        buf(2 * rows, feat),
        buf(rows, feat),
        buf(2, half, feat),
        buf(half, feat),
        buf(half, feat),
        buf(half, feat),
        buf(half, feat),
        buf(half, feat),
        buf(half, feat),
        buf(half, feat),
        buf(half, feat, dtype=F32),
        buf(rows, feat),
        buf(rows, pooled, dtype=F32),
        buf(rows, pooled),
        buf(half, feat),
        pltpu.SemaphoreType.DMA((SENDS,)),
        pltpu.SemaphoreType.DMA((4, count, 2)),
        pltpu.SemaphoreType.DMA((count,)),
        pltpu.SemaphoreType.DMA((48,)),
        pltpu.SemaphoreType.DMA((4,)),
        pltpu.SemaphoreType.DMA((4, 2)),
    ]
    hbm = pl.BlockSpec(memory_space=pltpu.HBM)
    vmem = pl.BlockSpec(memory_space=pltpu.VMEM)
    return pl.pallas_call(
        functools.partial(layer_kernel, dims),
        out_shape=jax.ShapeDtypeStruct((half, feat), tokens.dtype),
        in_specs=[hbm] * 6 + [vmem] * 3,
        out_specs=hbm,
        scratch_shapes=scratch,
        compiler_params=pltpu.CompilerParams(
            collective_id=1, has_side_effects=True, vmem_limit_bytes=67043328
        ),
        name="whole_layer",
    )(tokens, w_gate, w_up, w_down, w_mix_in, w_mix_out, pool_w, scale, gains)


def paired(dims, mesh):
    return (
        len(dims) == 3
        and dims[0][0] == 4
        and dims[1][0] == 2
        and dims[2][0] == 2
        and mesh.shape["tp"] == 2
    )


def solution(mesh):
    in_specs = (
        P("fs", None),
        P("fs", "tp"),
        P("fs", "tp"),
        P("tp", "fs"),
        P("fs", "tp"),
        P("tp", "fs"),
        P("tp", None, None),
        P("tp"),
        P(),
    )
    out_specs = P(("fs", "tp"), None)
    dims = line_dims(mesh)
    act = whole_layer if paired(dims, mesh) else body
    return jax.shard_map(
        functools.partial(act, dims), mesh=mesh, in_specs=in_specs, out_specs=out_specs, check_vma=False
    )
```

```python
import functools
import itertools

import jax
import jax.numpy as jnp
from jax import lax
from jax.experimental import pallas as pl
from jax.experimental.pallas import tpu as pltpu
from jax.sharding import PartitionSpec as P

LEN = 64
MESH = pl.DeviceIdType.MESH


def line_dims(mesh):
    devices = mesh.devices.reshape(mesh.shape["fs"], -1)[:, 0]
    count = len(devices)
    coords = [tuple(getattr(d, "coords", ())) for d in devices]
    dims = []
    for axis in range(len(coords[0])):
        values = sorted({c[axis] for c in coords})
        if len(values) > 1:
            stride = next(i for i in range(count) if coords[i][axis] != coords[0][axis])
            dims.append((len(values), stride, axis, values))
    dims.sort(key=lambda d: -d[1])
    good = len(dims) > 0 and all(
        sum(vals.index(c[axis]) * stride for _, stride, axis, vals in dims) == i
        for i, c in enumerate(coords)
    )
    if not good:
        return ((count, 1),)
    return tuple((d[0], d[1]) for d in dims)


def near(position, size, rank):
    inner = jnp.minimum(position, size - 1 - position)
    alternating = rank <= 2 * inner
    distance = jnp.where(alternating, (rank + 1) // 2, rank - inner)
    toward_high = jnp.where(alternating, rank % 2 == 1, 2 * position < size - 1)
    step = jnp.where(toward_high, 1, -1)
    return position + step * distance, -step


def piece_plan(dims, order):
    sizes = [dims[d][0] for d in order]
    slots = []
    for ranks in itertools.product(*[range(n) for n in sizes]):
        slots.append(ranks)
    slots.sort(key=lambda r: (sum(r), r))
    return slots


class Piece:
    def __init__(self, index, dims, order, src_of, dst_of):
        self.index, self.dims, self.order = index, dims, order
        self.src_of, self.dst_of = src_of, dst_of
        self.slots = piece_plan(dims, order)

    def locate(self, me, ranks):
        source, last, away = me, -1, None
        for place, (d, rank) in enumerate(zip(self.order, ranks)):
            if rank > 0:
                size, stride = self.dims[d]
                position = (me // stride) % size
                found, step = near(position, size, rank)
                source = source + (found - position) * stride
                last, away = place, step
        return source, last, away

    def sends(self, me, ranks):
        _, last, away = self.locate(me, ranks)
        out = []
        for place, d in enumerate(self.order):
            size, stride = self.dims[d]
            position = (me // stride) % size
            if place == last:
                if size > 2:
                    ok = jnp.logical_and(position + away >= 0, position + away < size)
                    out.append((ok, me + away * stride))
            elif place > last:
                if size == 2:
                    out.append((None, me + (1 - 2 * position) * stride))
                else:
                    out.append((position + 1 < size, me + stride))
                    out.append((position > 0, me - stride))
        return out


def when(condition, act):
    if condition is None:
        act()
    else:
        pl.when(condition)(act)


def spread(pieces, me, chunk, send_sem, recv_sem, low, high, mode):
    todo = []
    for piece in pieces:
        for ranks in piece.slots:
            todo.append((sum(ranks), piece, ranks))
    todo.sort(key=lambda t: t[0])
    for depth, piece, ranks in todo:
        if not low <= depth < high:
            continue
        source, last, _ = piece.locate(me, ranks)
        landed = piece.dst_of(chunk, source)
        origin = piece.src_of(chunk) if depth == 0 else landed
        recv = recv_sem.at[chunk, piece.index, source]
        if depth > 0 and mode == "start":
            pltpu.make_async_copy(landed, landed, recv).wait()
        base = piece.first_send[ranks]
        for offset, (ok, target) in enumerate(piece.sends(me, ranks)):
            copy = pltpu.make_async_remote_copy(
                src_ref=origin,
                dst_ref=landed,
                send_sem=send_sem.at[chunk, base + offset],
                recv_sem=recv,
                device_id={"fs": target},
                device_id_type=MESH,
            )
            when(ok, copy.start if mode == "start" else copy.wait_send)


def number_sends(pieces):
    total = 0
    for piece in pieces:
        piece.first_send = {}
        for ranks in piece.slots:
            piece.first_send[ranks] = total
            last = max([i for i, r in enumerate(ranks) if r > 0], default=-1)
            for place, d in enumerate(piece.order):
                size = piece.dims[d][0]
                if place == last:
                    total += 1 if size > 2 else 0
                elif place > last:
                    total += 1 if size == 2 else 2
    return total


def cut(extent, unit, share):
    return max(unit, min(extent - unit, round(extent * share / unit) * unit))


def gather_plan(dims, refs, outs, blocks):
    gate, up, down, mix_in, mix_out = refs
    gate_o, up_o, down_o, mix_in_o, mix_out_o = outs
    n = len(dims)
    first = tuple(range(n))
    second = first[1:] + first[:1]
    third = first[-1:] + first[:-1]
    pooled = mix_out.shape[0]

    def rows(ref, out, start_of, size):
        return (
            lambda c: ref.at[pl.ds(start_of(c), size), :],
            lambda c, s: out.at[s, pl.ds(start_of(c), size), :],
        )

    def at(block, offset):
        return lambda c: pl.multiple_of(c * block + offset, 16)

    block, tall = gate.shape[0] // blocks, down.shape[0] // blocks
    down_cut = cut(tall, 16, 2 / 3)
    main = [
        Piece(0, dims, first, *rows(gate, gate_o, at(block, 0), block)),
        Piece(1, dims, third, *rows(up, up_o, at(block, 0), block)),
        Piece(2, dims, first, *rows(down, down_o, at(tall, 0), down_cut)),
        Piece(3, dims, second, *rows(down, down_o, at(tall, down_cut), tall - down_cut)),
    ]
    mix_cut = cut(pooled, 16, 2 / 3)

    def fixed(offset):
        return lambda c: offset

    mix = [
        Piece(0, dims, first, *rows(mix_in, mix_in_o, fixed(0), mix_in.shape[0])),
        Piece(1, dims, third, *rows(mix_out, mix_out_o, fixed(0), mix_cut)),
        Piece(2, dims, second, *rows(mix_out, mix_out_o, fixed(mix_cut), pooled - mix_cut)),
    ]
    return main, mix


def gather_kernel(dims, blocks, *args):
    refs, outs = args[:5], args[5:10]
    beside = None
    if len(args) > 13:
        beside = args[10:12]
        args = args[:10] + args[12:]
    send_sem, recv_sem, local_sem = args[10:13]
    me = lax.axis_index("fs")
    barrier = pltpu.get_barrier_semaphore()
    expected = 0
    for size, stride in dims:
        position = (me // stride) % size
        for step, ok in ((1, position + 1 < size), (-1, position > 0)):
            def signal(step=step, stride=stride):
                pl.semaphore_signal(
                    barrier, inc=1, device_id={"fs": me + step * stride}, device_id_type=MESH
                )

            pl.when(ok)(signal)
            expected = expected + jnp.where(ok, 1, 0)
    pl.semaphore_wait(barrier, expected)

    main, mix = gather_plan(dims, refs, outs, blocks)
    number_sends(main)
    number_sends(mix)
    deepest = sum(size - 1 for size, _ in dims) + 1
    early = min(3, deepest)

    locals_ = []
    for i, (ref, out) in enumerate(zip(refs, outs)):
        if beside is not None and i in (2, 4):
            continue
        locals_.append(pltpu.make_async_copy(ref, out.at[me], local_sem.at[i]))

    go = functools.partial(spread, send_sem=send_sem, recv_sem=recv_sem)
    def shard_in(source, stage, sem, shard, across):
        return pltpu.make_async_copy(
            source, stage.at[:, pl.ds(shard * across, across)], sem.at[shard]
        )

    def lay_in(own, part, stage, sem, rows, height):
        for shard in range(part.shape[0]):
            for mine, source in ((True, own), (False, part.at[shard])):

                @pl.when((me == shard) if mine else (me != shard))
                def _(source=source, shard=shard):
                    piece = source.at[pl.ds(rows, height), :]
                    shard_in(piece, stage, sem, shard, part.shape[2]).start()

    def lay_out(part, whole, stage, sem, rows, height, mode):
        if mode == "start":
            for shard in range(part.shape[0]):
                piece = part.at[shard, pl.ds(rows, height), :]
                shard_in(piece, stage, sem, shard, part.shape[2]).wait()
        copy = pltpu.make_async_copy(
            stage, whole.at[pl.ds(rows, height), :], sem.at[part.shape[0]]
        )
        copy.start() if mode == "start" else copy.wait()

    if beside is not None:
        down_stage, mix_stage, down_sem, mix_sem = args[13:]
        tall = down_stage.shape[1]

        pooled = mix_stage.shape[0]

    def rows_of(c):
        return c * tall if isinstance(c, int) else pl.multiple_of(c * tall, 16)

    def down_in(c):
        slot = c % 2
        lay_in(refs[2], outs[2], down_stage.at[slot], down_sem.at[slot], rows_of(c), tall)

    def down_out(c, mode="start"):
        slot = c % 2
        lay_out(outs[2], beside[0], down_stage.at[slot], down_sem.at[slot], rows_of(c), tall, mode)

    go(mix, me, blocks, low=0, high=1, mode="start")
    go(main, me, 0, low=0, high=1, mode="start")
    for copy in locals_:
        copy.start()
    go(mix, me, blocks, low=1, high=deepest, mode="start")
    if beside is not None:
        lay_in(refs[4], outs[4], mix_stage, mix_sem, 0, pooled)

    def step(i, carry):
        @pl.when(i + 1 < blocks)
        def _():
            go(main, me, i + 1, low=0, high=1, mode="start")

        go(main, me, i, low=1, high=early, mode="start")

        @pl.when(i > 0)
        def _():
            go(main, me, i - 1, low=early, high=deepest, mode="start")

        if beside is not None:

            @pl.when(i > 2)
            def _():
                down_out(i - 3, "end")

            @pl.when(i > 0)
            def _():
                down_in(i - 1)

            @pl.when(i > 1)
            def _():
                down_out(i - 2)

        return carry

    lax.fori_loop(0, blocks, step, 0)
    go(main, me, blocks - 1, low=early, high=deepest, mode="start")
    if beside is not None:
        if blocks > 2:
            down_out(blocks - 3, "end")
        down_in(blocks - 1)
        if blocks > 1:
            down_out(blocks - 2)
        lay_out(outs[4], beside[1], mix_stage, mix_sem, 0, pooled, "start")
        down_out(blocks - 1)

    def finish(i, carry):
        go(main, me, i, low=0, high=deepest, mode="end")
        return carry

    lax.fori_loop(0, blocks, finish, 0)
    go(mix, me, blocks, low=0, high=deepest, mode="end")
    if beside is not None:
        if blocks > 1:
            down_out(blocks - 2, "end")
        down_out(blocks - 1, "end")
        lay_out(outs[4], beside[1], mix_stage, mix_sem, 0, pooled, "end")
    for copy in locals_:
        copy.wait()


def gather_weights(dims, w_gate, w_up, w_down, w_mix_in, w_mix_out):
    count = 1
    for size, _ in dims:
        count *= size
    tiles = (w_gate.shape[0] // 16, w_down.shape[0] // 16)
    blocks = next(b for b in (8, 4, 2, 1) if tiles[0] % b == 0 and tiles[1] % b == 0)
    weights = (w_gate, w_up, w_down, w_mix_in, w_mix_out)
    shapes = [jax.ShapeDtypeStruct((count, *a.shape), a.dtype) for a in weights]

    class Shape:
        def __init__(self, shape):
            self.shape = shape

    stand_in = [Shape(a.shape) for a in weights]
    main, mix = gather_plan(dims, stand_in, [Shape(s.shape) for s in shapes], blocks)
    sends = max(number_sends(main), number_sends(mix))
    scratch = [
        pltpu.SemaphoreType.DMA((blocks + 1, sends)),
        pltpu.SemaphoreType.DMA((blocks + 1, len(main), count)),
        pltpu.SemaphoreType.DMA((5,)),
    ]
    laid = w_down.shape[1] % 128 == 0
    if laid:
        tall, full = w_down.shape[0] // blocks, w_down.shape[1] * count
        shapes += [jax.ShapeDtypeStruct((a.shape[0], full), a.dtype) for a in (w_down, w_mix_out)]
        scratch += [
            pltpu.VMEM((2, tall, full), w_down.dtype),
            pltpu.VMEM((w_mix_out.shape[0], full), w_mix_out.dtype),
            pltpu.SemaphoreType.DMA((2, count + 1)),
            pltpu.SemaphoreType.DMA((count + 1,)),
        ]
    outs = pl.pallas_call(
        functools.partial(gather_kernel, dims, blocks),
        out_shape=shapes,
        in_specs=[pl.BlockSpec(memory_space=pltpu.HBM)] * 5,
        out_specs=[pl.BlockSpec(memory_space=pltpu.HBM)] * len(shapes),
        scratch_shapes=scratch,
        compiler_params=pltpu.CompilerParams(collective_id=0, has_side_effects=True),
        name="gather_weights",
    )(*weights)

    def stacked(a):
        return a.reshape(-1, a.shape[2])

    def beside(a):
        return jnp.transpose(a, (1, 0, 2)).reshape(a.shape[1], -1)

    gate, up, down, mix_in, mix_out = outs[:5]
    if laid:
        return stacked(gate), stacked(up), outs[5], stacked(mix_in), outs[6]
    return stacked(gate), stacked(up), beside(down), stacked(mix_in), beside(mix_out)


def rms_scale(values, gain):
    return values * lax.rsqrt(jnp.mean(values * values, axis=-1, keepdims=True) + 1e-06) * gain


def total_over_tp(left_rows, right_matrix):
    part = jnp.dot(left_rows, right_matrix, preferred_element_type=jnp.float32)
    part = part.astype(jnp.bfloat16)
    if lax.axis_size("tp") == 2:
        other = lax.ppermute(part, "tp", ((0, 1), (1, 0)))
        return part.astype(jnp.float32) + other.astype(jnp.float32)
    return lax.psum(part.astype(jnp.float32), "tp")


def own_total_over_tp(left_rows, right_matrix):
    part = jnp.dot(left_rows, right_matrix, preferred_element_type=jnp.float32)
    part = part.astype(jnp.bfloat16)
    if lax.axis_size("tp") == 2:
        mine = own_rows_of(part)
        half = mine.shape[0]
        theirs = lax.dynamic_slice_in_dim(part, (1 - lax.axis_index("tp")) * half, half, 0)
        other = lax.ppermute(theirs, "tp", ((0, 1), (1, 0)))
        return mine.astype(jnp.float32) + other.astype(jnp.float32)
    return lax.psum_scatter(part.astype(jnp.float32), "tp", scatter_dimension=0, tiled=True)


def own_rows_of(array):
    count = array.shape[0] // lax.axis_size("tp")
    return lax.dynamic_slice_in_dim(array, lax.axis_index("tp") * count, count, 0)


def body(dims, tokens, w_gate, w_up, w_down, w_mix_in, w_mix_out, pool_w, pool_scale, norm_gains):
    rows_all = tokens.shape[0]
    stream = tokens.astype(jnp.float32)
    normed = rms_scale(stream, norm_gains[0]).astype(jnp.bfloat16)
    gate_full, up_full, down_full, mix_in_full, mix_out_full = gather_weights(
        dims, w_gate, w_up, w_down, w_mix_in, w_mix_out
    )
    gate_first = jnp.dot(normed, gate_full, preferred_element_type=jnp.float32)
    up_first = jnp.dot(normed, up_full, preferred_element_type=jnp.float32)
    hidden = (jax.nn.silu(gate_first) * up_first).astype(jnp.bfloat16)
    stream = stream + 0.5 * rms_scale(total_over_tp(hidden, down_full), norm_gains[1])
    normed = rms_scale(stream, norm_gains[2]).astype(jnp.bfloat16)
    pooled_in = jnp.dot(normed, mix_in_full, preferred_element_type=jnp.float32)
    pooled_in = pooled_in.astype(jnp.bfloat16)
    groups_here = pool_w.shape[0]
    group_dim = pool_w.shape[1]
    values = pooled_in.astype(jnp.float32).reshape(rows_all // LEN, LEN, groups_here, group_dim)
    totals = jnp.cumsum(values, axis=1)
    position = jnp.arange(1, LEN + 1).astype(jnp.float32)[None, :, None, None]
    window_ids = (lax.axis_index("tp") * groups_here + jnp.arange(groups_here)) % 4
    average = jnp.zeros_like(values)
    for window_slot in range(4):
        window = 2 ** (1 + window_slot)
        lagged = jnp.pad(totals, ((0, 0), (window, 0), (0, 0), (0, 0)))[:, :LEN]
        candidate = (totals - lagged) / jnp.minimum(position, float(window))
        average = jnp.where((window_ids == window_slot)[None, None, :, None], candidate, average)
    deviation = (average - values).astype(jnp.bfloat16)
    regrouped = jnp.einsum("btgi,gio->btgo", deviation, pool_w, preferred_element_type=jnp.float32)
    regrouped = (
        regrouped.reshape(rows_all, groups_here * group_dim) * pool_scale.astype(jnp.float32)
    ).astype(jnp.bfloat16)
    stream = stream + rms_scale(total_over_tp(regrouped, mix_out_full), norm_gains[3])
    normed = rms_scale(stream, norm_gains[4]).astype(jnp.bfloat16)
    gate_second = jnp.dot(normed, gate_full, preferred_element_type=jnp.float32)
    up_second = jnp.dot(normed, up_full, preferred_element_type=jnp.float32)
    hidden = (jax.nn.silu(gate_second) * up_second).astype(jnp.bfloat16)
    stream_own = own_rows_of(stream)
    stream_own = stream_own + 0.5 * rms_scale(own_total_over_tp(hidden, down_full), norm_gains[5])
    return stream_own.astype(jnp.bfloat16)


def silu(v):
    return v / (1.0 + jnp.exp(-v))


def rms_value(values, gain):
    return values * lax.rsqrt(jnp.mean(values * values, axis=-1, keepdims=True) + 1e-06) * gain


def runs(first, count, most=32):
    out, at = [], first
    while at < first + count:
        size = min(most, first + count - at)
        out.append((at, size))
        at += size
    return out


class Sends:
    def __init__(self, sem):
        self.sem, self.count, self.pending = sem, 0, {}

    def put(self, src, dst, recv, to, ok=None):
        slot = self.count % SENDS
        self.count += 1
        self.settle(slot)
        copy = pltpu.make_async_remote_copy(
            src_ref=src,
            dst_ref=dst,
            send_sem=self.sem.at[slot],
            recv_sem=recv,
            device_id=to,
            device_id_type=MESH,
        )
        when(ok, copy.start)
        self.pending[slot] = (ok, copy)

    def settle(self, slot):
        if slot in self.pending:
            ok, copy = self.pending.pop(slot)
            when(ok, copy.wait_send)

    def drain(self):
        for slot in list(self.pending):
            self.settle(slot)


SENDS = 96
F32, BF16 = jnp.float32, jnp.bfloat16


def layer_kernel(dims, *refs):
    (tokens, gate, up, down, mix_in, mix_out, pool_w, pool_scale, gains, out) = refs[:10]
    (gate_v, up_v, down_v, min_v, mout_v) = refs[10:15]
    (tok_v, norm_v, own_v, far_v, hid_v, part_v, part2_v, partm_v) = refs[15:23]
    (got1, got2o, got2f, gotm, sum1, sum2, far1, far2) = refs[23:31]
    (stream_v, mid_v, pin_v, rg_v, out_v) = refs[31:36]
    (send_sem, ff_sem, mix_sem, act_sem, local_sem, loc_ff) = refs[36:]
    (nz, sz), (_, sy), (_, sx) = dims
    me, core = lax.axis_index("fs"), lax.axis_index("tp")
    z = me // sz
    col = me - z * sz
    xn = me + (1 - 2 * ((me // sx) % 2)) * sx
    yn = me + (1 - 2 * ((me // sy) % 2)) * sy
    dg = xn + yn - me
    sign = 1 - 2 * (z % 2)
    peer = me + sign * sz
    depth = gate.shape[0]
    hid = gate_v.shape[1]
    rows = tokens.shape[0]
    half = rows // 2
    wide = down.shape[1]
    feat = tokens.shape[1]
    span = sz * wide

    barrier = pltpu.get_barrier_semaphore()
    friends = [({"fs": xn}), ({"fs": yn}), ({"tp": 1 - core})]
    for k in range(1, nz):
        friends.append({"fs": lax.rem(z + k, nz) * sz + col})
    for to in friends:
        pl.semaphore_signal(barrier, inc=1, device_id=to, device_id_type=MESH)
    pl.semaphore_wait(barrier, len(friends))

    sends = Sends(send_sem)

    def mo(v, n):
        return v if isinstance(v, int) else pl.multiple_of(v, n)

    def plane(p):
        return near(z, nz, p)[0] if p else z

    weights = ((gate, gate_v), (up, up_v), (down, down_v))

    def own_piece(m, h, u):
        ref = weights[m][0]
        if m < 2:
            return ref.at[pl.ds(u * (depth // 2), depth // 2), pl.ds(mo(h * hid, 128), hid)]
        return ref.at[pl.ds(mo(h * hid + u * (hid // 2), 16), hid // 2), :]

    def place(m, src, u):
        buf = weights[m][1]
        if m < 2:
            return buf.at[pl.ds(mo(src * depth + u * (depth // 2), 16), depth // 2), :]
        return buf.at[src, pl.ds(u * (hid // 2), hid // 2), :]

    def arrived(ref, sem):
        pltpu.make_async_copy(ref, ref, sem).wait()

    locals_ = {}

    def local(key, src, dst, sem):
        copy = pltpu.make_async_copy(src, dst, sem)
        copy.start()
        locals_[key] = copy

    steps = [(m, 0) for m in range(2)] + [(m, p) for m in range(2) for p in range(1, nz)]
    steps += [(m, p) for m in range(2, 4) for p in range(nz)]

    def pieces(m):
        return range(2) if m < 3 else range(1)

    tall = mix_out.shape[0]
    early = tall // 4
    late_rows = pl.ds(0, tall - early)
    early_rows = pl.ds(tall - early, early)

    def spot(m, src, u):
        return place(m, src, u) if m < 3 else mout_v.at[src, late_rows, :]

    def sem_of(m, src, u):
        return ff_sem.at[m, src]

    def origin(m, h, u):
        return own_piece(m, h, u) if m < 3 else mix_out.at[late_rows, :]

    def stage0(n):
        m, p = steps[n]
        if p == 0:
            return
        t = plane(p)
        for u in pieces(m):
            sends.put(origin(m, t % 2, u), spot(m, me, u), sem_of(m, me, u), {"fs": t * sz + col})

    def stage1(n):
        m, p = steps[n]
        src = plane(p) * sz + col
        if p:
            came(m, src)
        for u in pieces(m):
            for nb in (xn, yn):
                first = spot(m, src, u) if p else origin(m, z % 2, u)
                sends.put(first, spot(m, src, u), sem_of(m, src, u), {"fs": nb})
            if not p:
                key = local_sem.at[0] if m == 3 else loc_ff.at[m, u]
                local((m, u), origin(m, z % 2, u), spot(m, me, u), key)

    def shard(m, src):
        if m < 2:
            return weights[m][1].at[pl.ds(mo(src * depth, 16), depth), :]
        return down_v.at[src] if m < 3 else spot(m, src, 0)

    def came(m, src):
        arrived(shard(m, src), ff_sem.at[m, src])

    def three(p):
        shift = plane(p) * sz - z * sz
        return xn + shift, yn + shift, dg + shift

    def relay(m, p, u, across):
        a, b, _ = three(p)
        src, to = (a, yn) if across else (b, xn)
        came(m, src)
        sends.put(spot(m, src, u), spot(m, src, u), sem_of(m, src, u), {"fs": to})

    def stage2(n):
        m, p = steps[n]
        if m < 3:
            relay(m, p, 0, True)
            relay(m, p, 1, False)
        else:
            relay(m, p, 0, p % 2 == 0)

    def stage3(n):
        m, p = steps[n]
        a, b, d = three(p)
        if m == 3:
            came(m, b if p % 2 == 0 else a)
        came(m, d)
        if p == 0:
            for u in pieces(m):
                locals_[(m, u)].wait()

    def mix_at(k, src):
        if k == 0:
            return min_v.at[pl.ds(mo(src * depth, 16), depth), :]
        return mout_v.at[src, early_rows, :]

    mixes = (mix_in, mix_out.at[early_rows, :])

    def mix_own():
        for k, ref in enumerate(mixes):
            for nb in (xn, yn):
                sends.put(ref, mix_at(k, me), mix_sem.at[k, me], {"fs": nb})
            local(("mix", k), ref, mix_at(k, me), loc_ff.at[3, k])

    def mix_turn():
        for k, (src, to) in enumerate(((xn, yn), (yn, xn))):
            arrived(mix_at(k, src), mix_sem.at[k, src])
            sends.put(mix_at(k, src), mix_at(k, src), mix_sem.at[k, src], {"fs": to})

    def mix_up():
        for k, src in enumerate((yn, xn)):
            arrived(mix_at(k, src), mix_sem.at[k, src])
        for k in range(2):
            arrived(mix_at(k, dg), mix_sem.at[k, dg])
            locals_[("mix", k)].wait()
            for src in (me, xn, yn, dg):
                here = mix_at(k, src)
                for step in (1, -1):
                    ok = jnp.logical_and(z + step >= 0, z + step < nz)
                    sends.put(here, here, mix_sem.at[k, src], {"fs": me + step * sz}, ok)

    def mix_on(p, forward=True):
        found, away = near(z, nz, p)
        shift = (found - z) * sz
        inside = jnp.logical_and(z + away >= 0, z + away < nz)
        for k in range(2):
            for src in (me + shift, xn + shift, yn + shift, dg + shift):
                here, sem = mix_at(k, src), mix_sem.at[k, src]
                if forward:
                    when(inside, functools.partial(arrived, here, sem))
                    sends.put(here, here, sem, {"fs": me + away * sz}, inside)
                else:
                    when(jnp.logical_not(inside), functools.partial(arrived, here, sem))

    mine = pl.ds(mo(core * half, 16), half)
    theirs = pl.ds(mo((1 - core) * half, 16), half)
    mine_far = pl.ds(mo(rows + core * half, 16), half)
    theirs_far = pl.ds(mo(rows + (1 - core) * half, 16), half)
    partner = {"tp": 1 - core}
    buddy = {"fs": peer}

    def tokens_out():
        sends.put(tokens.at[mine, :], tok_v.at[mine_far, :], act_sem.at[0], buddy)
        local("tok", tokens, tok_v.at[pl.ds(0, rows), :], local_sem.at[1])

    def tokens_on():
        here = tok_v.at[mine_far, :]
        arrived(here, act_sem.at[0])
        sends.put(here, here, act_sem.at[1], partner)

    def first_norm():
        arrived(tok_v.at[theirs_far, :], act_sem.at[1])
        locals_["tok"].wait()

        def block(i, carry):
            at = pl.ds(pl.multiple_of(i * 32, 32), 32)
            v = tok_v[at, :].astype(F32)
            norm_v[at, :] = rms_value(v, gains[0:1, :]).astype(BF16)
            return carry

        lax.fori_loop(0, 2 * rows // 32, block, 0)

    def gate_up(src, at, dst):
        def tile(cols, n):
            w = jnp.concatenate([gate_v[:, cols], up_v[:, cols]], axis=1)
            both = jnp.dot(src[at, :], w, preferred_element_type=F32)
            hid_v[dst, cols] = (silu(both[:, :n]) * both[:, n:]).astype(BF16)

        whole = hid // 256

        def body(j, carry):
            tile(pl.ds(pl.multiple_of(j * 256, 256), 256), 256)
            return carry

        lax.fori_loop(0, whole, body, 0)
        if hid % 256:
            tile(pl.ds(whole * 256, hid % 256), hid % 256)

    def down_block(first, many, at):
        w = jnp.concatenate([down_v[first + i] for i in range(many)], axis=1)
        return jnp.dot(hid_v[at, :], w, preferred_element_type=F32).astype(BF16)

    def cols_of(first, many):
        return pl.ds(mo(first * wide, 128), many * wide)

    def down1(first, many, sem):
        cols = cols_of(first, many)
        for i, (base, other) in enumerate(((rows, theirs_far), (0, theirs))):
            at = pl.ds(base, rows)
            part_v[at, cols] = down_block(first, many, at)
            sends.put(part_v.at[other, cols], got1.at[1 - i, :, cols], act_sem.at[sem + i], partner)

    def reduce1(first, many, sem):
        cols = cols_of(first, many)
        for i in range(2):
            arrived(got1.at[1 - i, :, cols], act_sem.at[sem + i])
        total = part_v[mine_far, cols].astype(F32) + got1[1, :, cols].astype(F32)
        sum1[:, cols] = total.astype(BF16)
        sends.put(sum1.at[:, cols], far1.at[:, cols], sum_sem(first, many), buddy)

    row_y = (me // sy) % 2

    def near_pair(p):
        return plane(p) * sz + row_y * sy

    def far_pair(p):
        return plane(p) * sz + (1 - row_y) * sy

    def sum_sem(first, many):
        t = first // sz
        return act_sem.at[29 + 2 * t + ((first // sy) % 2 if many < sz else 0)]

    def first_stream():
        buddy_z = z + sign
        for p in range(nz):
            t = near(buddy_z, nz, p)[0] if p else buddy_z
            if p < nz - 1:
                cols = cols_of(t * sz, sz)
                arrived(far1.at[:, cols], sum_sem(t * sz, sz))
            else:
                for k in range(2):
                    cols = cols_of(t * sz + k * sy, sy)
                    arrived(far1.at[:, cols], sum_sem(t * sz + k * sy, sy))
        for start, size in runs(0, half):
            r = pl.ds(start, size)
            at = pl.ds(pl.multiple_of(core * half + start, 16), size)
            y = part_v[at, :].astype(F32) + got1[0, r, :].astype(F32) + far1[r, :].astype(F32)
            s = tok_v[at, :].astype(F32) + 0.5 * rms_value(y, gains[1:2, :])
            stream_v[r, :] = s
            mid_v[at, :] = rms_value(s, gains[2:3, :]).astype(BF16)
        sends.put(mid_v.at[mine, :], mid_v.at[mine, :], act_sem.at[2], partner)

    def into_pool(at):
        v = jnp.dot(mid_v[at, :], min_v[...], preferred_element_type=F32)
        pin_v[at, :] = v.astype(BF16).astype(F32)

    def pool():
        length = LEN
        groups, dim = pool_w.shape[0], pool_w.shape[1]
        t = lax.broadcasted_iota(jnp.int32, (rows, dim), 0) % length
        for g in range(groups):
            cols = slice(g * dim, (g + 1) * dim)
            v = pin_v[:, cols]
            window = 2 ** (1 + g % 4)
            total, k = v, 1
            while k < window:
                total = total + jnp.where(t >= k, pltpu.roll(total, k, 0), 0.0)
                k *= 2
            count = jnp.minimum(t + 1, window).astype(F32)
            dev = (total / count - v).astype(BF16)
            o = jnp.dot(dev, pool_w[g], preferred_element_type=F32)
            o = o * pool_scale[cols].astype(F32).reshape(1, dim)
            rg_v[:, cols] = o.astype(BF16)

    def out_pool(at):
        for t in range(nz):
            w = jnp.concatenate([mout_v[t * sz + i] for i in range(sz)], axis=1)
            v = jnp.dot(rg_v[at, :], w, preferred_element_type=F32)
            partm_v[at, pl.ds(t * span, span)] = v.astype(BF16)

    units = half // 16
    most = -(-units * 2 // 5)
    firsts = [min(most * k, units) * 16 for k in range(4)]
    chunks = [(a, b - a) for a, b in zip(firsts[:-1], firsts[1:]) if b > a]

    def second_stream():
        for k, (first, count) in enumerate(chunks):
            arrived(gotm.at[pl.ds(first, count), :], act_sem.at[14 + k])
            for start, size in runs(first, count):
                r = pl.ds(start, size)
                at = pl.ds(pl.multiple_of(core * half + start, 16), size)
                y = partm_v[at, :].astype(F32) + gotm[r, :].astype(F32)
                s = stream_v[r, :] + rms_value(y, gains[3:4, :])
                stream_v[r, :] = s
                own_v[at, :] = rms_value(s, gains[4:5, :]).astype(BF16)
            src = own_v.at[pl.ds(mo(core * half + first, 16), count), :]
            sends.put(src, far_at(k, core), act_sem.at[17 + k], buddy)
            sends.put(src, src, act_sem.at[29 + 2 * nz + k], partner)

    def far_rows(k, c):
        first, count = chunks[k]
        return mo(2 * first + c * count, 16), count

    def far_at(k, c):
        return far_v.at[pl.ds(*far_rows(k, c)), :]

    def far_on(k):
        arrived(far_at(k, core), act_sem.at[17 + k])
        sends.put(far_at(k, core), far_at(k, core), act_sem.at[20 + k], partner)

    def down2(base, count, low, high):
        at = pl.ds(base, count)

        def body(t, carry):
            part2_v[at, pl.ds(pl.multiple_of(t * span, 128), span)] = down_block(t * sz, sz, at)
            return carry

        lax.fori_loop(low, high, body, 0)

    def far_part(k, c):
        first, count = far_rows(k, c)
        return pl.ds(mo(rows + first, 16), count)

    last = len(steps)
    stage1(0)
    for n in range(2, 6):
        stage0(n)
    stage1(1)
    mix_own()
    tokens_out()
    stage2(0)
    stage2(1)
    all_mine = pl.ds(0, rows)
    all_far = pl.ds(rows, rows)

    z_order = {0: (6, 7), 2: (9,), 3: (10, 11)}
    z_order.update({2 * nz - 1 + k: (3 * nz + 1 + k,) for k in range(nz - 1)})

    def advance(i):
        for n in z_order.get(i, ()):
            stage0(n)
        if i + 2 < last:
            stage1(i + 2)
        if 0 < i < last - 1:
            stage2(i + 1)
        stage3(i)

    final = 3 * nz - 1
    for i in range(final):
        advance(i)
        if i == 0:
            mix_turn()
        if i == 1:
            mix_up()
        if i == 2:
            tokens_on()
        if i == 4:
            first_norm()
        for p, when_on in enumerate((5, 6)):
            if i == when_on:
                mix_on(p + 1)
        if i == 2 * nz - 1:
            gate_up(norm_v, all_mine, all_mine)
        if i == 2 * nz:
            gate_up(norm_v, all_far, all_far)
            for p in range(3, nz):
                mix_on(p)
            down1(plane(0) * sz, sz, 4)
        if i == 2 * nz + 1:
            down1(plane(1) * sz, sz, 6)
            reduce1(plane(0) * sz, sz, 4)
        if i == 2 * nz + 2:
            down1(plane(2) * sz, sz, 8)
            reduce1(plane(1) * sz, sz, 6)
    late = range(3 * nz, last)
    for n in late[2:]:
        stage1(n - 1)
    stage1(last - 1)
    stage2(late[0])
    d = three(nz - 1)[2]
    down1(near_pair(nz - 1), sy, 10)
    reduce1(plane(2) * sz, sz, 8)
    came(2, d)
    down1(far_pair(nz - 1), sy, 12)
    reduce1(near_pair(nz - 1), sy, 10)
    stage2(late[1])
    reduce1(far_pair(nz - 1), sy, 12)
    for n in late[2:]:
        stage2(n)
    for p in range(1, nz):
        mix_on(p, forward=False)
    first_stream()
    into_pool(mine)
    arrived(mid_v.at[theirs, :], act_sem.at[2])
    into_pool(theirs)
    pool()
    for n in late:
        stage3(n)
    out_pool(theirs)
    for k, (first, count) in enumerate(chunks):
        src = partm_v.at[pl.ds(mo((1 - core) * half + first, 16), count), :]
        sends.put(src, gotm.at[pl.ds(first, count), :], act_sem.at[14 + k], partner)
    out_pool(mine)
    second_stream()

    def far_product(k):
        first, count = chunks[k]
        arrived(far_at(k, 1 - core), act_sem.at[20 + k])
        gate_up(far_v, pl.ds(2 * first, 2 * count), pl.ds(rows + 2 * first, 2 * count))
        if 0 < k < len(chunks) - 1:
            far_on(k + 1)
        down2(rows + 2 * first, 2 * count, 0, nz)
        here = got2f.at[pl.ds(first, count), :]
        sends.put(part2_v.at[far_part(k, 1 - core), :], here, act_sem.at[23 + k], partner)

    def far_sum(k):
        here = pl.ds(*chunks[k])
        arrived(got2f.at[here, :], act_sem.at[23 + k])
        total = part2_v[far_part(k, core), :].astype(F32) + got2f[here, :].astype(F32)
        sum2[here, :] = total.astype(BF16)
        sends.put(sum2.at[here, :], far2.at[here, :], act_sem.at[26 + k], buddy)

    for k, (first, count) in enumerate(chunks):
        here = pl.ds(mo((1 - core) * half + first, 16), count)
        arrived(own_v.at[here, :], act_sem.at[29 + 2 * nz + k])
    gate_up(own_v, all_mine, all_mine)
    far_on(0)
    down2(0, rows, 0, nz // 2)
    far_product(0)
    far_on(1)
    down2(0, rows, nz // 2, nz)
    sends.put(part2_v.at[theirs, :], got2o, act_sem.at[3], partner)
    far_sum(0)
    for k in range(1, len(chunks)):
        far_product(k)
        far_sum(k)
    arrived(got2o, act_sem.at[3])
    for k, (first, count) in enumerate(chunks):
        arrived(far2.at[pl.ds(first, count), :], act_sem.at[26 + k])
        for start, size in runs(first, count):
            r = pl.ds(start, size)
            at = pl.ds(pl.multiple_of(core * half + start, 16), size)
            y = part2_v[at, :].astype(F32) + got2o[r, :].astype(F32) + far2[r, :].astype(F32)
            s = stream_v[r, :] + 0.5 * rms_value(y, gains[5:6, :])
            out_v[r, :] = s.astype(BF16)
    leave = pltpu.make_async_copy(out_v, out, local_sem.at[2])
    leave.start()
    sends.drain()
    leave.wait()


def whole_layer(dims, tokens, w_gate, w_up, w_down, w_mix_in, w_mix_out, pool_w, pool_scale, gains):
    count = 1
    for size, _ in dims:
        count *= size
    nz = dims[0][0]
    depth, units = w_gate.shape
    hid = units // 2
    rows, feat = tokens.shape
    half = rows // 2
    wide = w_down.shape[1]
    pooled = w_mix_in.shape[1]

    def buf(*shape, dtype=BF16):
        return pltpu.VMEM(shape, dtype)

    scratch = [
        buf(count * depth, hid),
        buf(count * depth, hid),
        buf(count, hid, wide),
        buf(count * depth, pooled),
        buf(count, w_mix_out.shape[0], wide),
        buf(2 * rows, feat),
        buf(2 * rows, feat),
        buf(rows, feat),
        buf(rows, feat),
        buf(2 * rows, hid),
        buf(2 * rows, feat),
        buf(2 * rows, feat),
        buf(rows, feat),
        buf(2, half, feat),
        buf(half, feat),
        buf(half, feat),
        buf(half, feat),
        buf(half, feat),
        buf(half, feat),
        buf(half, feat),
        buf(half, feat),
        buf(half, feat, dtype=F32),
        buf(rows, feat),
        buf(rows, pooled, dtype=F32),
        buf(rows, pooled),
        buf(half, feat),
        pltpu.SemaphoreType.DMA((SENDS,)),
        pltpu.SemaphoreType.DMA((4, count)),
        pltpu.SemaphoreType.DMA((2, count)),
        pltpu.SemaphoreType.DMA((32 + 2 * nz,)),
        pltpu.SemaphoreType.DMA((4,)),
        pltpu.SemaphoreType.DMA((4, 2)),
    ]
    hbm = pl.BlockSpec(memory_space=pltpu.HBM)
    vmem = pl.BlockSpec(memory_space=pltpu.VMEM)
    return pl.pallas_call(
        functools.partial(layer_kernel, dims),
        out_shape=jax.ShapeDtypeStruct((half, feat), tokens.dtype),
        in_specs=[hbm] * 6 + [vmem] * 3,
        out_specs=hbm,
        scratch_shapes=scratch,
        compiler_params=pltpu.CompilerParams(
            collective_id=1, has_side_effects=True, vmem_limit_bytes=67043328
        ),
        name="whole_layer",
    )(tokens, w_gate, w_up, w_down, w_mix_in, w_mix_out, pool_w, pool_scale, gains)


def paired(dims, mesh):
    return (
        len(dims) == 3
        and dims[0][0] == 4
        and dims[1][0] == 2
        and dims[2][0] == 2
        and mesh.shape["tp"] == 2
    )


def solution(mesh):
    in_specs = (
        P("fs", None),
        P("fs", "tp"),
        P("fs", "tp"),
        P("tp", "fs"),
        P("fs", "tp"),
        P("tp", "fs"),
        P("tp", None, None),
        P("tp"),
        P(),
    )
    out_specs = P(("fs", "tp"), None)
    dims = line_dims(mesh)
    act = whole_layer if paired(dims, mesh) else body
    return jax.shard_map(
        functools.partial(act, dims), mesh=mesh, in_specs=in_specs, out_specs=out_specs, check_vma=False
    )
```

```python
import functools
import itertools

import jax
import jax.numpy as jnp
from jax import lax
from jax.experimental import pallas as pl
from jax.experimental.pallas import tpu as pltpu
from jax.sharding import PartitionSpec as P

LEN = 64
MESH = pl.DeviceIdType.MESH


def line_dims(mesh):
    devices = mesh.devices.reshape(mesh.shape["fs"], -1)[:, 0]
    count = len(devices)
    coords = [tuple(getattr(d, "coords", ())) for d in devices]
    dims = []
    for axis in range(len(coords[0])):
        values = sorted({c[axis] for c in coords})
        if len(values) > 1:
            stride = next(i for i in range(count) if coords[i][axis] != coords[0][axis])
            dims.append((len(values), stride, axis, values))
    dims.sort(key=lambda d: -d[1])
    good = len(dims) > 0 and all(
        sum(vals.index(c[axis]) * stride for _, stride, axis, vals in dims) == i
        for i, c in enumerate(coords)
    )
    if not good:
        return ((count, 1),)
    return tuple((d[0], d[1]) for d in dims)


def near(position, size, rank):
    inner = jnp.minimum(position, size - 1 - position)
    alternating = rank <= 2 * inner
    distance = jnp.where(alternating, (rank + 1) // 2, rank - inner)
    toward_high = jnp.where(alternating, rank % 2 == 1, 2 * position < size - 1)
    step = jnp.where(toward_high, 1, -1)
    return position + step * distance, -step


def piece_plan(dims, order):
    sizes = [dims[d][0] for d in order]
    slots = []
    for ranks in itertools.product(*[range(n) for n in sizes]):
        slots.append(ranks)
    slots.sort(key=lambda r: (sum(r), r))
    return slots


class Piece:
    def __init__(self, index, dims, order, src_of, dst_of):
        self.index, self.dims, self.order = index, dims, order
        self.src_of, self.dst_of = src_of, dst_of
        self.slots = piece_plan(dims, order)

    def locate(self, me, ranks):
        source, last, away = me, -1, None
        for place, (d, rank) in enumerate(zip(self.order, ranks)):
            if rank > 0:
                size, stride = self.dims[d]
                position = (me // stride) % size
                found, step = near(position, size, rank)
                source = source + (found - position) * stride
                last, away = place, step
        return source, last, away

    def sends(self, me, ranks):
        _, last, away = self.locate(me, ranks)
        out = []
        for place, d in enumerate(self.order):
            size, stride = self.dims[d]
            position = (me // stride) % size
            if place == last:
                if size > 2:
                    ok = jnp.logical_and(position + away >= 0, position + away < size)
                    out.append((ok, me + away * stride))
            elif place > last:
                if size == 2:
                    out.append((None, me + (1 - 2 * position) * stride))
                else:
                    out.append((position + 1 < size, me + stride))
                    out.append((position > 0, me - stride))
        return out


def when(condition, act):
    if condition is None:
        act()
    else:
        pl.when(condition)(act)


def spread(pieces, me, chunk, send_sem, recv_sem, low, high, mode):
    todo = []
    for piece in pieces:
        for ranks in piece.slots:
            todo.append((sum(ranks), piece, ranks))
    todo.sort(key=lambda t: t[0])
    for depth, piece, ranks in todo:
        if not low <= depth < high:
            continue
        source, last, _ = piece.locate(me, ranks)
        landed = piece.dst_of(chunk, source)
        origin = piece.src_of(chunk) if depth == 0 else landed
        recv = recv_sem.at[chunk, piece.index, source]
        if depth > 0 and mode == "start":
            pltpu.make_async_copy(landed, landed, recv).wait()
        base = piece.first_send[ranks]
        for offset, (ok, target) in enumerate(piece.sends(me, ranks)):
            copy = pltpu.make_async_remote_copy(
                src_ref=origin,
                dst_ref=landed,
                send_sem=send_sem.at[chunk, base + offset],
                recv_sem=recv,
                device_id={"fs": target},
                device_id_type=MESH,
            )
            when(ok, copy.start if mode == "start" else copy.wait_send)


def number_sends(pieces):
    total = 0
    for piece in pieces:
        piece.first_send = {}
        for ranks in piece.slots:
            piece.first_send[ranks] = total
            last = max([i for i, r in enumerate(ranks) if r > 0], default=-1)
            for place, d in enumerate(piece.order):
                size = piece.dims[d][0]
                if place == last:
                    total += 1 if size > 2 else 0
                elif place > last:
                    total += 1 if size == 2 else 2
    return total


def cut(extent, unit, share):
    return max(unit, min(extent - unit, round(extent * share / unit) * unit))


def gather_plan(dims, refs, outs, blocks):
    gate, up, down, mix_in, mix_out = refs
    gate_o, up_o, down_o, mix_in_o, mix_out_o = outs
    n = len(dims)
    first = tuple(range(n))
    second = first[1:] + first[:1]
    third = first[-1:] + first[:-1]
    pooled = mix_out.shape[0]

    def rows(ref, out, start_of, size):
        return (
            lambda c: ref.at[pl.ds(start_of(c), size), :],
            lambda c, s: out.at[s, pl.ds(start_of(c), size), :],
        )

    def at(block, offset):
        return lambda c: pl.multiple_of(c * block + offset, 16)

    block, tall = gate.shape[0] // blocks, down.shape[0] // blocks
    down_cut = cut(tall, 16, 2 / 3)
    main = [
        Piece(0, dims, first, *rows(gate, gate_o, at(block, 0), block)),
        Piece(1, dims, third, *rows(up, up_o, at(block, 0), block)),
        Piece(2, dims, first, *rows(down, down_o, at(tall, 0), down_cut)),
        Piece(3, dims, second, *rows(down, down_o, at(tall, down_cut), tall - down_cut)),
    ]
    mix_cut = cut(pooled, 16, 2 / 3)

    def fixed(offset):
        return lambda c: offset

    mix = [
        Piece(0, dims, first, *rows(mix_in, mix_in_o, fixed(0), mix_in.shape[0])),
        Piece(1, dims, third, *rows(mix_out, mix_out_o, fixed(0), mix_cut)),
        Piece(2, dims, second, *rows(mix_out, mix_out_o, fixed(mix_cut), pooled - mix_cut)),
    ]
    return main, mix


def gather_kernel(dims, blocks, *args):
    refs, outs = args[:5], args[5:10]
    beside = None
    if len(args) > 13:
        beside = args[10:12]
        args = args[:10] + args[12:]
    send_sem, recv_sem, local_sem = args[10:13]
    me = lax.axis_index("fs")
    barrier = pltpu.get_barrier_semaphore()
    expected = 0
    for size, stride in dims:
        position = (me // stride) % size
        for step, ok in ((1, position + 1 < size), (-1, position > 0)):
            def signal(step=step, stride=stride):
                pl.semaphore_signal(
                    barrier, inc=1, device_id={"fs": me + step * stride}, device_id_type=MESH
                )

            pl.when(ok)(signal)
            expected = expected + jnp.where(ok, 1, 0)
    pl.semaphore_wait(barrier, expected)

    main, mix = gather_plan(dims, refs, outs, blocks)
    number_sends(main)
    number_sends(mix)
    deepest = sum(size - 1 for size, _ in dims) + 1
    early = min(3, deepest)

    locals_ = []
    for i, (ref, out) in enumerate(zip(refs, outs)):
        if beside is not None and i in (2, 4):
            continue
        locals_.append(pltpu.make_async_copy(ref, out.at[me], local_sem.at[i]))

    go = functools.partial(spread, send_sem=send_sem, recv_sem=recv_sem)
    def shard_in(source, stage, sem, shard, across):
        return pltpu.make_async_copy(
            source, stage.at[:, pl.ds(shard * across, across)], sem.at[shard]
        )

    def lay_in(own, part, stage, sem, rows, height):
        for shard in range(part.shape[0]):
            for mine, source in ((True, own), (False, part.at[shard])):

                @pl.when((me == shard) if mine else (me != shard))
                def _(source=source, shard=shard):
                    piece = source.at[pl.ds(rows, height), :]
                    shard_in(piece, stage, sem, shard, part.shape[2]).start()

    def lay_out(part, whole, stage, sem, rows, height, mode):
        if mode == "start":
            for shard in range(part.shape[0]):
                piece = part.at[shard, pl.ds(rows, height), :]
                shard_in(piece, stage, sem, shard, part.shape[2]).wait()
        copy = pltpu.make_async_copy(
            stage, whole.at[pl.ds(rows, height), :], sem.at[part.shape[0]]
        )
        copy.start() if mode == "start" else copy.wait()

    if beside is not None:
        down_stage, mix_stage, down_sem, mix_sem = args[13:]
        tall = down_stage.shape[1]

        pooled = mix_stage.shape[0]

    def rows_of(c):
        return c * tall if isinstance(c, int) else pl.multiple_of(c * tall, 16)

    def down_in(c):
        slot = c % 2
        lay_in(refs[2], outs[2], down_stage.at[slot], down_sem.at[slot], rows_of(c), tall)

    def down_out(c, mode="start"):
        slot = c % 2
        lay_out(outs[2], beside[0], down_stage.at[slot], down_sem.at[slot], rows_of(c), tall, mode)

    go(mix, me, blocks, low=0, high=1, mode="start")
    go(main, me, 0, low=0, high=1, mode="start")
    for copy in locals_:
        copy.start()
    go(mix, me, blocks, low=1, high=deepest, mode="start")
    if beside is not None:
        lay_in(refs[4], outs[4], mix_stage, mix_sem, 0, pooled)

    def step(i, carry):
        @pl.when(i + 1 < blocks)
        def _():
            go(main, me, i + 1, low=0, high=1, mode="start")

        go(main, me, i, low=1, high=early, mode="start")

        @pl.when(i > 0)
        def _():
            go(main, me, i - 1, low=early, high=deepest, mode="start")

        if beside is not None:

            @pl.when(i > 2)
            def _():
                down_out(i - 3, "end")

            @pl.when(i > 0)
            def _():
                down_in(i - 1)

            @pl.when(i > 1)
            def _():
                down_out(i - 2)

        return carry

    lax.fori_loop(0, blocks, step, 0)
    go(main, me, blocks - 1, low=early, high=deepest, mode="start")
    if beside is not None:
        if blocks > 2:
            down_out(blocks - 3, "end")
        down_in(blocks - 1)
        if blocks > 1:
            down_out(blocks - 2)
        lay_out(outs[4], beside[1], mix_stage, mix_sem, 0, pooled, "start")
        down_out(blocks - 1)

    def finish(i, carry):
        go(main, me, i, low=0, high=deepest, mode="end")
        return carry

    lax.fori_loop(0, blocks, finish, 0)
    go(mix, me, blocks, low=0, high=deepest, mode="end")
    if beside is not None:
        if blocks > 1:
            down_out(blocks - 2, "end")
        down_out(blocks - 1, "end")
        lay_out(outs[4], beside[1], mix_stage, mix_sem, 0, pooled, "end")
    for copy in locals_:
        copy.wait()


def gather_weights(dims, w_gate, w_up, w_down, w_mix_in, w_mix_out):
    count = 1
    for size, _ in dims:
        count *= size
    tiles = (w_gate.shape[0] // 16, w_down.shape[0] // 16)
    blocks = next(b for b in (8, 4, 2, 1) if tiles[0] % b == 0 and tiles[1] % b == 0)
    weights = (w_gate, w_up, w_down, w_mix_in, w_mix_out)
    shapes = [jax.ShapeDtypeStruct((count, *a.shape), a.dtype) for a in weights]

    class Shape:
        def __init__(self, shape):
            self.shape = shape

    stand_in = [Shape(a.shape) for a in weights]
    main, mix = gather_plan(dims, stand_in, [Shape(s.shape) for s in shapes], blocks)
    sends = max(number_sends(main), number_sends(mix))
    scratch = [
        pltpu.SemaphoreType.DMA((blocks + 1, sends)),
        pltpu.SemaphoreType.DMA((blocks + 1, len(main), count)),
        pltpu.SemaphoreType.DMA((5,)),
    ]
    laid = w_down.shape[1] % 128 == 0
    if laid:
        tall, full = w_down.shape[0] // blocks, w_down.shape[1] * count
        shapes += [jax.ShapeDtypeStruct((a.shape[0], full), a.dtype) for a in (w_down, w_mix_out)]
        scratch += [
            pltpu.VMEM((2, tall, full), w_down.dtype),
            pltpu.VMEM((w_mix_out.shape[0], full), w_mix_out.dtype),
            pltpu.SemaphoreType.DMA((2, count + 1)),
            pltpu.SemaphoreType.DMA((count + 1,)),
        ]
    outs = pl.pallas_call(
        functools.partial(gather_kernel, dims, blocks),
        out_shape=shapes,
        in_specs=[pl.BlockSpec(memory_space=pltpu.HBM)] * 5,
        out_specs=[pl.BlockSpec(memory_space=pltpu.HBM)] * len(shapes),
        scratch_shapes=scratch,
        compiler_params=pltpu.CompilerParams(collective_id=0, has_side_effects=True),
        name="gather_weights",
    )(*weights)

    def stacked(a):
        return a.reshape(-1, a.shape[2])

    def beside(a):
        return jnp.transpose(a, (1, 0, 2)).reshape(a.shape[1], -1)

    gate, up, down, mix_in, mix_out = outs[:5]
    if laid:
        return stacked(gate), stacked(up), outs[5], stacked(mix_in), outs[6]
    return stacked(gate), stacked(up), beside(down), stacked(mix_in), beside(mix_out)


def rms_scale(values, gain):
    return values * lax.rsqrt(jnp.mean(values * values, axis=-1, keepdims=True) + 1e-06) * gain


def total_over_tp(left_rows, right_matrix):
    part = jnp.dot(left_rows, right_matrix, preferred_element_type=jnp.float32)
    part = part.astype(jnp.bfloat16)
    if lax.axis_size("tp") == 2:
        other = lax.ppermute(part, "tp", ((0, 1), (1, 0)))
        return part.astype(jnp.float32) + other.astype(jnp.float32)
    return lax.psum(part.astype(jnp.float32), "tp")


def own_total_over_tp(left_rows, right_matrix):
    part = jnp.dot(left_rows, right_matrix, preferred_element_type=jnp.float32)
    part = part.astype(jnp.bfloat16)
    if lax.axis_size("tp") == 2:
        mine = own_rows_of(part)
        half = mine.shape[0]
        theirs = lax.dynamic_slice_in_dim(part, (1 - lax.axis_index("tp")) * half, half, 0)
        other = lax.ppermute(theirs, "tp", ((0, 1), (1, 0)))
        return mine.astype(jnp.float32) + other.astype(jnp.float32)
    return lax.psum_scatter(part.astype(jnp.float32), "tp", scatter_dimension=0, tiled=True)


def own_rows_of(array):
    count = array.shape[0] // lax.axis_size("tp")
    return lax.dynamic_slice_in_dim(array, lax.axis_index("tp") * count, count, 0)


def body(dims, tokens, w_gate, w_up, w_down, w_mix_in, w_mix_out, pool_w, pool_scale, norm_gains):
    rows_all = tokens.shape[0]
    stream = tokens.astype(jnp.float32)
    normed = rms_scale(stream, norm_gains[0]).astype(jnp.bfloat16)
    gate_full, up_full, down_full, mix_in_full, mix_out_full = gather_weights(
        dims, w_gate, w_up, w_down, w_mix_in, w_mix_out
    )
    gate_first = jnp.dot(normed, gate_full, preferred_element_type=jnp.float32)
    up_first = jnp.dot(normed, up_full, preferred_element_type=jnp.float32)
    hidden = (jax.nn.silu(gate_first) * up_first).astype(jnp.bfloat16)
    stream = stream + 0.5 * rms_scale(total_over_tp(hidden, down_full), norm_gains[1])
    normed = rms_scale(stream, norm_gains[2]).astype(jnp.bfloat16)
    pooled_in = jnp.dot(normed, mix_in_full, preferred_element_type=jnp.float32)
    pooled_in = pooled_in.astype(jnp.bfloat16)
    groups_here = pool_w.shape[0]
    group_dim = pool_w.shape[1]
    values = pooled_in.astype(jnp.float32).reshape(rows_all // LEN, LEN, groups_here, group_dim)
    totals = jnp.cumsum(values, axis=1)
    position = jnp.arange(1, LEN + 1).astype(jnp.float32)[None, :, None, None]
    window_ids = (lax.axis_index("tp") * groups_here + jnp.arange(groups_here)) % 4
    average = jnp.zeros_like(values)
    for window_slot in range(4):
        window = 2 ** (1 + window_slot)
        lagged = jnp.pad(totals, ((0, 0), (window, 0), (0, 0), (0, 0)))[:, :LEN]
        candidate = (totals - lagged) / jnp.minimum(position, float(window))
        average = jnp.where((window_ids == window_slot)[None, None, :, None], candidate, average)
    deviation = (average - values).astype(jnp.bfloat16)
    regrouped = jnp.einsum("btgi,gio->btgo", deviation, pool_w, preferred_element_type=jnp.float32)
    regrouped = (
        regrouped.reshape(rows_all, groups_here * group_dim) * pool_scale.astype(jnp.float32)
    ).astype(jnp.bfloat16)
    stream = stream + rms_scale(total_over_tp(regrouped, mix_out_full), norm_gains[3])
    normed = rms_scale(stream, norm_gains[4]).astype(jnp.bfloat16)
    gate_second = jnp.dot(normed, gate_full, preferred_element_type=jnp.float32)
    up_second = jnp.dot(normed, up_full, preferred_element_type=jnp.float32)
    hidden = (jax.nn.silu(gate_second) * up_second).astype(jnp.bfloat16)
    stream_own = own_rows_of(stream)
    stream_own = stream_own + 0.5 * rms_scale(own_total_over_tp(hidden, down_full), norm_gains[5])
    return stream_own.astype(jnp.bfloat16)


def silu(v):
    return v / (1.0 + jnp.exp(-v))


def rms_value(values, gain):
    return values * lax.rsqrt(jnp.mean(values * values, axis=-1, keepdims=True) + 1e-06) * gain


def runs(first, count, most=32):
    out, at = [], first
    while at < first + count:
        size = min(most, first + count - at)
        out.append((at, size))
        at += size
    return out


class Sends:
    def __init__(self, sem):
        self.sem, self.count, self.pending = sem, 0, {}

    def put(self, src, dst, recv, to, ok=None):
        slot = self.count % SENDS
        self.count += 1
        self.settle(slot)
        copy = pltpu.make_async_remote_copy(
            src_ref=src,
            dst_ref=dst,
            send_sem=self.sem.at[slot],
            recv_sem=recv,
            device_id=to,
            device_id_type=MESH,
        )
        when(ok, copy.start)
        self.pending[slot] = (ok, copy)

    def settle(self, slot):
        if slot in self.pending:
            ok, copy = self.pending.pop(slot)
            when(ok, copy.wait_send)

    def drain(self):
        for slot in list(self.pending):
            self.settle(slot)


SENDS = 48
F32, BF16 = jnp.float32, jnp.bfloat16


def layer_kernel(dims, *refs):
    (tokens, gate, up, down, mix_in, mix_out, pool_far, scale_far, gains_far, out) = refs[:10]
    (gate_v, up_v, down_v, min_v, mout_v) = refs[10:15]
    (tok_v, norm_v, own_v, far_v, hid_v, part_v, part2_v, partm_v) = refs[15:23]
    (got1, got2o, got2f, gotm, sum1, sum2, far1, far2) = refs[23:31]
    (stream_v, mid_v, pin_v, rg_v, out_v) = refs[31:36]
    (pool_w, pool_scale, gains) = refs[36:39]
    (send_sem, ff_sem, mix_sem, act_sem, local_sem, loc_ff) = refs[39:]
    (nz, sz), (_, sy), (_, sx) = dims
    me, core = lax.axis_index("fs"), lax.axis_index("tp")
    z = me // sz
    col = me - z * sz
    xn = me + (1 - 2 * ((me // sx) % 2)) * sx
    yn = me + (1 - 2 * ((me // sy) % 2)) * sy
    dg = xn + yn - me
    sign = 1 - 2 * (z % 2)
    peer = me + sign * sz
    depth = gate.shape[0]
    hid = gate_v.shape[1]
    rows = tokens.shape[0]
    half = rows // 2
    wide = down.shape[1]
    feat = tokens.shape[1]
    span = sz * wide

    barrier = pltpu.get_barrier_semaphore()
    friends = [({"fs": xn}), ({"fs": yn}), ({"tp": 1 - core})]
    for k in range(1, nz):
        friends.append({"fs": lax.rem(z + k, nz) * sz + col})
    for to in friends:
        pl.semaphore_signal(barrier, inc=1, device_id=to, device_id_type=MESH)
    pl.semaphore_wait(barrier, len(friends))

    sends = Sends(send_sem)

    def mo(v, n):
        return v if isinstance(v, int) else pl.multiple_of(v, n)

    def plane(p):
        return near(z, nz, p)[0] if p else z

    weights = ((gate, gate_v), (up, up_v), (down, down_v))

    def own_piece(m, h, u):
        ref = weights[m][0]
        if m < 2:
            return ref.at[pl.ds(u * (depth // 2), depth // 2), pl.ds(mo(h * hid, 128), hid)]
        return ref.at[pl.ds(mo(h * hid + u * (hid // 2), 16), hid // 2), :]

    def place(m, src, u):
        buf = weights[m][1]
        if m < 2:
            return buf.at[pl.ds(mo(src * depth + u * (depth // 2), 16), depth // 2), :]
        return buf.at[src, pl.ds(u * (hid // 2), hid // 2), :]

    def arrived(ref, sem):
        pltpu.make_async_copy(ref, ref, sem).wait()

    locals_ = {}

    def local(key, src, dst, sem):
        copy = pltpu.make_async_copy(src, dst, sem)
        copy.start()
        locals_[key] = copy

    steps = [(m, 0) for m in range(2)] + [(m, p) for m in range(2) for p in range(1, nz)]
    steps += [(m, p) for m in range(2, 4) for p in range(nz)]

    def pieces(m):
        return range(2) if m < 3 else range(1)

    tall = mix_out.shape[0]
    early = tall // 4
    late_rows = pl.ds(0, tall - early)
    early_rows = pl.ds(tall - early, early)

    def spot(m, src, u):
        return place(m, src, u) if m < 3 else mout_v.at[src, late_rows, :]

    def sem_of(m, src, u):
        return ff_sem.at[m, src]

    def origin(m, h, u):
        return own_piece(m, h, u) if m < 3 else mix_out.at[late_rows, :]

    def stage0(n):
        m, p = steps[n]
        if p == 0:
            return
        t = plane(p)
        for u in pieces(m):
            sends.put(origin(m, t % 2, u), spot(m, me, u), sem_of(m, me, u), {"fs": t * sz + col})

    def stage1(n):
        m, p = steps[n]
        src = plane(p) * sz + col
        if p:
            came(m, src)
        for u in pieces(m):
            for nb in (xn, yn):
                first = spot(m, src, u) if p else origin(m, z % 2, u)
                sends.put(first, spot(m, src, u), sem_of(m, src, u), {"fs": nb})
            if not p:
                key = local_sem.at[0] if m == 3 else loc_ff.at[m, u]
                local((m, u), origin(m, z % 2, u), spot(m, me, u), key)

    def shard(m, src):
        if m < 2:
            return weights[m][1].at[pl.ds(mo(src * depth, 16), depth), :]
        return down_v.at[src] if m < 3 else spot(m, src, 0)

    def came(m, src):
        arrived(shard(m, src), ff_sem.at[m, src])

    def three(p):
        shift = plane(p) * sz - z * sz
        return xn + shift, yn + shift, dg + shift

    def relay(m, p, u, across):
        a, b, _ = three(p)
        src, to = (a, yn) if across else (b, xn)
        came(m, src)
        sends.put(spot(m, src, u), spot(m, src, u), sem_of(m, src, u), {"fs": to})

    def stage2(n):
        m, p = steps[n]
        if m < 3:
            relay(m, p, 0, True)
            relay(m, p, 1, False)
        else:
            relay(m, p, 0, p % 2 == 0)

    def stage3(n):
        m, p = steps[n]
        a, b, d = three(p)
        if m == 3:
            came(m, b if p % 2 == 0 else a)
        came(m, d)
        if p == 0:
            for u in pieces(m):
                locals_[(m, u)].wait()

    def mix_at(k, src):
        if k == 0:
            return min_v.at[pl.ds(mo(src * depth, 16), depth), :]
        return mout_v.at[src, early_rows, :]

    mixes = (mix_in, mix_out.at[early_rows, :])

    def mix_own():
        for k, ref in enumerate(mixes):
            for nb in (xn, yn):
                sends.put(ref, mix_at(k, me), mix_sem.at[k, me], {"fs": nb})
            local(("mix", k), ref, mix_at(k, me), loc_ff.at[3, k])

    def mix_turn():
        for k, (src, to) in enumerate(((xn, yn), (yn, xn))):
            arrived(mix_at(k, src), mix_sem.at[k, src])
            sends.put(mix_at(k, src), mix_at(k, src), mix_sem.at[k, src], {"fs": to})

    def mix_up():
        for k, src in enumerate((yn, xn)):
            arrived(mix_at(k, src), mix_sem.at[k, src])
        for k in range(2):
            arrived(mix_at(k, dg), mix_sem.at[k, dg])
            locals_[("mix", k)].wait()
            for src in (me, xn, yn, dg):
                here = mix_at(k, src)
                for step in (1, -1):
                    ok = jnp.logical_and(z + step >= 0, z + step < nz)
                    sends.put(here, here, mix_sem.at[k, src], {"fs": me + step * sz}, ok)

    def mix_on(p, forward=True):
        found, away = near(z, nz, p)
        shift = (found - z) * sz
        inside = jnp.logical_and(z + away >= 0, z + away < nz)
        for k in range(2):
            for src in (me + shift, xn + shift, yn + shift, dg + shift):
                here, sem = mix_at(k, src), mix_sem.at[k, src]
                if forward:
                    when(inside, functools.partial(arrived, here, sem))
                    sends.put(here, here, sem, {"fs": me + away * sz}, inside)
                else:
                    when(jnp.logical_not(inside), functools.partial(arrived, here, sem))

    mine = pl.ds(mo(core * half, 16), half)
    theirs = pl.ds(mo((1 - core) * half, 16), half)
    mine_far = pl.ds(mo(rows + core * half, 16), half)
    theirs_far = pl.ds(mo(rows + (1 - core) * half, 16), half)
    partner = {"tp": 1 - core}
    buddy = {"fs": peer}

    def tokens_out():
        sends.put(tokens.at[mine, :], tok_v.at[mine_far, :], act_sem.at[0], buddy)
        local("tok", tokens, tok_v.at[pl.ds(0, rows), :], local_sem.at[1])
        small = ((pool_far, pool_w), (scale_far, pool_scale), (gains_far, gains))
        for k, (src, dst) in enumerate(small):
            local(("small", k), src, dst, local_sem.at[5 + k])

    def tokens_on():
        here = tok_v.at[mine_far, :]
        arrived(here, act_sem.at[0])
        sends.put(here, here, act_sem.at[1], partner)

    def first_norm():
        arrived(tok_v.at[theirs_far, :], act_sem.at[1])
        locals_["tok"].wait()
        for k in range(3):
            locals_[("small", k)].wait()

        def block(i, carry):
            at = pl.ds(pl.multiple_of(i * 32, 32), 32)
            v = tok_v[at, :].astype(F32)
            norm_v[at, :] = rms_value(v, gains[0:1, :]).astype(BF16)
            return carry

        lax.fori_loop(0, 2 * rows // 32, block, 0)

    tiles = hid // 256

    def gate_up(src, at, dst, low=0, high=None):
        def tile(cols, n):
            w = jnp.concatenate([gate_v[:, cols], up_v[:, cols]], axis=1)
            both = jnp.dot(src[at, :], w, preferred_element_type=F32)
            hid_v[dst, cols] = (silu(both[:, :n]) * both[:, n:]).astype(BF16)

        def body(j, carry):
            tile(pl.ds(pl.multiple_of(j * 256, 256), 256), 256)
            return carry

        lax.fori_loop(low, tiles if high is None else high, body, 0)
        if hid % 256 and high is None:
            tile(pl.ds(tiles * 256, hid % 256), hid % 256)

    def down_block(first, many, at):
        w = jnp.concatenate([down_v[first + i] for i in range(many)], axis=1)
        return jnp.dot(hid_v[at, :], w, preferred_element_type=F32).astype(BF16)

    def cols_of(first, many):
        return pl.ds(mo(first * wide, 128), many * wide)

    def down1(first, many, sem):
        cols = cols_of(first, many)
        for i, (base, other) in enumerate(((rows, theirs_far), (0, theirs))):
            at = pl.ds(base, rows)
            part_v[at, cols] = down_block(first, many, at)
            sends.put(part_v.at[other, cols], got1.at[1 - i, :, cols], act_sem.at[sem + i], partner)

    def reduce1(first, many, sem):
        cols = cols_of(first, many)
        for i in range(2):
            arrived(got1.at[1 - i, :, cols], act_sem.at[sem + i])
        total = part_v[mine_far, cols].astype(F32) + got1[1, :, cols].astype(F32)
        sum1[:, cols] = total.astype(BF16)
        sends.put(sum1.at[:, cols], far1.at[:, cols], sum_sem(first, many), buddy)

    row_y = (me // sy) % 2

    def near_pair(p):
        return plane(p) * sz + row_y * sy

    def far_pair(p):
        return plane(p) * sz + (1 - row_y) * sy

    def sum_sem(first, many):
        t = first // sz
        return act_sem.at[29 + 2 * t + ((first // sy) % 2 if many < sz else 0)]

    def first_stream():
        buddy_z = z + sign
        for p in range(nz):
            t = near(buddy_z, nz, p)[0] if p else buddy_z
            if p < nz - 1:
                cols = cols_of(t * sz, sz)
                arrived(far1.at[:, cols], sum_sem(t * sz, sz))
            else:
                for k in range(2):
                    cols = cols_of(t * sz + k * sy, sy)
                    arrived(far1.at[:, cols], sum_sem(t * sz + k * sy, sy))
        for start, size in runs(0, half):
            r = pl.ds(start, size)
            at = pl.ds(pl.multiple_of(core * half + start, 16), size)
            y = part_v[at, :].astype(F32) + got1[0, r, :].astype(F32) + far1[r, :].astype(F32)
            s = tok_v[at, :].astype(F32) + 0.5 * rms_value(y, gains[1:2, :])
            stream_v[r, :] = s
            mid_v[at, :] = rms_value(s, gains[2:3, :]).astype(BF16)
        sends.put(mid_v.at[mine, :], mid_v.at[mine, :], act_sem.at[2], partner)

    def into_pool(at):
        v = jnp.dot(mid_v[at, :], min_v[...], preferred_element_type=F32)
        pin_v[at, :] = v.astype(BF16).astype(F32)

    def pool():
        length = LEN
        groups, dim = pool_w.shape[0], pool_w.shape[1]
        t = lax.broadcasted_iota(jnp.int32, (rows, dim), 0) % length
        for g in range(groups):
            cols = slice(g * dim, (g + 1) * dim)
            v = pin_v[:, cols]
            window = 2 ** (1 + g % 4)
            total, k = v, 1
            while k < window:
                total = total + jnp.where(t >= k, pltpu.roll(total, k, 0), 0.0)
                k *= 2
            count = jnp.minimum(t + 1, window).astype(F32)
            dev = (total / count - v).astype(BF16)
            o = jnp.dot(dev, pool_w[g], preferred_element_type=F32)
            o = o * pool_scale[cols].astype(F32).reshape(1, dim)
            rg_v[:, cols] = o.astype(BF16)

    def out_pool(at):
        for t in range(nz):
            w = jnp.concatenate([mout_v[t * sz + i] for i in range(sz)], axis=1)
            v = jnp.dot(rg_v[at, :], w, preferred_element_type=F32)
            partm_v[at, pl.ds(t * span, span)] = v.astype(BF16)

    units = half // 16
    firsts = [16 * k for k in (0, units * 3 // 10, units * 7 // 10, units)]
    chunks = [(a, b - a) for a, b in zip(firsts[:-1], firsts[1:]) if b > a]

    def own_rows(k):
        first, count = chunks[k]
        return own_v.at[pl.ds(mo(core * half + first, 16), count), :]

    def share(k):
        sends.put(own_rows(k), far_at(k, core), act_sem.at[17 + k], buddy)

    def second_stream():
        for k, (first, count) in enumerate(chunks):
            arrived(gotm.at[pl.ds(first, count), :], act_sem.at[14 + k])
            for start, size in runs(first, count):
                r = pl.ds(start, size)
                at = pl.ds(pl.multiple_of(core * half + start, 16), size)
                y = partm_v[at, :].astype(F32) + gotm[r, :].astype(F32)
                s = stream_v[r, :] + rms_value(y, gains[3:4, :])
                stream_v[r, :] = s
                own_v[at, :] = rms_value(s, gains[4:5, :]).astype(BF16)
            if k == 0:
                share(0)
            src = own_rows(k)
            sends.put(src, src, act_sem.at[29 + 2 * nz + k], partner)

    def far_rows(k, c):
        first, count = chunks[k]
        return mo(2 * first + c * count, 16), count

    def far_at(k, c):
        return far_v.at[pl.ds(*far_rows(k, c)), :]

    def far_on(k):
        arrived(far_at(k, core), act_sem.at[17 + k])
        sends.put(far_at(k, core), far_at(k, core), act_sem.at[20 + k], partner)

    def down2(base, count, low, high):
        at = pl.ds(base, count)

        def body(t, carry):
            part2_v[at, pl.ds(pl.multiple_of(t * span, 128), span)] = down_block(t * sz, sz, at)
            return carry

        lax.fori_loop(low, high, body, 0)

    def far_part(k, c):
        first, count = far_rows(k, c)
        return pl.ds(mo(rows + first, 16), count)

    last = len(steps)
    stage1(0)
    for n in range(2, 6):
        stage0(n)
    stage1(1)
    mix_own()
    tokens_out()
    stage2(0)
    stage2(1)
    all_mine = pl.ds(0, rows)
    all_far = pl.ds(rows, rows)

    z_order = {0: (6, 7), 2: (9,), 3: (10, 11)}
    z_order.update({2 * nz - 1 + k: (3 * nz + 1 + k,) for k in range(nz - 1)})

    def advance(i):
        for n in z_order.get(i, ()):
            stage0(n)
        if i + 2 < last:
            stage1(i + 2)
        if 0 < i < last - 1:
            stage2(i + 1)
        stage3(i)

    final = 3 * nz - 1
    for i in range(final):
        advance(i)
        if i == 0:
            mix_turn()
        if i == 1:
            mix_up()
        if i == 2:
            tokens_on()
        if i == 4:
            first_norm()
        for p, when_on in enumerate((5, 6)):
            if i == when_on:
                mix_on(p + 1)
        if i == 2 * nz - 1:
            gate_up(norm_v, all_mine, all_mine)
        if i == 2 * nz:
            gate_up(norm_v, all_far, all_far)
            for p in range(3, nz):
                mix_on(p)
            down1(plane(0) * sz, sz, 4)
        if i == 2 * nz + 1:
            down1(plane(1) * sz, sz, 6)
            reduce1(plane(0) * sz, sz, 4)
        if i == 2 * nz + 2:
            down1(plane(2) * sz, sz, 8)
            reduce1(plane(1) * sz, sz, 6)
    late = range(3 * nz, last)
    for n in late[2:]:
        stage1(n - 1)
    stage1(last - 1)
    stage2(late[0])
    d = three(nz - 1)[2]
    down1(near_pair(nz - 1), sy, 10)
    reduce1(plane(2) * sz, sz, 8)
    came(2, d)
    down1(far_pair(nz - 1), sy, 12)
    reduce1(near_pair(nz - 1), sy, 10)
    stage2(late[1])
    reduce1(far_pair(nz - 1), sy, 12)
    for n in late[2:]:
        stage2(n)
    for p in range(1, nz):
        mix_on(p, forward=False)
    first_stream()
    into_pool(mine)
    arrived(mid_v.at[theirs, :], act_sem.at[2])
    into_pool(theirs)
    pool()
    for n in late:
        stage3(n)
    out_pool(theirs)
    for k, (first, count) in enumerate(chunks):
        src = partm_v.at[pl.ds(mo((1 - core) * half + first, 16), count), :]
        sends.put(src, gotm.at[pl.ds(first, count), :], act_sem.at[14 + k], partner)
    out_pool(mine)
    second_stream()

    def far_product(k):
        first, count = chunks[k]
        arrived(far_at(k, 1 - core), act_sem.at[20 + k])
        src, dst = pl.ds(2 * first, 2 * count), pl.ds(rows + 2 * first, 2 * count)
        gate_up(far_v, src, dst, 0, tiles // 2)
        if k:
            far_sum(k - 1)
        gate_up(far_v, src, dst, tiles // 2)
        if k + 1 < len(chunks):
            far_on(k + 1)
        down2(rows + 2 * first, 2 * count, 0, nz)
        here = got2f.at[pl.ds(first, count), :]
        sends.put(part2_v.at[far_part(k, 1 - core), :], here, act_sem.at[23 + k], partner)

    def far_sum(k):
        here = pl.ds(*chunks[k])
        arrived(got2f.at[here, :], act_sem.at[23 + k])
        total = part2_v[far_part(k, core), :].astype(F32) + got2f[here, :].astype(F32)
        sum2[here, :] = total.astype(BF16)
        sends.put(sum2.at[here, :], far2.at[here, :], act_sem.at[26 + k], buddy)

    for k, (first, count) in enumerate(chunks):
        here = pl.ds(mo((1 - core) * half + first, 16), count)
        arrived(own_v.at[here, :], act_sem.at[29 + 2 * nz + k])
    gate_up(own_v, all_mine, all_mine, 0, tiles // 2)
    share(1)
    gate_up(own_v, all_mine, all_mine, tiles // 2)
    far_on(0)
    share(2)
    down2(0, rows, 0, nz // 2)
    for k in range(len(chunks)):
        far_product(k)
    down2(0, rows, nz // 2, nz)
    sends.put(part2_v.at[theirs, :], got2o, act_sem.at[3], partner)
    far_sum(len(chunks) - 1)
    arrived(got2o, act_sem.at[3])
    for k, (first, count) in enumerate(chunks):
        arrived(far2.at[pl.ds(first, count), :], act_sem.at[26 + k])
        for start, size in runs(first, count):
            r = pl.ds(start, size)
            at = pl.ds(pl.multiple_of(core * half + start, 16), size)
            y = part2_v[at, :].astype(F32) + got2o[r, :].astype(F32) + far2[r, :].astype(F32)
            s = stream_v[r, :] + 0.5 * rms_value(y, gains[5:6, :])
            out_v[r, :] = s.astype(BF16)
        here = pl.ds(first, count)
        local(("out", k), out_v.at[here, :], out.at[here, :], local_sem.at[2 + k])
    sends.drain()
    for k in range(len(chunks)):
        locals_[("out", k)].wait()


def whole_layer(dims, tokens, w_gate, w_up, w_down, w_mix_in, w_mix_out, pool_w, pool_scale, gains):
    count = 1
    for size, _ in dims:
        count *= size
    nz = dims[0][0]
    depth, units = w_gate.shape
    hid = units // 2
    rows, feat = tokens.shape
    half = rows // 2
    wide = w_down.shape[1]
    pooled = w_mix_in.shape[1]

    def buf(*shape, dtype=BF16):
        return pltpu.VMEM(shape, dtype)

    scratch = [
        buf(count * depth, hid),
        buf(count * depth, hid),
        buf(count, hid, wide),
        buf(count * depth, pooled),
        buf(count, w_mix_out.shape[0], wide),
        buf(2 * rows, feat),
        buf(2 * rows, feat),
        buf(rows, feat),
        buf(rows, feat),
        buf(2 * rows, hid),
        buf(2 * rows, feat),
        buf(2 * rows, feat),
        buf(rows, feat),
        buf(2, half, feat),
        buf(half, feat),
        buf(half, feat),
        buf(half, feat),
        buf(half, feat),
        buf(half, feat),
        buf(half, feat),
        buf(half, feat),
        buf(half, feat, dtype=F32),
        buf(rows, feat),
        buf(rows, pooled, dtype=F32),
        buf(rows, pooled),
        buf(half, feat),
        buf(*pool_w.shape),
        buf(*pool_scale.shape),
        buf(*gains.shape, dtype=F32),
        pltpu.SemaphoreType.DMA((SENDS,)),
        pltpu.SemaphoreType.DMA((4, count)),
        pltpu.SemaphoreType.DMA((2, count)),
        pltpu.SemaphoreType.DMA((32 + 2 * nz,)),
        pltpu.SemaphoreType.DMA((8,)),
        pltpu.SemaphoreType.DMA((4, 2)),
    ]
    hbm = pl.BlockSpec(memory_space=pltpu.HBM)
    return pl.pallas_call(
        functools.partial(layer_kernel, dims),
        out_shape=jax.ShapeDtypeStruct((half, feat), tokens.dtype),
        in_specs=[hbm] * 9,
        out_specs=hbm,
        scratch_shapes=scratch,
        compiler_params=pltpu.CompilerParams(
            collective_id=1, has_side_effects=True, vmem_limit_bytes=67043328
        ),
        name="whole_layer",
    )(tokens, w_gate, w_up, w_down, w_mix_in, w_mix_out, pool_w, pool_scale, gains)


def paired(dims, mesh):
    return (
        len(dims) == 3
        and dims[0][0] == 4
        and dims[1][0] == 2
        and dims[2][0] == 2
        and mesh.shape["tp"] == 2
    )


def solution(mesh):
    in_specs = (
        P("fs", None),
        P("fs", "tp"),
        P("fs", "tp"),
        P("tp", "fs"),
        P("fs", "tp"),
        P("tp", "fs"),
        P("tp", None, None),
        P("tp"),
        P(),
    )
    out_specs = P(("fs", "tp"), None)
    dims = line_dims(mesh)
    act = whole_layer if paired(dims, mesh) else body
    return jax.shard_map(
        functools.partial(act, dims), mesh=mesh, in_specs=in_specs, out_specs=out_specs, check_vma=False
    )
```

```python
import functools
import itertools

import jax
import jax.numpy as jnp
from jax import lax
from jax.experimental import pallas as pl
from jax.experimental.pallas import tpu as pltpu
from jax.sharding import PartitionSpec as P

LEN = 64
MESH = pl.DeviceIdType.MESH


def line_dims(mesh):
    devices = mesh.devices.reshape(mesh.shape["fs"], -1)[:, 0]
    count = len(devices)
    coords = [tuple(getattr(d, "coords", ())) for d in devices]
    dims = []
    for axis in range(len(coords[0])):
        values = sorted({c[axis] for c in coords})
        if len(values) > 1:
            stride = next(i for i in range(count) if coords[i][axis] != coords[0][axis])
            dims.append((len(values), stride, axis, values))
    dims.sort(key=lambda d: -d[1])
    good = len(dims) > 0 and all(
        sum(vals.index(c[axis]) * stride for _, stride, axis, vals in dims) == i
        for i, c in enumerate(coords)
    )
    if not good:
        return ((count, 1),)
    return tuple((d[0], d[1]) for d in dims)


def near(position, size, rank):
    inner = jnp.minimum(position, size - 1 - position)
    alternating = rank <= 2 * inner
    distance = jnp.where(alternating, (rank + 1) // 2, rank - inner)
    toward_high = jnp.where(alternating, rank % 2 == 1, 2 * position < size - 1)
    step = jnp.where(toward_high, 1, -1)
    return position + step * distance, -step


def piece_plan(dims, order):
    sizes = [dims[d][0] for d in order]
    slots = []
    for ranks in itertools.product(*[range(n) for n in sizes]):
        slots.append(ranks)
    slots.sort(key=lambda r: (sum(r), r))
    return slots


class Piece:
    def __init__(self, index, dims, order, src_of, dst_of):
        self.index, self.dims, self.order = index, dims, order
        self.src_of, self.dst_of = src_of, dst_of
        self.slots = piece_plan(dims, order)

    def locate(self, me, ranks):
        source, last, away = me, -1, None
        for place, (d, rank) in enumerate(zip(self.order, ranks)):
            if rank > 0:
                size, stride = self.dims[d]
                position = (me // stride) % size
                found, step = near(position, size, rank)
                source = source + (found - position) * stride
                last, away = place, step
        return source, last, away

    def sends(self, me, ranks):
        _, last, away = self.locate(me, ranks)
        out = []
        for place, d in enumerate(self.order):
            size, stride = self.dims[d]
            position = (me // stride) % size
            if place == last:
                if size > 2:
                    ok = jnp.logical_and(position + away >= 0, position + away < size)
                    out.append((ok, me + away * stride))
            elif place > last:
                if size == 2:
                    out.append((None, me + (1 - 2 * position) * stride))
                else:
                    out.append((position + 1 < size, me + stride))
                    out.append((position > 0, me - stride))
        return out


def when(condition, act):
    if condition is None:
        act()
    else:
        pl.when(condition)(act)


def spread(pieces, me, chunk, send_sem, recv_sem, low, high, mode):
    todo = []
    for piece in pieces:
        for ranks in piece.slots:
            todo.append((sum(ranks), piece, ranks))
    todo.sort(key=lambda t: t[0])
    for depth, piece, ranks in todo:
        if not low <= depth < high:
            continue
        source, last, _ = piece.locate(me, ranks)
        landed = piece.dst_of(chunk, source)
        origin = piece.src_of(chunk) if depth == 0 else landed
        recv = recv_sem.at[chunk, piece.index, source]
        if depth > 0 and mode == "start":
            pltpu.make_async_copy(landed, landed, recv).wait()
        base = piece.first_send[ranks]
        for offset, (ok, target) in enumerate(piece.sends(me, ranks)):
            copy = pltpu.make_async_remote_copy(
                src_ref=origin,
                dst_ref=landed,
                send_sem=send_sem.at[chunk, base + offset],
                recv_sem=recv,
                device_id={"fs": target},
                device_id_type=MESH,
            )
            when(ok, copy.start if mode == "start" else copy.wait_send)


def number_sends(pieces):
    total = 0
    for piece in pieces:
        piece.first_send = {}
        for ranks in piece.slots:
            piece.first_send[ranks] = total
            last = max([i for i, r in enumerate(ranks) if r > 0], default=-1)
            for place, d in enumerate(piece.order):
                size = piece.dims[d][0]
                if place == last:
                    total += 1 if size > 2 else 0
                elif place > last:
                    total += 1 if size == 2 else 2
    return total


def cut(extent, unit, share):
    return max(unit, min(extent - unit, round(extent * share / unit) * unit))


def gather_plan(dims, refs, outs, blocks):
    gate, up, down, mix_in, mix_out = refs
    gate_o, up_o, down_o, mix_in_o, mix_out_o = outs
    n = len(dims)
    first = tuple(range(n))
    second = first[1:] + first[:1]
    third = first[-1:] + first[:-1]
    pooled = mix_out.shape[0]

    def rows(ref, out, start_of, size):
        return (
            lambda c: ref.at[pl.ds(start_of(c), size), :],
            lambda c, s: out.at[s, pl.ds(start_of(c), size), :],
        )

    def at(block, offset):
        return lambda c: pl.multiple_of(c * block + offset, 16)

    block, tall = gate.shape[0] // blocks, down.shape[0] // blocks
    down_cut = cut(tall, 16, 2 / 3)
    main = [
        Piece(0, dims, first, *rows(gate, gate_o, at(block, 0), block)),
        Piece(1, dims, third, *rows(up, up_o, at(block, 0), block)),
        Piece(2, dims, first, *rows(down, down_o, at(tall, 0), down_cut)),
        Piece(3, dims, second, *rows(down, down_o, at(tall, down_cut), tall - down_cut)),
    ]
    mix_cut = cut(pooled, 16, 2 / 3)

    def fixed(offset):
        return lambda c: offset

    mix = [
        Piece(0, dims, first, *rows(mix_in, mix_in_o, fixed(0), mix_in.shape[0])),
        Piece(1, dims, third, *rows(mix_out, mix_out_o, fixed(0), mix_cut)),
        Piece(2, dims, second, *rows(mix_out, mix_out_o, fixed(mix_cut), pooled - mix_cut)),
    ]
    return main, mix


def gather_kernel(dims, blocks, *args):
    refs, outs = args[:5], args[5:10]
    beside = None
    if len(args) > 13:
        beside = args[10:12]
        args = args[:10] + args[12:]
    send_sem, recv_sem, local_sem = args[10:13]
    me = lax.axis_index("fs")
    barrier = pltpu.get_barrier_semaphore()
    expected = 0
    for size, stride in dims:
        position = (me // stride) % size
        for step, ok in ((1, position + 1 < size), (-1, position > 0)):
            def signal(step=step, stride=stride):
                pl.semaphore_signal(
                    barrier, inc=1, device_id={"fs": me + step * stride}, device_id_type=MESH
                )

            pl.when(ok)(signal)
            expected = expected + jnp.where(ok, 1, 0)
    pl.semaphore_wait(barrier, expected)

    main, mix = gather_plan(dims, refs, outs, blocks)
    number_sends(main)
    number_sends(mix)
    deepest = sum(size - 1 for size, _ in dims) + 1
    early = min(3, deepest)

    locals_ = []
    for i, (ref, out) in enumerate(zip(refs, outs)):
        if beside is not None and i in (2, 4):
            continue
        locals_.append(pltpu.make_async_copy(ref, out.at[me], local_sem.at[i]))

    go = functools.partial(spread, send_sem=send_sem, recv_sem=recv_sem)
    def shard_in(source, stage, sem, shard, across):
        return pltpu.make_async_copy(
            source, stage.at[:, pl.ds(shard * across, across)], sem.at[shard]
        )

    def lay_in(own, part, stage, sem, rows, height):
        for shard in range(part.shape[0]):
            for mine, source in ((True, own), (False, part.at[shard])):

                @pl.when((me == shard) if mine else (me != shard))
                def _(source=source, shard=shard):
                    piece = source.at[pl.ds(rows, height), :]
                    shard_in(piece, stage, sem, shard, part.shape[2]).start()

    def lay_out(part, whole, stage, sem, rows, height, mode):
        if mode == "start":
            for shard in range(part.shape[0]):
                piece = part.at[shard, pl.ds(rows, height), :]
                shard_in(piece, stage, sem, shard, part.shape[2]).wait()
        copy = pltpu.make_async_copy(
            stage, whole.at[pl.ds(rows, height), :], sem.at[part.shape[0]]
        )
        copy.start() if mode == "start" else copy.wait()

    if beside is not None:
        down_stage, mix_stage, down_sem, mix_sem = args[13:]
        tall = down_stage.shape[1]

        pooled = mix_stage.shape[0]

    def rows_of(c):
        return c * tall if isinstance(c, int) else pl.multiple_of(c * tall, 16)

    def down_in(c):
        slot = c % 2
        lay_in(refs[2], outs[2], down_stage.at[slot], down_sem.at[slot], rows_of(c), tall)

    def down_out(c, mode="start"):
        slot = c % 2
        lay_out(outs[2], beside[0], down_stage.at[slot], down_sem.at[slot], rows_of(c), tall, mode)

    go(mix, me, blocks, low=0, high=1, mode="start")
    go(main, me, 0, low=0, high=1, mode="start")
    for copy in locals_:
        copy.start()
    go(mix, me, blocks, low=1, high=deepest, mode="start")
    if beside is not None:
        lay_in(refs[4], outs[4], mix_stage, mix_sem, 0, pooled)

    def step(i, carry):
        @pl.when(i + 1 < blocks)
        def _():
            go(main, me, i + 1, low=0, high=1, mode="start")

        go(main, me, i, low=1, high=early, mode="start")

        @pl.when(i > 0)
        def _():
            go(main, me, i - 1, low=early, high=deepest, mode="start")

        if beside is not None:

            @pl.when(i > 2)
            def _():
                down_out(i - 3, "end")

            @pl.when(i > 0)
            def _():
                down_in(i - 1)

            @pl.when(i > 1)
            def _():
                down_out(i - 2)

        return carry

    lax.fori_loop(0, blocks, step, 0)
    go(main, me, blocks - 1, low=early, high=deepest, mode="start")
    if beside is not None:
        if blocks > 2:
            down_out(blocks - 3, "end")
        down_in(blocks - 1)
        if blocks > 1:
            down_out(blocks - 2)
        lay_out(outs[4], beside[1], mix_stage, mix_sem, 0, pooled, "start")
        down_out(blocks - 1)

    def finish(i, carry):
        go(main, me, i, low=0, high=deepest, mode="end")
        return carry

    lax.fori_loop(0, blocks, finish, 0)
    go(mix, me, blocks, low=0, high=deepest, mode="end")
    if beside is not None:
        if blocks > 1:
            down_out(blocks - 2, "end")
        down_out(blocks - 1, "end")
        lay_out(outs[4], beside[1], mix_stage, mix_sem, 0, pooled, "end")
    for copy in locals_:
        copy.wait()


def gather_weights(dims, w_gate, w_up, w_down, w_mix_in, w_mix_out):
    count = 1
    for size, _ in dims:
        count *= size
    tiles = (w_gate.shape[0] // 16, w_down.shape[0] // 16)
    blocks = next(b for b in (8, 4, 2, 1) if tiles[0] % b == 0 and tiles[1] % b == 0)
    weights = (w_gate, w_up, w_down, w_mix_in, w_mix_out)
    shapes = [jax.ShapeDtypeStruct((count, *a.shape), a.dtype) for a in weights]

    class Shape:
        def __init__(self, shape):
            self.shape = shape

    stand_in = [Shape(a.shape) for a in weights]
    main, mix = gather_plan(dims, stand_in, [Shape(s.shape) for s in shapes], blocks)
    sends = max(number_sends(main), number_sends(mix))
    scratch = [
        pltpu.SemaphoreType.DMA((blocks + 1, sends)),
        pltpu.SemaphoreType.DMA((blocks + 1, len(main), count)),
        pltpu.SemaphoreType.DMA((5,)),
    ]
    laid = w_down.shape[1] % 128 == 0
    if laid:
        tall, full = w_down.shape[0] // blocks, w_down.shape[1] * count
        shapes += [jax.ShapeDtypeStruct((a.shape[0], full), a.dtype) for a in (w_down, w_mix_out)]
        scratch += [
            pltpu.VMEM((2, tall, full), w_down.dtype),
            pltpu.VMEM((w_mix_out.shape[0], full), w_mix_out.dtype),
            pltpu.SemaphoreType.DMA((2, count + 1)),
            pltpu.SemaphoreType.DMA((count + 1,)),
        ]
    outs = pl.pallas_call(
        functools.partial(gather_kernel, dims, blocks),
        out_shape=shapes,
        in_specs=[pl.BlockSpec(memory_space=pltpu.HBM)] * 5,
        out_specs=[pl.BlockSpec(memory_space=pltpu.HBM)] * len(shapes),
        scratch_shapes=scratch,
        compiler_params=pltpu.CompilerParams(collective_id=0, has_side_effects=True),
        name="gather_weights",
    )(*weights)

    def stacked(a):
        return a.reshape(-1, a.shape[2])

    def beside(a):
        return jnp.transpose(a, (1, 0, 2)).reshape(a.shape[1], -1)

    gate, up, down, mix_in, mix_out = outs[:5]
    if laid:
        return stacked(gate), stacked(up), outs[5], stacked(mix_in), outs[6]
    return stacked(gate), stacked(up), beside(down), stacked(mix_in), beside(mix_out)


def rms_scale(values, gain):
    return values * lax.rsqrt(jnp.mean(values * values, axis=-1, keepdims=True) + 1e-06) * gain


def total_over_tp(left_rows, right_matrix):
    part = jnp.dot(left_rows, right_matrix, preferred_element_type=jnp.float32)
    part = part.astype(jnp.bfloat16)
    if lax.axis_size("tp") == 2:
        other = lax.ppermute(part, "tp", ((0, 1), (1, 0)))
        return part.astype(jnp.float32) + other.astype(jnp.float32)
    return lax.psum(part.astype(jnp.float32), "tp")


def own_total_over_tp(left_rows, right_matrix):
    part = jnp.dot(left_rows, right_matrix, preferred_element_type=jnp.float32)
    part = part.astype(jnp.bfloat16)
    if lax.axis_size("tp") == 2:
        mine = own_rows_of(part)
        half = mine.shape[0]
        theirs = lax.dynamic_slice_in_dim(part, (1 - lax.axis_index("tp")) * half, half, 0)
        other = lax.ppermute(theirs, "tp", ((0, 1), (1, 0)))
        return mine.astype(jnp.float32) + other.astype(jnp.float32)
    return lax.psum_scatter(part.astype(jnp.float32), "tp", scatter_dimension=0, tiled=True)


def own_rows_of(array):
    count = array.shape[0] // lax.axis_size("tp")
    return lax.dynamic_slice_in_dim(array, lax.axis_index("tp") * count, count, 0)


def body(dims, tokens, w_gate, w_up, w_down, w_mix_in, w_mix_out, pool_w, pool_scale, norm_gains):
    rows_all = tokens.shape[0]
    stream = tokens.astype(jnp.float32)
    normed = rms_scale(stream, norm_gains[0]).astype(jnp.bfloat16)
    gate_full, up_full, down_full, mix_in_full, mix_out_full = gather_weights(
        dims, w_gate, w_up, w_down, w_mix_in, w_mix_out
    )
    gate_first = jnp.dot(normed, gate_full, preferred_element_type=jnp.float32)
    up_first = jnp.dot(normed, up_full, preferred_element_type=jnp.float32)
    hidden = (jax.nn.silu(gate_first) * up_first).astype(jnp.bfloat16)
    stream = stream + 0.5 * rms_scale(total_over_tp(hidden, down_full), norm_gains[1])
    normed = rms_scale(stream, norm_gains[2]).astype(jnp.bfloat16)
    pooled_in = jnp.dot(normed, mix_in_full, preferred_element_type=jnp.float32)
    pooled_in = pooled_in.astype(jnp.bfloat16)
    groups_here = pool_w.shape[0]
    group_dim = pool_w.shape[1]
    values = pooled_in.astype(jnp.float32).reshape(rows_all // LEN, LEN, groups_here, group_dim)
    totals = jnp.cumsum(values, axis=1)
    position = jnp.arange(1, LEN + 1).astype(jnp.float32)[None, :, None, None]
    window_ids = (lax.axis_index("tp") * groups_here + jnp.arange(groups_here)) % 4
    average = jnp.zeros_like(values)
    for window_slot in range(4):
        window = 2 ** (1 + window_slot)
        lagged = jnp.pad(totals, ((0, 0), (window, 0), (0, 0), (0, 0)))[:, :LEN]
        candidate = (totals - lagged) / jnp.minimum(position, float(window))
        average = jnp.where((window_ids == window_slot)[None, None, :, None], candidate, average)
    deviation = (average - values).astype(jnp.bfloat16)
    regrouped = jnp.einsum("btgi,gio->btgo", deviation, pool_w, preferred_element_type=jnp.float32)
    regrouped = (
        regrouped.reshape(rows_all, groups_here * group_dim) * pool_scale.astype(jnp.float32)
    ).astype(jnp.bfloat16)
    stream = stream + rms_scale(total_over_tp(regrouped, mix_out_full), norm_gains[3])
    normed = rms_scale(stream, norm_gains[4]).astype(jnp.bfloat16)
    gate_second = jnp.dot(normed, gate_full, preferred_element_type=jnp.float32)
    up_second = jnp.dot(normed, up_full, preferred_element_type=jnp.float32)
    hidden = (jax.nn.silu(gate_second) * up_second).astype(jnp.bfloat16)
    stream_own = own_rows_of(stream)
    stream_own = stream_own + 0.5 * rms_scale(own_total_over_tp(hidden, down_full), norm_gains[5])
    return stream_own.astype(jnp.bfloat16)


def silu(v):
    return v / (1.0 + jnp.exp(-v))


def rms_value(values, gain):
    return values * lax.rsqrt(jnp.mean(values * values, axis=-1, keepdims=True) + 1e-06) * gain


def runs(first, count, most=32):
    out, at = [], first
    while at < first + count:
        size = min(most, first + count - at)
        out.append((at, size))
        at += size
    return out


class Sends:
    def __init__(self, sem):
        self.sem, self.count, self.pending = sem, 0, {}

    def put(self, src, dst, recv, to, ok=None):
        slot = self.count % SENDS
        self.count += 1
        self.settle(slot)
        copy = pltpu.make_async_remote_copy(
            src_ref=src,
            dst_ref=dst,
            send_sem=self.sem.at[slot],
            recv_sem=recv,
            device_id=to,
            device_id_type=MESH,
        )
        when(ok, copy.start)
        self.pending[slot] = (ok, copy)

    def settle(self, slot):
        if slot in self.pending:
            ok, copy = self.pending.pop(slot)
            when(ok, copy.wait_send)

    def drain(self):
        for slot in list(self.pending):
            self.settle(slot)


SENDS = 48
F32, BF16 = jnp.float32, jnp.bfloat16


def layer_kernel(dims, *refs):
    (tokens, gate, up, down, mix_in, mix_out, pool_far, scale_far, gains_far, out) = refs[:10]
    (gate_v, up_v, down_v, min_v, mout_v) = refs[10:15]
    (tok_v, norm_v, own_v, far_v, hid_v, part_v, part2_v, partm_v) = refs[15:23]
    (got1, got2o, got2f, gotm, sum1, sum2, far1, far2) = refs[23:31]
    (stream_v, mid_v, pin_v, rg_v, out_v) = refs[31:36]
    (pool_w, pool_scale, gains) = refs[36:39]
    (send_sem, ff_sem, mix_sem, act_sem, local_sem, loc_ff) = refs[39:]
    (nz, sz), (_, sy), (_, sx) = dims
    me, core = lax.axis_index("fs"), lax.axis_index("tp")
    z = me // sz
    col = me - z * sz
    xn = me + (1 - 2 * ((me // sx) % 2)) * sx
    yn = me + (1 - 2 * ((me // sy) % 2)) * sy
    dg = xn + yn - me
    sign = 1 - 2 * (z % 2)
    peer = me + sign * sz
    depth = gate.shape[0]
    hid = gate_v.shape[1]
    rows = tokens.shape[0]
    half = rows // 2
    wide = down.shape[1]
    feat = tokens.shape[1]
    span = sz * wide

    barrier = pltpu.get_barrier_semaphore()
    friends = [({"fs": xn}), ({"fs": yn}), ({"tp": 1 - core})]
    for k in range(1, nz):
        friends.append({"fs": lax.rem(z + k, nz) * sz + col})
    for to in friends:
        pl.semaphore_signal(barrier, inc=1, device_id=to, device_id_type=MESH)
    pl.semaphore_wait(barrier, len(friends))

    sends = Sends(send_sem)

    def mo(v, n):
        return v if isinstance(v, int) else pl.multiple_of(v, n)

    def plane(p):
        return near(z, nz, p)[0] if p else z

    weights = ((gate, gate_v), (up, up_v), (down, down_v))

    def own_piece(m, h, u):
        ref = weights[m][0]
        if m < 2:
            return ref.at[pl.ds(u * (depth // 2), depth // 2), pl.ds(mo(h * hid, 128), hid)]
        return ref.at[pl.ds(mo(h * hid + u * (hid // 2), 16), hid // 2), :]

    def place(m, src, u):
        buf = weights[m][1]
        if m < 2:
            return buf.at[pl.ds(mo(src * depth + u * (depth // 2), 16), depth // 2), :]
        return buf.at[src, pl.ds(u * (hid // 2), hid // 2), :]

    def arrived(ref, sem):
        pltpu.make_async_copy(ref, ref, sem).wait()

    locals_ = {}

    def local(key, src, dst, sem):
        copy = pltpu.make_async_copy(src, dst, sem)
        copy.start()
        locals_[key] = copy

    steps = [(m, 0) for m in range(2)] + [(m, p) for m in range(2) for p in range(1, nz)]
    steps += [(m, p) for m in range(2, 4) for p in range(nz)]

    def pieces(m):
        return range(2) if m < 3 else range(1)

    tall = mix_out.shape[0]
    early = tall // 4
    late_rows = pl.ds(0, tall - early)
    early_rows = pl.ds(tall - early, early)

    def spot(m, src, u):
        return place(m, src, u) if m < 3 else mout_v.at[src, late_rows, :]

    def sem_of(m, src, u):
        return ff_sem.at[m, src]

    def origin(m, h, u):
        return own_piece(m, h, u) if m < 3 else mix_out.at[late_rows, :]

    def stage0(n):
        m, p = steps[n]
        if p == 0:
            return
        t = plane(p)
        for u in pieces(m):
            sends.put(origin(m, t % 2, u), spot(m, me, u), sem_of(m, me, u), {"fs": t * sz + col})

    def stage1(n):
        m, p = steps[n]
        src = plane(p) * sz + col
        if p:
            came(m, src)
        for u in pieces(m):
            for nb in (xn, yn):
                first = spot(m, src, u) if p else origin(m, z % 2, u)
                sends.put(first, spot(m, src, u), sem_of(m, src, u), {"fs": nb})
            if not p:
                key = local_sem.at[0] if m == 3 else loc_ff.at[m, u]
                local((m, u), origin(m, z % 2, u), spot(m, me, u), key)

    def shard(m, src):
        if m < 2:
            return weights[m][1].at[pl.ds(mo(src * depth, 16), depth), :]
        return down_v.at[src] if m < 3 else spot(m, src, 0)

    def came(m, src):
        arrived(shard(m, src), ff_sem.at[m, src])

    def three(p):
        shift = plane(p) * sz - z * sz
        return xn + shift, yn + shift, dg + shift

    def relay(m, p, u, across):
        a, b, _ = three(p)
        src, to = (a, yn) if across else (b, xn)
        came(m, src)
        sends.put(spot(m, src, u), spot(m, src, u), sem_of(m, src, u), {"fs": to})

    def stage2(n):
        m, p = steps[n]
        if m < 3:
            relay(m, p, 0, True)
            relay(m, p, 1, False)
        else:
            relay(m, p, 0, p % 2 == 0)

    def stage3(n):
        m, p = steps[n]
        a, b, d = three(p)
        if m == 3:
            came(m, b if p % 2 == 0 else a)
        came(m, d)
        if p == 0:
            for u in pieces(m):
                locals_[(m, u)].wait()

    def mix_at(k, src):
        if k == 0:
            return min_v.at[pl.ds(mo(src * depth, 16), depth), :]
        return mout_v.at[src, early_rows, :]

    mixes = (mix_in, mix_out.at[early_rows, :])

    def mix_own():
        for k, ref in enumerate(mixes):
            for nb in (xn, yn):
                sends.put(ref, mix_at(k, me), mix_sem.at[k, me], {"fs": nb})
            local(("mix", k), ref, mix_at(k, me), loc_ff.at[3, k])

    def mix_turn():
        for k, (src, to) in enumerate(((xn, yn), (yn, xn))):
            arrived(mix_at(k, src), mix_sem.at[k, src])
            sends.put(mix_at(k, src), mix_at(k, src), mix_sem.at[k, src], {"fs": to})

    def mix_up():
        for k, src in enumerate((yn, xn)):
            arrived(mix_at(k, src), mix_sem.at[k, src])
        for k in range(2):
            arrived(mix_at(k, dg), mix_sem.at[k, dg])
            locals_[("mix", k)].wait()
            for src in (me, xn, yn, dg):
                here = mix_at(k, src)
                for step in (1, -1):
                    ok = jnp.logical_and(z + step >= 0, z + step < nz)
                    sends.put(here, here, mix_sem.at[k, src], {"fs": me + step * sz}, ok)

    def mix_on(p, forward=True):
        found, away = near(z, nz, p)
        shift = (found - z) * sz
        inside = jnp.logical_and(z + away >= 0, z + away < nz)
        for k in range(2):
            for src in (me + shift, xn + shift, yn + shift, dg + shift):
                here, sem = mix_at(k, src), mix_sem.at[k, src]
                if forward:
                    when(inside, functools.partial(arrived, here, sem))
                    sends.put(here, here, sem, {"fs": me + away * sz}, inside)
                else:
                    when(jnp.logical_not(inside), functools.partial(arrived, here, sem))

    mine = pl.ds(mo(core * half, 16), half)
    theirs = pl.ds(mo((1 - core) * half, 16), half)
    mine_far = pl.ds(mo(rows + core * half, 16), half)
    theirs_far = pl.ds(mo(rows + (1 - core) * half, 16), half)
    partner = {"tp": 1 - core}
    buddy = {"fs": peer}

    def tokens_out():
        sends.put(tokens.at[mine, :], tok_v.at[mine_far, :], act_sem.at[0], buddy)
        local("tok", tokens, tok_v.at[pl.ds(0, rows), :], local_sem.at[1])
        small = ((pool_far, pool_w), (scale_far, pool_scale), (gains_far, gains))
        for k, (src, dst) in enumerate(small):
            local(("small", k), src, dst, local_sem.at[5 + k])

    def tokens_on():
        here = tok_v.at[mine_far, :]
        arrived(here, act_sem.at[0])
        sends.put(here, here, act_sem.at[1], partner)

    def first_norm():
        arrived(tok_v.at[theirs_far, :], act_sem.at[1])
        locals_["tok"].wait()
        for k in range(3):
            locals_[("small", k)].wait()

        def block(i, carry):
            at = pl.ds(pl.multiple_of(i * 32, 32), 32)
            v = tok_v[at, :].astype(F32)
            norm_v[at, :] = rms_value(v, gains[0:1, :]).astype(BF16)
            return carry

        lax.fori_loop(0, 2 * rows // 32, block, 0)

    tiles = hid // 256

    def gate_up(src, at, dst, low=0, high=None):
        def tile(cols, n):
            w = jnp.concatenate([gate_v[:, cols], up_v[:, cols]], axis=1)
            both = jnp.dot(src[at, :], w, preferred_element_type=F32)
            hid_v[dst, cols] = (silu(both[:, :n]) * both[:, n:]).astype(BF16)

        def body(j, carry):
            tile(pl.ds(pl.multiple_of(j * 256, 256), 256), 256)
            return carry

        lax.fori_loop(low, tiles if high is None else high, body, 0)
        if hid % 256 and high is None:
            tile(pl.ds(tiles * 256, hid % 256), hid % 256)

    def down_block(first, many, at):
        w = jnp.concatenate([down_v[first + i] for i in range(many)], axis=1)
        return jnp.dot(hid_v[at, :], w, preferred_element_type=F32).astype(BF16)

    def cols_of(first, many):
        return pl.ds(mo(first * wide, 128), many * wide)

    def down1(first, many, sem):
        cols = cols_of(first, many)
        for i, (base, other) in enumerate(((rows, theirs_far), (0, theirs))):
            at = pl.ds(base, rows)
            part_v[at, cols] = down_block(first, many, at)
            sends.put(part_v.at[other, cols], got1.at[1 - i, :, cols], act_sem.at[sem + i], partner)

    def reduce1(first, many, sem):
        cols = cols_of(first, many)
        for i in range(2):
            arrived(got1.at[1 - i, :, cols], act_sem.at[sem + i])
        total = part_v[mine_far, cols].astype(F32) + got1[1, :, cols].astype(F32)
        sum1[:, cols] = total.astype(BF16)
        sends.put(sum1.at[:, cols], far1.at[:, cols], sum_sem(first, many), buddy)

    row_y = (me // sy) % 2

    def near_pair(p):
        return plane(p) * sz + row_y * sy

    def far_pair(p):
        return plane(p) * sz + (1 - row_y) * sy

    def sum_sem(first, many):
        t = first // sz
        return act_sem.at[29 + 2 * t + ((first // sy) % 2 if many < sz else 0)]

    def first_stream():
        buddy_z = z + sign
        for p in range(nz):
            t = near(buddy_z, nz, p)[0] if p else buddy_z
            if p < nz - 1:
                cols = cols_of(t * sz, sz)
                arrived(far1.at[:, cols], sum_sem(t * sz, sz))
            else:
                for k in range(2):
                    cols = cols_of(t * sz + k * sy, sy)
                    arrived(far1.at[:, cols], sum_sem(t * sz + k * sy, sy))
        for start, size in runs(0, half):
            r = pl.ds(start, size)
            at = pl.ds(pl.multiple_of(core * half + start, 16), size)
            y = part_v[at, :].astype(F32) + got1[0, r, :].astype(F32) + far1[r, :].astype(F32)
            s = tok_v[at, :].astype(F32) + 0.5 * rms_value(y, gains[1:2, :])
            stream_v[r, :] = s
            mid_v[at, :] = rms_value(s, gains[2:3, :]).astype(BF16)
        sends.put(mid_v.at[mine, :], mid_v.at[mine, :], act_sem.at[2], partner)

    def into_pool(at):
        v = jnp.dot(mid_v[at, :], min_v[...], preferred_element_type=F32)
        pin_v[at, :] = v.astype(BF16).astype(F32)

    def pool():
        length = LEN
        groups, dim = pool_w.shape[0], pool_w.shape[1]
        t = lax.broadcasted_iota(jnp.int32, (rows, dim), 0) % length
        for g in range(groups):
            cols = slice(g * dim, (g + 1) * dim)
            v = pin_v[:, cols]
            window = 2 ** (1 + g % 4)
            total, k = v, 1
            while k < window:
                total = total + jnp.where(t >= k, pltpu.roll(total, k, 0), 0.0)
                k *= 2
            count = jnp.minimum(t + 1, window).astype(F32)
            dev = (total / count - v).astype(BF16)
            o = jnp.dot(dev, pool_w[g], preferred_element_type=F32)
            o = o * pool_scale[cols].astype(F32).reshape(1, dim)
            rg_v[:, cols] = o.astype(BF16)

    def out_pool(at):
        for t in range(nz):
            w = jnp.concatenate([mout_v[t * sz + i] for i in range(sz)], axis=1)
            v = jnp.dot(rg_v[at, :], w, preferred_element_type=F32)
            partm_v[at, pl.ds(t * span, span)] = v.astype(BF16)

    units = half // 16
    firsts = [16 * k for k in (0, units * 3 // 10, units * 7 // 10, units)]
    chunks = [(a, b - a) for a, b in zip(firsts[:-1], firsts[1:]) if b > a]

    def own_rows(k):
        first, count = chunks[k]
        return own_v.at[pl.ds(mo(core * half + first, 16), count), :]

    def share(k):
        sends.put(own_rows(k), far_at(k, core), act_sem.at[17 + k], buddy)

    def second_stream():
        for k, (first, count) in enumerate(chunks):
            arrived(gotm.at[pl.ds(first, count), :], act_sem.at[14 + k])
            for start, size in runs(first, count):
                r = pl.ds(start, size)
                at = pl.ds(pl.multiple_of(core * half + start, 16), size)
                y = partm_v[at, :].astype(F32) + gotm[r, :].astype(F32)
                s = stream_v[r, :] + rms_value(y, gains[3:4, :])
                stream_v[r, :] = s
                own_v[at, :] = rms_value(s, gains[4:5, :]).astype(BF16)
            if k == 0:
                share(0)
            src = own_rows(k)
            sends.put(src, src, act_sem.at[29 + 2 * nz + k], partner)

    def far_rows(k, c):
        first, count = chunks[k]
        return mo(2 * first + c * count, 16), count

    def far_at(k, c):
        return far_v.at[pl.ds(*far_rows(k, c)), :]

    def far_on(k):
        arrived(far_at(k, core), act_sem.at[17 + k])
        sends.put(far_at(k, core), far_at(k, core), act_sem.at[20 + k], partner)

    def down2(base, count, low, high):
        at = pl.ds(base, count)

        def body(t, carry):
            part2_v[at, pl.ds(pl.multiple_of(t * span, 128), span)] = down_block(t * sz, sz, at)
            return carry

        lax.fori_loop(low, high, body, 0)

    def far_part(k, c):
        first, count = far_rows(k, c)
        return pl.ds(mo(rows + first, 16), count)

    last = len(steps)
    stage1(0)
    for n in range(2, 6):
        stage0(n)
    stage1(1)
    mix_own()
    tokens_out()
    stage2(0)
    stage2(1)
    all_mine = pl.ds(0, rows)
    all_far = pl.ds(rows, rows)

    z_order = {0: (6, 7), 2: (9,), 3: (10,), 4: (11,)}
    z_order.update({nz + 1 + k: (3 * nz + 1 + k,) for k in range(nz - 1)})

    def advance(i):
        for n in z_order.get(i, ()):
            stage0(n)
        if i + 2 < last:
            stage1(i + 2)
        if 0 < i < last - 1:
            stage2(i + 1)
        stage3(i)

    final = 3 * nz - 1
    for i in range(final):
        advance(i)
        if i == 0:
            mix_turn()
        if i == 1:
            mix_up()
        if i == 2:
            tokens_on()
        if i == 4:
            first_norm()
        for p, when_on in enumerate((5, 6)):
            if i == when_on:
                mix_on(p + 1)
        if i == 2 * nz - 1:
            gate_up(norm_v, all_mine, all_mine)
        if i == 2 * nz:
            gate_up(norm_v, all_far, all_far)
            for p in range(3, nz):
                mix_on(p)
            down1(plane(0) * sz, sz, 4)
        if i == 2 * nz + 1:
            down1(plane(1) * sz, sz, 6)
            reduce1(plane(0) * sz, sz, 4)
        if i == 2 * nz + 2:
            down1(plane(2) * sz, sz, 8)
            reduce1(plane(1) * sz, sz, 6)
    late = range(3 * nz, last)
    for n in late[2:]:
        stage1(n - 1)
    stage1(last - 1)
    stage2(late[0])
    d = three(nz - 1)[2]
    down1(near_pair(nz - 1), sy, 10)
    reduce1(plane(2) * sz, sz, 8)
    came(2, d)
    down1(far_pair(nz - 1), sy, 12)
    reduce1(near_pair(nz - 1), sy, 10)
    reduce1(far_pair(nz - 1), sy, 12)
    stage2(late[1])
    for n in late[2:]:
        stage2(n)
    for p in range(1, nz):
        mix_on(p, forward=False)
    first_stream()
    into_pool(mine)
    arrived(mid_v.at[theirs, :], act_sem.at[2])
    into_pool(theirs)
    pool()
    for n in late:
        stage3(n)
    out_pool(theirs)
    for k, (first, count) in enumerate(chunks):
        src = partm_v.at[pl.ds(mo((1 - core) * half + first, 16), count), :]
        sends.put(src, gotm.at[pl.ds(first, count), :], act_sem.at[14 + k], partner)
    out_pool(mine)
    second_stream()

    def far_product(k):
        first, count = chunks[k]
        arrived(far_at(k, 1 - core), act_sem.at[20 + k])
        src, dst = pl.ds(2 * first, 2 * count), pl.ds(rows + 2 * first, 2 * count)
        gate_up(far_v, src, dst, 0, tiles // 2)
        if k:
            far_sum(k - 1)
        gate_up(far_v, src, dst, tiles // 2)
        if k + 1 < len(chunks):
            far_on(k + 1)
        down2(rows + 2 * first, 2 * count, 0, nz)
        here = got2f.at[pl.ds(first, count), :]
        sends.put(part2_v.at[far_part(k, 1 - core), :], here, act_sem.at[23 + k], partner)

    def far_sum(k):
        here = pl.ds(*chunks[k])
        arrived(got2f.at[here, :], act_sem.at[23 + k])
        total = part2_v[far_part(k, core), :].astype(F32) + got2f[here, :].astype(F32)
        sum2[here, :] = total.astype(BF16)
        sends.put(sum2.at[here, :], far2.at[here, :], act_sem.at[26 + k], buddy)

    for k, (first, count) in enumerate(chunks):
        here = pl.ds(mo((1 - core) * half + first, 16), count)
        arrived(own_v.at[here, :], act_sem.at[29 + 2 * nz + k])
    gate_up(own_v, all_mine, all_mine, 0, tiles // 2)
    share(1)
    gate_up(own_v, all_mine, all_mine, tiles // 2)
    far_on(0)
    share(2)
    down2(0, rows, 0, nz // 2)
    for k in range(len(chunks)):
        far_product(k)
    down2(0, rows, nz // 2, nz)
    sends.put(part2_v.at[theirs, :], got2o, act_sem.at[3], partner)
    far_sum(len(chunks) - 1)
    arrived(got2o, act_sem.at[3])
    for k, (first, count) in enumerate(chunks):
        arrived(far2.at[pl.ds(first, count), :], act_sem.at[26 + k])
        for start, size in runs(first, count):
            r = pl.ds(start, size)
            at = pl.ds(pl.multiple_of(core * half + start, 16), size)
            y = part2_v[at, :].astype(F32) + got2o[r, :].astype(F32) + far2[r, :].astype(F32)
            s = stream_v[r, :] + 0.5 * rms_value(y, gains[5:6, :])
            out_v[r, :] = s.astype(BF16)
        here = pl.ds(first, count)
        local(("out", k), out_v.at[here, :], out.at[here, :], local_sem.at[2 + k])
    sends.drain()
    for k in range(len(chunks)):
        locals_[("out", k)].wait()


def whole_layer(dims, tokens, w_gate, w_up, w_down, w_mix_in, w_mix_out, pool_w, pool_scale, gains):
    count = 1
    for size, _ in dims:
        count *= size
    nz = dims[0][0]
    depth, units = w_gate.shape
    hid = units // 2
    rows, feat = tokens.shape
    half = rows // 2
    wide = w_down.shape[1]
    pooled = w_mix_in.shape[1]

    def buf(*shape, dtype=BF16):
        return pltpu.VMEM(shape, dtype)

    scratch = [
        buf(count * depth, hid),
        buf(count * depth, hid),
        buf(count, hid, wide),
        buf(count * depth, pooled),
        buf(count, w_mix_out.shape[0], wide),
        buf(2 * rows, feat),
        buf(2 * rows, feat),
        buf(rows, feat),
        buf(rows, feat),
        buf(2 * rows, hid),
        buf(2 * rows, feat),
        buf(2 * rows, feat),
        buf(rows, feat),
        buf(2, half, feat),
        buf(half, feat),
        buf(half, feat),
        buf(half, feat),
        buf(half, feat),
        buf(half, feat),
        buf(half, feat),
        buf(half, feat),
        buf(half, feat, dtype=F32),
        buf(rows, feat),
        buf(rows, pooled, dtype=F32),
        buf(rows, pooled),
        buf(half, feat),
        buf(*pool_w.shape),
        buf(*pool_scale.shape),
        buf(*gains.shape, dtype=F32),
        pltpu.SemaphoreType.DMA((SENDS,)),
        pltpu.SemaphoreType.DMA((4, count)),
        pltpu.SemaphoreType.DMA((2, count)),
        pltpu.SemaphoreType.DMA((32 + 2 * nz,)),
        pltpu.SemaphoreType.DMA((8,)),
        pltpu.SemaphoreType.DMA((4, 2)),
    ]
    hbm = pl.BlockSpec(memory_space=pltpu.HBM)
    return pl.pallas_call(
        functools.partial(layer_kernel, dims),
        out_shape=jax.ShapeDtypeStruct((half, feat), tokens.dtype),
        in_specs=[hbm] * 9,
        out_specs=hbm,
        scratch_shapes=scratch,
        compiler_params=pltpu.CompilerParams(
            collective_id=1, has_side_effects=True, vmem_limit_bytes=67043328
        ),
        name="whole_layer",
    )(tokens, w_gate, w_up, w_down, w_mix_in, w_mix_out, pool_w, pool_scale, gains)


def paired(dims, mesh):
    return (
        len(dims) == 3
        and dims[0][0] == 4
        and dims[1][0] == 2
        and dims[2][0] == 2
        and mesh.shape["tp"] == 2
    )


def solution(mesh):
    in_specs = (
        P("fs", None),
        P("fs", "tp"),
        P("fs", "tp"),
        P("tp", "fs"),
        P("fs", "tp"),
        P("tp", "fs"),
        P("tp", None, None),
        P("tp"),
        P(),
    )
    out_specs = P(("fs", "tp"), None)
    dims = line_dims(mesh)
    act = whole_layer if paired(dims, mesh) else body
    return jax.shard_map(
        functools.partial(act, dims), mesh=mesh, in_specs=in_specs, out_specs=out_specs, check_vma=False
    )
```
